256 devices in a mesh: grp: 2 (over y), sp: 16 (over z), fs: 4 (over x), tp: 2 (over core).
Axes of the slice: x: 4, y: 2, z: 16, core: 2. Of those that a mesh axis runs over, the one named last changes fastest.
The devices are a block of a 4x16x16 slice.
Arguments:
- tokens: bfloat16 [16, 1024, 2048], P(('grp', 'fs'), 'sp'), parts along dimension 0, may hold values from -6 to 6
- pre_gain: float32 [2048], replicated, may hold values from 0.1 to 1.9
- query_weight: bfloat16 [2048, 1024], P(('sp', 'fs'), 'tp'), may hold values from -0.125 to 0.125
- key_weight: bfloat16 [2048, 1024], P(('sp', 'fs'), 'tp'), may hold values from -0.125 to 0.125
- value_weight: bfloat16 [2048, 1024], P(('sp', 'fs'), 'tp'), may hold values from -0.125 to 0.125
- beta_weight: bfloat16 [2048, 8], replicated, may hold values from -0.125 to 0.125
- decay_weight: bfloat16 [2048, 8], replicated, may hold values from -0.125 to 0.125
- decay_rate: float32 [8], replicated, may hold values from 0 to 1
- delta_gain: float32 [128], replicated, may hold values from 0.1 to 1.9
- query_down: bfloat16 [2048, 512], P(('sp', 'fs')), may hold values from -0.125 to 0.125
- latent_down: bfloat16 [2048, 256], P(('sp', 'fs')), may hold values from -0.125 to 0.125
- rope_weight: bfloat16 [2048, 32], replicated, may hold values from -0.125 to 0.125
- query_gain: float32 [512], replicated, may hold values from 0.1 to 1.9
- latent_gain: float32 [256], replicated, may hold values from 0.1 to 1.9
- query_up: bfloat16 [512, 1536], P(None, 'tp'), may hold values from -4 to 4
- latent_up: bfloat16 [256, 2048], P(None, 'tp'), may hold values from -4 to 4
- delta_out: bfloat16 [1024, 2048], P('tp', ('sp', 'fs')), may hold values from -8 to 8
- latent_out: bfloat16 [1024, 2048], P('tp', ('sp', 'fs')), may hold values from -8 to 8
- post_gain: float32 [2048], P('tp'), may hold values from 0.1 to 1.9
Outputs:
- mixed_out: bfloat16 [16, 1024, 2048], P(('grp', 'fs'), 'sp', 'tp'), parts along dimension 0
The draws below stay inside these ranges and needn't reach their ends.
There are 2 independent parts, one for each index of `grp`. The reference program is written for one: setup_inputs(seed, part) draws one part's arguments, and reference() takes and returns one part's arrays. A program takes and returns all parts, laid end to end along the dimension named above; an argument that names none is the same for every part. Nothing has to cross between parts.
All inputs are finite; a program needn't handle non-finite values.
Results may differ from the reference program's by a relative error of at most 0.018.
The reference program's roundings to bfloat16 on the way count: a program that leaves them out, or rounds other values in their place, can miss the bound.
Values may be sent and summed in bfloat16 or wider, within the bound.
A program may use at most 128 MiB of HBM per device.

```python
import math
import jax
import jax.numpy as jnp
from jax import lax

D = 2048
DELTA_HEADS = 8
HEAD = 128
LATENT_HEADS = 16
NOPE = 64
ROPE = 32
VDIM = 64
QRANK = 512
KVRANK = 256
BLOCK = 64
SEQS = 8
LENGTH = 1024


def draw_decay_rate(key, part):
    slow_key, fast_key, order_key = jax.random.split(key, 3)
    slow_rate = jnp.exp(jax.random.uniform(slow_key, (DELTA_HEADS,), jnp.float32, math.log(0.3), math.log(1.5))) / LENGTH
    fast_rate = jnp.exp(jax.random.uniform(fast_key, (DELTA_HEADS,), jnp.float32, math.log(0.025), math.log(0.06)))
    head_order = jax.random.permutation(order_key, DELTA_HEADS)
    return jnp.where(head_order < DELTA_HEADS // 2, fast_rate, slow_rate)


def column_scaled(key, row_count):
    entry_key, jitter_key = jax.random.split(key)
    entries = jnp.clip(jax.random.normal(entry_key, (row_count, D), jnp.float32), -6.0, 6.0)
    jitter = jax.random.uniform(jitter_key, (D,), jnp.float32, -0.5, 0.5)
    column_tilt = 2.2 * (jnp.arange(D, dtype=jnp.float32) / D - 0.5)
    fan_scale = (DELTA_HEADS * HEAD + LATENT_HEADS * VDIM) ** (-0.5)
    return entries * jnp.exp(column_tilt + jitter)[None, :] * fan_scale


def draw_delta_out(key, part):
    return column_scaled(jax.random.fold_in(key, 11), DELTA_HEADS * HEAD).astype(jnp.bfloat16)


def draw_latent_out(key, part):
    return column_scaled(jax.random.fold_in(key, 23), LATENT_HEADS * VDIM).astype(jnp.bfloat16)


def expansion_base(key, rank, head_width):
    entries = jnp.clip(jax.random.normal(key, (rank, LATENT_HEADS, head_width), jnp.float32), -6.0, 6.0)
    return entries / math.sqrt(rank)


def draw_query_up(key, part):
    entries = expansion_base(jax.random.fold_in(key, 31), QRANK, NOPE + ROPE)
    return entries.reshape(QRANK, LATENT_HEADS * (NOPE + ROPE)).astype(jnp.bfloat16)


def draw_latent_up(key, part):
    entries = expansion_base(jax.random.fold_in(key, 53), KVRANK, NOPE + VDIM)
    return entries.reshape(KVRANK, LATENT_HEADS * (NOPE + VDIM)).astype(jnp.bfloat16)


def shard_levels(stream_key, extent, cuts, low, largest):
    def one(axis_at, parts):
        heights = jax.random.uniform(jax.random.fold_in(jax.random.fold_in(stream_key, 6), axis_at), (parts,), jnp.float32, low / len(cuts), largest / len(cuts))
        return jnp.repeat(jnp.exp(heights), extent[axis_at] // parts).reshape((-1,) + (1,) * (len(extent) - axis_at - 1))

    factor_of = one(*cuts[0])
    for cut in cuts[1:]:
        factor_of = factor_of * one(*cut)
    return factor_of


def gaussian(stream_key, dims, scale, limit, cuts=(), held_as=jnp.bfloat16):
    result = scale * jax.random.normal(stream_key, dims, jnp.float32)
    if cuts:
        result = result * shard_levels(stream_key, dims, cuts, -0.22, 0.18)
    return jnp.clip(result, -limit, limit).astype(held_as)


def setup_inputs(seed: int = 0, part: int = 0) -> dict:
    key_of = jax.random.split(jax.random.key(seed), 20)
    own_keys = jax.random.split(jax.random.fold_in(key_of[19], part), 20)
    tokens = gaussian(own_keys[0], (SEQS, LENGTH, D), 1.0, 6.0, ((0, 4), (1, 16)))
    pre_gain = jnp.clip(1.0 + 0.18 * jax.random.normal(key_of[1], (D,), jnp.float32), 0.1, 1.9)
    query_weight = gaussian(key_of[2], (D, DELTA_HEADS * HEAD), D ** -0.5, 0.125, ((0, 64), (1, 2)))
    key_weight = gaussian(key_of[3], (D, DELTA_HEADS * HEAD), D ** -0.5, 0.125, ((0, 64), (1, 2)))
    value_weight = gaussian(key_of[4], (D, DELTA_HEADS * HEAD), D ** -0.5, 0.125, ((0, 64), (1, 2)))
    beta_weight = gaussian(key_of[5], (D, DELTA_HEADS), D ** -0.5, 0.125)
    decay_weight = gaussian(key_of[6], (D, DELTA_HEADS), D ** -0.5, 0.125)
    decay_rate = draw_decay_rate(jax.random.fold_in(key_of[19], 71), part)
    delta_gain = jnp.clip(1.0 + 0.18 * jax.random.normal(key_of[8], (HEAD,), jnp.float32), 0.1, 1.9)
    query_down = gaussian(key_of[9], (D, QRANK), D ** -0.5, 0.125, ((0, 64),))
    latent_down = gaussian(key_of[10], (D, KVRANK), D ** -0.5, 0.125, ((0, 64),))
    rope_weight = gaussian(key_of[11], (D, ROPE), D ** -0.5, 0.125)
    query_gain = jnp.clip(1.0 + 0.18 * jax.random.normal(key_of[12], (QRANK,), jnp.float32), 0.1, 1.9)
    latent_gain = jnp.clip(1.0 + 0.18 * jax.random.normal(key_of[13], (KVRANK,), jnp.float32), 0.1, 1.9)
    query_up = draw_query_up(jax.random.fold_in(key_of[19], 71), part)
    latent_up = draw_latent_up(jax.random.fold_in(key_of[19], 71), part)
    delta_out = draw_delta_out(jax.random.fold_in(key_of[19], 71), part)
    latent_out = draw_latent_out(jax.random.fold_in(key_of[19], 71), part)
    post_gain = jnp.clip(1.0 + 0.18 * jax.random.normal(key_of[18], (D,), jnp.float32), 0.1, 1.9)
    return dict(tokens=tokens, pre_gain=pre_gain, query_weight=query_weight, key_weight=key_weight, value_weight=value_weight, beta_weight=beta_weight, decay_weight=decay_weight, decay_rate=decay_rate, delta_gain=delta_gain, query_down=query_down, latent_down=latent_down, rope_weight=rope_weight, query_gain=query_gain, latent_gain=latent_gain, query_up=query_up, latent_up=latent_up, delta_out=delta_out, latent_out=latent_out, post_gain=post_gain)


NORM_EPS = 1e-06
ROPE_THETA = 10000.0
HIGHEST = lax.Precision.HIGHEST

def stored(values):
    return lax.optimization_barrier(values.astype(jnp.bfloat16))

def rms_scale(values):
    return lax.rsqrt(lax.optimization_barrier(jnp.mean(values * values, axis=-1, keepdims=True)) + NORM_EPS)

def unit_rows(values):
    return values * lax.rsqrt(lax.optimization_barrier(jnp.sum(values * values, axis=-1, keepdims=True)) + NORM_EPS)

def rope_tables(positions, rope_width):
    frequency = ROPE_THETA ** (-jnp.arange(0, rope_width, 2, dtype=jnp.float32) / rope_width)
    angles = positions.astype(jnp.float32)[:, None] * frequency[None, :]
    return (jnp.cos(angles), jnp.sin(angles))

def rotate(values, cosine_table, sine_table):
    lower_half, upper_half = jnp.split(values, 2, axis=-1)
    return jnp.concatenate([lower_half * cosine_table - upper_half * sine_table, upper_half * cosine_table + lower_half * sine_table], axis=-1)

def delta_terms(query_vectors, key_vectors, value_vectors, beta_gate, log_decay):
    length, head_count, head_width = query_vectors.shape
    nblocks = length // BLOCK

    def split_blocks(tensor):
        return jnp.moveaxis(tensor.reshape((nblocks, BLOCK, head_count) + tensor.shape[2:]), 2, 0)
    query_vectors = split_blocks(query_vectors)
    key_vectors = split_blocks(key_vectors)
    value_vectors = split_blocks(value_vectors)
    beta_gate = split_blocks(beta_gate)
    gate_sum = jnp.cumsum(split_blocks(log_decay), axis=-1)
    position = jnp.arange(BLOCK)
    strict = position[:, None] > position[None, :]
    causal = position[:, None] >= position[None, :]
    gate_gap = gate_sum[..., :, None] - gate_sum[..., None, :]
    strict_decay = jnp.where(strict, jnp.exp(jnp.where(strict, gate_gap, 0.0)), 0.0)
    causal_decay = jnp.where(causal, jnp.exp(jnp.where(causal, gate_gap, 0.0)), 0.0)
    keys_scaled = key_vectors * beta_gate[..., None]
    lower_mat = jnp.einsum('hnid,hnjd->hnij', keys_scaled, key_vectors, precision=HIGHEST) * strict_decay
    identity = jnp.eye(BLOCK, dtype=jnp.float32)
    inverse = jax.scipy.linalg.solve_triangular(identity + lower_mat, jnp.broadcast_to(identity, lower_mat.shape), lower=True)
    new_values = jnp.einsum('hnij,hnjd->hnid', inverse, value_vectors * beta_gate[..., None], precision=HIGHEST)
    key_weights = jnp.einsum('hnij,hnjd->hnid', inverse, keys_scaled * jnp.exp(gate_sum)[..., None], precision=HIGHEST)
    scores = jnp.einsum('hnid,hnjd->hnij', query_vectors, key_vectors, precision=HIGHEST) * causal_decay
    last_gate = gate_sum[..., -1]
    query_decay = query_vectors * jnp.exp(gate_sum)[..., None]
    key_decay = key_vectors * jnp.exp(last_gate[..., None] - gate_sum)[..., None]
    return (query_decay, key_decay, new_values, key_weights, scores, last_gate)

def delta_rule(query_vectors, key_vectors, value_vectors, beta_gate, log_decay):
    head_count, head_width = (query_vectors.shape[1], query_vectors.shape[2])
    block_terms = delta_terms(query_vectors, key_vectors, value_vectors, beta_gate, log_decay)
    inputs = tuple((jnp.moveaxis(tensor, 1, 0) for tensor in block_terms))

    def advance(carried, block_in):
        query_decay, key_decay, new_values, key_weights, scores, last_gate = block_in
        corrected = new_values - jnp.einsum('hcd,hde->hce', key_weights, carried, precision=HIGHEST)
        output = jnp.einsum('hcd,hde->hce', query_decay, carried, precision=HIGHEST) + jnp.einsum('hij,hje->hie', scores, corrected, precision=HIGHEST)
        carried = carried * jnp.exp(last_gate)[:, None, None] + jnp.einsum('hcd,hce->hde', key_decay, corrected, precision=HIGHEST)
        return (carried, output)
    zero_state = jnp.zeros((head_count, head_width, head_width), jnp.float32)
    _, outputs = lax.scan(advance, zero_state, inputs)
    return jnp.transpose(outputs, (0, 2, 1, 3)).reshape(-1, head_count, head_width)

def reference(tokens, pre_gain, query_weight, key_weight, value_weight, beta_weight, decay_weight, decay_rate, delta_gain, query_down, latent_down, rope_weight, query_gain, latent_gain, query_up, latent_up, delta_out, latent_out, post_gain):
    f32 = jnp.float32

    def one_sequence(sequence):
        length = sequence.shape[0]
        positions = jnp.arange(length)
        seq_float = sequence.astype(f32)
        normed = stored(seq_float * rms_scale(seq_float) * pre_gain)
        raw_query = stored(jnp.dot(normed, query_weight, preferred_element_type=f32))
        raw_key = stored(jnp.dot(normed, key_weight, preferred_element_type=f32))
        raw_value = stored(jnp.dot(normed, value_weight, preferred_element_type=f32))
        q_latent = stored(jnp.dot(normed, query_down, preferred_element_type=f32))
        kv_latent = stored(jnp.dot(normed, latent_down, preferred_element_type=f32))
        rope_raw = stored(jnp.dot(normed, rope_weight, preferred_element_type=f32))
        beta_gate = jax.nn.sigmoid(jnp.dot(normed, beta_weight, preferred_element_type=f32))
        log_decay = -decay_rate[None, :] * jax.nn.softplus(jnp.dot(normed, decay_weight, preferred_element_type=f32))
        query_vectors = unit_rows(jax.nn.silu(raw_query.astype(f32)).reshape(length, DELTA_HEADS, HEAD)) * HEAD ** (-0.5)
        key_vectors = unit_rows(jax.nn.silu(raw_key.astype(f32)).reshape(length, DELTA_HEADS, HEAD))
        value_vectors = jax.nn.silu(raw_value.astype(f32)).reshape(length, DELTA_HEADS, HEAD)
        delta_raw = delta_rule(query_vectors, key_vectors, value_vectors, beta_gate, log_decay)
        delta_heads = stored(delta_raw * rms_scale(delta_raw) * delta_gain).reshape(length, DELTA_HEADS * HEAD)
        q_lat32 = q_latent.astype(f32)
        kv_lat32 = kv_latent.astype(f32)
        q_normed = stored(q_lat32 * rms_scale(q_lat32) * query_gain)
        kv_normed = stored(kv_lat32 * rms_scale(kv_lat32) * latent_gain)
        cosine_table, sine_table = rope_tables(positions, ROPE)
        rope_keys = stored(rotate(rope_raw.astype(f32), cosine_table, sine_table)).astype(f32)
        query_all = stored(jnp.dot(q_normed, query_up, preferred_element_type=f32)).reshape(length, LATENT_HEADS, NOPE + ROPE)
        kv_all = stored(jnp.dot(kv_normed, latent_up, preferred_element_type=f32)).reshape(length, LATENT_HEADS, NOPE + VDIM)
        query_plain = query_all[..., :NOPE].astype(f32)
        query_turned = stored(rotate(query_all[..., NOPE:].astype(f32), cosine_table[:, None, :], sine_table[:, None, :])).astype(f32)
        key_plain = kv_all[..., :NOPE].astype(f32)
        value_rows = kv_all[..., NOPE:].astype(f32)
        score_scale = (NOPE + ROPE) ** (-0.5)
        query_span = math.gcd(length, 512)
        key_block = positions // BLOCK

        def attend(block_index):
            row_start = block_index * query_span
            plain_rows = lax.dynamic_slice_in_dim(query_plain, row_start, query_span, 0)
            turned_rows = lax.dynamic_slice_in_dim(query_turned, row_start, query_span, 0)
            logits = (jnp.einsum('qhd,khd->hqk', plain_rows, key_plain) + jnp.einsum('qhd,kd->hqk', turned_rows, rope_keys)) * score_scale
            query_block = (row_start + jnp.arange(query_span)) // BLOCK
            allowed = key_block[None, :] <= query_block[:, None]
            logits = jnp.where(allowed[None], logits, -jnp.inf)
            peak = lax.optimization_barrier(jnp.max(logits, axis=-1, keepdims=True))
            weights = jnp.where(allowed[None], jnp.exp(logits - peak), 0.0)
            row_sum = lax.optimization_barrier(jnp.sum(weights, axis=-1))
            weights_b = stored(weights).astype(f32)
            weighted = jnp.einsum('hqk,khd->qhd', weights_b, value_rows)
            return stored(weighted / jnp.transpose(row_sum)[:, :, None]).reshape(query_span, LATENT_HEADS * VDIM)
        latent_heads = lax.map(attend, jnp.arange(length // query_span)).reshape(length, LATENT_HEADS * VDIM)
        half_delta = DELTA_HEADS * HEAD // 2
        half_latent = LATENT_HEADS * VDIM // 2
        mixed = jnp.zeros((length, D), f32)
        for group_index in range(2):
            group_heads = jnp.concatenate([delta_heads[:, group_index * half_delta:(group_index + 1) * half_delta], latent_heads[:, group_index * half_latent:(group_index + 1) * half_latent]], axis=1)
            group_rows = jnp.concatenate([delta_out[group_index * half_delta:(group_index + 1) * half_delta], latent_out[group_index * half_latent:(group_index + 1) * half_latent]], axis=0)
            group_term = jnp.dot(group_heads, group_rows, preferred_element_type=f32)
            mixed = mixed + stored(group_term).astype(f32)
        return (mixed * rms_scale(mixed) * post_gain).astype(jnp.bfloat16)
    return lax.map(one_sequence, tokens)
```

```python
import functools
import math

import jax
import jax.numpy as jnp
from jax import lax
from jax.experimental import pallas as pl
from jax.experimental.pallas import tpu as pltpu
from jax.sharding import PartitionSpec as P

HEAD = 128
NOPE = 64
ROPE = 32
VDIM = 64
BLOCK = 64
LANES = 128

NORM_EPS = 1e-06
ROPE_THETA = 10000.0
F32 = jnp.float32
BF16 = jnp.bfloat16
MESH = pl.DeviceIdType.MESH
VM = pltpu.VMEM


def remote(src, dst, send_sem, recv_sem, where):
    return pltpu.make_async_remote_copy(
        src_ref=src,
        dst_ref=dst,
        send_sem=send_sem,
        recv_sem=recv_sem,
        device_id=where,
        device_id_type=MESH,
    )


def greet(places, count):
    barrier = pltpu.get_barrier_semaphore()
    for place in places:
        pl.semaphore_signal(barrier, inc=1, device_id=place, device_id_type=MESH)
    pl.semaphore_wait(barrier, count)


def mm(left, right):
    return lax.dot_general(
        left.astype(BF16), right.astype(BF16), (((1,), (0,)), ((), ())), preferred_element_type=F32
    )


def mm_nt(left, right):
    return lax.dot_general(
        left.astype(BF16), right.astype(BF16), (((1,), (1,)), ((), ())), preferred_element_type=F32
    )


def project_kernel(
    nz, nx, tok_ref, wp_ref, out_ref, toks, ws,
    loc_sem, tok_send, tok_recv, fwd_send, fwd_recv, wx_send, wx_recv, r_send, r_recv, l_send, l_recv,
):
    z, x, t = lax.axis_index("sp"), lax.axis_index("fs"), lax.axis_index("tp")
    rows = wp_ref.shape[1]
    right, left = {"sp": lax.rem(z + 1, nz)}, {"sp": lax.rem(z + nz - 1, nz)}
    partner = {"tp": 1 - t}
    others = [lax.rem(x + d, nx) for d in range(1, nx)]
    greet([{"fs": o} for o in others] + [right, left, partner], nx + 2)

    def chunk(slot, part):
        return ws.at[slot, pl.ds(part * rows, rows)]

    own_w = pltpu.make_async_copy(wp_ref.at[x], chunk(z, x), loc_sem.at[0])
    own_w.start()
    wx = [
        remote(wp_ref.at[o], chunk(z, x), wx_send.at[d], wx_recv.at[d], {"fs": o})
        for d, o in enumerate(others)
    ]
    for copy in wx:
        copy.start()
    own_t = pltpu.make_async_copy(tok_ref, toks.at[pl.ds(2 * x, 2)], loc_sem.at[1])
    own_t.start()
    tok = [
        remote(tok_ref.at[t], toks.at[2 * x + t], tok_send.at[d], tok_recv.at[d], {"fs": o})
        for d, o in enumerate(others)
    ]
    for copy in tok:
        copy.start()

    reach_r, reach_l = nz // 2, nz // 2 - 1

    def go_right(step, part, slot):
        return remote(
            chunk(slot, part), chunk(slot, part), r_send.at[step, part], r_recv.at[step, part], right
        )

    def go_left(step, part, slot):
        return remote(
            chunk(slot, part), chunk(slot, part), l_send.at[step, part], l_recv.at[step, part], left
        )

    for d in range(nx):
        part = lax.rem(x + nx - d, nx)
        if d == 0:
            own_w.wait()
        else:
            wx[d - 1].wait_recv()
        go_right(0, part, z).start()
        go_left(0, part, z).start()

    def ring(step, carry):
        from_left = lax.rem(z + 2 * nz - 1 - step, nz)
        from_right = lax.rem(z + 1 + step, nz)
        for d in range(nx):
            part = lax.rem(x + nx - d, nx)
            go_right(step, part, from_left).wait_recv()

            @pl.when(step < reach_r - 1)
            def _():
                go_right(step + 1, part, from_left).start()

            @pl.when(step < reach_l)
            def _():
                go_left(step, part, from_right).wait_recv()

            @pl.when(step < reach_l - 1)
            def _():
                go_left(step + 1, part, from_right).start()

        return carry

    lax.fori_loop(0, reach_r, ring, 0)

    own_t.wait()
    fwd = []
    for d in range(nx - 1):
        source = lax.rem(x + nx - 1 - d, nx)
        tok[d].wait_recv()
        copy = remote(
            toks.at[2 * source + t], toks.at[2 * source + t], fwd_send.at[d], fwd_recv.at[d], partner
        )
        copy.start()
        fwd.append(copy)
    for copy in fwd:
        copy.wait_recv()

    depth = ws.shape[0] * ws.shape[1]
    weight = ws[...].reshape(depth, ws.shape[2])
    pair = 2 * toks.shape[1]

    def tile(i, carry):
        lhs = toks[pl.ds(2 * i, 2)].reshape(pair, depth)
        out_ref[pl.ds(pl.multiple_of(i * pair, pair), pair), :] = lax.dot_general(
            lhs, weight, (((1,), (0,)), ((), ())), preferred_element_type=F32
        )
        return carry

    lax.fori_loop(0, nx, tile, 0)

    for copy in wx + tok + fwd:
        copy.wait_send()

    def drain(step, carry):
        for part in range(nx):
            go_right(step, part, z).wait_send()

            @pl.when(step < reach_l)
            def _():
                go_left(step, part, z).wait_send()

        return carry

    lax.fori_loop(0, reach_r, drain, 0)


def project(nz, nx, normed, packed):
    seqs, length, width = normed.shape
    rows, cols = packed.shape[1:]
    dma = pltpu.SemaphoreType.DMA
    return pl.pallas_call(
        functools.partial(project_kernel, nz, nx),
        out_shape=jax.ShapeDtypeStruct((seqs * nx * length, cols), F32),
        in_specs=[pl.BlockSpec(memory_space=VM)] * 2,
        out_specs=pl.BlockSpec(memory_space=VM),
        scratch_shapes=[
            VM((seqs * nx, length, width), BF16),
            VM((nz, nx * rows, cols), BF16),
            dma((2,)),
            dma((nx - 1,)),
            dma((nx - 1,)),
            dma((nx - 1,)),
            dma((nx - 1,)),
            dma((nx - 1,)),
            dma((nx - 1,)),
            dma((nz // 2, nx)),
            dma((nz // 2, nx)),
            dma((nz // 2 - 1, nx)),
            dma((nz // 2 - 1, nx)),
        ],
        compiler_params=pltpu.CompilerParams(collective_id=1, has_side_effects=True),
        name="project",
    )(normed, packed)


def spread_kernel(
    nz, nx, d_ref, g_ref, l_ref, dr, gr, lr,
    loc_sem, d_send, d_recv, g_send, g_recv, l_send, l_recv,
):
    z, x, t = lax.axis_index("sp"), lax.axis_index("fs"), lax.axis_index("tp")
    half = nz // 2
    zh, zl = z // half, lax.rem(z, half)
    near = [
        (dx, dt, lax.rem(x + dx, nx), lax.rem(t + dt, 2), lax.rem(x + nx - dx, nx))
        for dx in range(nx)
        for dt in range(2)
        if dx or dt
    ]
    sources = [{"fs": back, "tp": to} for dx, dt, fx, to, back in near]
    sources += [{"sp": half * t + j, "tp": 1 - zh} for j in range(half)]
    greet(sources, len(sources))
    own = pltpu.make_async_copy(l_ref.at[x], lr.at[2 * x + t], loc_sem.at[0])
    own.start()
    copies = []
    for k, (dx, dt, fx, to, back) in enumerate(near):
        copies.append(
            remote(l_ref.at[fx], lr.at[2 * x + t], l_send.at[k], l_recv.at[k], {"fs": fx, "tp": to})
        )
    for s in range(half):
        where = {"sp": s + half * (1 - t), "tp": zh}
        copies.append(remote(g_ref.at[s], gr.at[zl], g_send.at[s], g_recv.at[zl], where))
        copies.append(remote(d_ref.at[s], dr.at[zl], d_send.at[s], d_recv.at[zl], where))
    for copy in copies:
        copy.start()
    for k, (dx, dt, fx, to, back) in enumerate(near):
        slot = lr.at[2 * back + to]
        remote(slot, slot, l_send.at[k], l_recv.at[k], {"fs": back, "tp": to}).wait_recv()
    for j in range(half):
        where = {"sp": half * t + j, "tp": 1 - zh}
        remote(gr.at[j], gr.at[j], g_send.at[j], g_recv.at[j], where).wait_recv()
        remote(dr.at[j], dr.at[j], d_send.at[j], d_recv.at[j], where).wait_recv()
    own.wait()
    for copy in copies:
        copy.wait_send()


def spread(nz, nx, blocks, gates, latents):
    half = nz // 2
    dma = pltpu.SemaphoreType.DMA
    near = 2 * nx - 1
    return pl.pallas_call(
        functools.partial(spread_kernel, nz, nx),
        out_shape=(
            jax.ShapeDtypeStruct((half, *blocks.shape[1:]), BF16),
            jax.ShapeDtypeStruct((half, *gates.shape[1:]), F32),
            jax.ShapeDtypeStruct((2 * nx, *latents.shape[1:]), BF16),
        ),
        in_specs=[pl.BlockSpec(memory_space=VM)] * 3,
        out_specs=(pl.BlockSpec(memory_space=VM),) * 3,
        scratch_shapes=[
            dma((1,)),
            dma((half,)),
            dma((half,)),
            dma((half,)),
            dma((half,)),
            dma((near,)),
            dma((near,)),
        ],
        compiler_params=pltpu.CompilerParams(collective_id=2, has_side_effects=True),
        name="spread",
    )(blocks, gates, latents)


def unit(values):
    return values * lax.rsqrt(jnp.sum(values * values, axis=-1, keepdims=True) + NORM_EPS)


def swish(values):
    return values * (1.0 / (1.0 + jnp.exp(-values)))


def delta_kernel(
    nz, nx, raw_ref, gate_ref, gain_ref, out_ref, state_out, state_in, ready,
    st_send, st_recv, h_send, h_recv,
):
    z, x, t = lax.axis_index("sp"), lax.axis_index("fs"), lax.axis_index("tp")
    half = nz // 2
    zh, zl = z // half, lax.rem(z, half)
    lane_t = 1 - zh
    sources = [
        {"fs": xl, "sp": 2 * x + sl + half * (1 - t), "tp": zh} for sl in range(2) for xl in range(nx)
    ]
    greet(sources + [{"tp": 1 - t}], half + 1)

    size = 2 * BLOCK
    row = lax.broadcasted_iota(jnp.int32, (size, size), 0)
    col = lax.broadcasted_iota(jnp.int32, (size, size), 1)
    eye = row == col
    same = (row // BLOCK) == (col // BLOCK)
    strict = same & (row > col)
    causal = same & (row >= col)
    wide_row = lax.broadcasted_iota(jnp.int32, (size, 2 * size), 0)

    def upright(line, where):
        return jnp.sum(jnp.where(where, line, 0.0), axis=1, keepdims=True)

    kept = []
    for p in range(half // 2):
        block = raw_ref[2 * p : 2 * p + 2].reshape(size, 3 * HEAD).astype(F32)
        q = unit(swish(block[:, :HEAD])) * HEAD**-0.5
        k = unit(swish(block[:, HEAD : 2 * HEAD]))
        v = swish(block[:, 2 * HEAD :])
        lines = gate_ref[2 * p] + gate_ref[2 * p + 1]
        beta_row, gate_row = lines[0:1], lines[1:2]
        beta, gate = upright(beta_row, eye), upright(gate_row, eye)
        last = upright(gate_row, col == (row // BLOCK) * BLOCK + BLOCK - 1)
        decay = jnp.exp(jnp.where(causal, gate - gate_row, 0.0))
        lower = jnp.where(strict, beta * mm_nt(k, k) * decay, 0.0)
        scores = jnp.where(causal, mm_nt(q, k) * decay, 0.0)
        inverse = jnp.where(eye, 1.0, 0.0) - jnp.where((row // 2 == col // 2), lower, 0.0)
        width = 2
        while width < BLOCK:
            pick = (row // (2 * width) == col // (2 * width)) & (row // width != col // width)
            inverse = inverse - mm(mm(inverse, jnp.where(pick, lower, 0.0)), inverse)
            width *= 2
        both = mm(inverse, jnp.concatenate([beta * v, beta * k * jnp.exp(gate)], axis=1))
        key_t = (k * jnp.exp(last - gate)).T
        moves = [
            mm(key_t, jnp.where(wide_row // BLOCK == h, both, 0.0)) for h in range(2)
        ]
        factors = [jnp.exp(last[h * BLOCK : h * BLOCK + 1]) for h in range(2)]
        kept.append((q * jnp.exp(gate), scores, both, moves, factors))

    total = jnp.concatenate([jnp.zeros((size, size), F32), jnp.where(eye, 1.0, 0.0)], axis=1)
    states = []
    for j in range(half):
        states.append(total)
        move, factor = kept[j // 2][3][j % 2], kept[j // 2][4][j % 2]
        grown = factor * total - mm(move[:, size:], total)
        total = jnp.concatenate([grown[:, :size] + move[:, :size], grown[:, size:]], axis=1)

    state_out[...] = total[:, :size]
    crossing = remote(state_out, state_in, st_send.at[0], st_recv.at[0], {"tp": 1 - t})

    @pl.when(t == 0)
    def _():
        state_in[...] = jnp.zeros_like(state_in)
        crossing.start()

    @pl.when(t == 1)
    def _():
        crossing.wait_recv()

    start = state_in[...]
    for p in range(half // 2):
        queries, scores, both, _, _ = kept[p]
        read, fixed = [], []
        for h in range(2):
            j = 2 * p + h
            state = states[j][:, :size] + mm(states[j][:, size:], start)
            span = slice(h * BLOCK, (h + 1) * BLOCK)
            got = mm(jnp.concatenate([both[span, size:], queries[span]], axis=0), state)
            fixed.append(both[span, :size] - got[:BLOCK])
            read.append(got[BLOCK:])
        raw = jnp.concatenate(read, axis=0) + mm(scores, jnp.concatenate(fixed, axis=0))
        raw = raw * lax.rsqrt(jnp.mean(raw * raw, axis=-1, keepdims=True) + NORM_EPS)
        heads = (raw * gain_ref[...]).astype(BF16)
        ready[2 * p] = heads[:BLOCK]
        ready[2 * p + 1] = heads[BLOCK:]

    home = [
        remote(
            ready.at[j],
            out_ref.at[lax.rem(zl, 2), x],
            h_send.at[j],
            h_recv.at[lax.rem(zl, 2), x],
            {"fs": zl // 2, "sp": half * t + j, "tp": lane_t},
        )
        for j in range(half)
    ]
    for copy in home:
        copy.start()
    for sl in range(2):
        for xl in range(nx):
            slot = out_ref.at[sl, xl]
            where = {"fs": xl, "sp": 2 * x + sl + half * (1 - t), "tp": zh}
            remote(slot, slot, h_send.at[0], h_recv.at[sl, xl], where).wait_recv()
    for copy in home:
        copy.wait_send()

    @pl.when(t == 0)
    def _():
        crossing.wait_send()


def delta(nz, nx, raw, gates, gain):
    half = nz // 2
    dma = pltpu.SemaphoreType.DMA
    return pl.pallas_call(
        functools.partial(delta_kernel, nz, nx),
        out_shape=jax.ShapeDtypeStruct((2, nx, BLOCK, HEAD), BF16),
        in_specs=[pl.BlockSpec(memory_space=VM)] * 3,
        out_specs=pl.BlockSpec(memory_space=VM),
        scratch_shapes=[
            VM((HEAD, HEAD), F32),
            VM((HEAD, HEAD), F32),
            VM((half, BLOCK, HEAD), BF16),
            dma((1,)),
            dma((1,)),
            dma((half,)),
            dma((2, nx)),
        ],
        compiler_params=pltpu.CompilerParams(collective_id=3, has_side_effects=True),
        name="delta",
    )(raw, gates, gain)


def sent_together(arrays, axis, dim, along):
    widths = [a.shape[along] for a in arrays]
    both = jnp.concatenate(arrays, axis=along)
    filled = lax.all_gather(both, axis, axis=dim, tiled=True)
    return tuple(jnp.split(filled, [sum(widths[:k]) for k in range(1, len(widths))], axis=along))


def gather_axes(array, axes, dim):
    if not axes:
        return array
    nearer = lax.all_gather(array, axes[-1], axis=dim, tiled=True)
    return gather_axes(nearer, axes[:-1], dim)


def copy_for_each(array, axis):
    devices = lax.axis_size(axis)
    return lax.all_to_all(
        jnp.broadcast_to(array[None], (devices, *array.shape)), axis, 0, 0, tiled=True
    )


def taken_together(array, axis):
    return copy_for_each(array, axis).astype(jnp.float32).sum(axis=0)


def stored(values):
    return lax.optimization_barrier(values.astype(jnp.bfloat16))


def rms_scale(values):
    return lax.rsqrt(jnp.mean(values * values, axis=-1, keepdims=True) + NORM_EPS)


def rope_tables(positions, rope_width):
    frequency = ROPE_THETA ** (-jnp.arange(0, rope_width, 2, dtype=jnp.float32) / rope_width)
    angles = positions.astype(jnp.float32)[:, None] * frequency[None, :]
    return (jnp.cos(angles), jnp.sin(angles))


def rotate(values, cosine_table, sine_table):
    lower_half, upper_half = jnp.split(values, 2, axis=-1)
    return jnp.concatenate(
        [
            lower_half * cosine_table - upper_half * sine_table,
            upper_half * cosine_table + lower_half * sine_table,
        ],
        axis=-1,
    )


def keep_same(current):
    return current


def local(
    tokens,
    pre_gain,
    query_weight,
    key_weight,
    value_weight,
    beta_weight,
    decay_weight,
    decay_rate,
    delta_gain,
    query_down,
    latent_down,
    rope_weight,
    query_gain,
    latent_gain,
    query_up,
    latent_up,
    delta_out,
    latent_out,
    post_gain,
):
    f32 = jnp.float32
    seq_count, token_count = (tokens.shape[0], tokens.shape[1])
    row_total = seq_count * token_count
    sequence = tokens.reshape(row_total, tokens.shape[2]).astype(f32)
    query_start = lax.axis_index("sp") * token_count
    positions = query_start + jnp.arange(token_count)
    normed = (sequence * rms_scale(sequence) * pre_gain).astype(jnp.bfloat16)
    head_group = lax.axis_index("tp")
    nz, nx = lax.axis_size("sp"), lax.axis_size("fs")
    z, x = lax.axis_index("sp"), lax.axis_index("fs")
    row_span = query_weight.shape[0]
    row_start = (z * nx + x) * row_span

    def own_rows(array):
        return lax.dynamic_slice_in_dim(array, row_start, row_span, 0)

    def for_cores(array):
        parts = array.reshape(row_span, nx, 2, -1)
        return lax.dynamic_index_in_dim(parts, head_group, 2, False)

    def for_heads(array):
        parts = array.reshape(row_span, 2, nx, -1)
        return lax.dynamic_index_in_dim(parts, head_group, 1, False)

    q_width = query_down.shape[1] // (2 * nx)
    kv_width = latent_down.shape[1] // (2 * nx)
    rope_width = rope_weight.shape[1] // (2 * nx)
    side = jnp.concatenate(
        [
            for_cores(query_down),
            for_cores(latent_down),
            for_cores(own_rows(rope_weight)),
            for_heads(own_rows(beta_weight)),
            for_heads(own_rows(decay_weight)),
        ],
        axis=-1,
    )
    at_beta = q_width + kv_width + rope_width
    side = jnp.pad(side, ((0, 0), (0, 0), (0, LANES - side.shape[-1])))
    packed = jnp.concatenate(
        [w.reshape(row_span, nx, HEAD) for w in (query_weight, key_weight, value_weight)] + [side],
        axis=-1,
    )
    packed = jnp.moveaxis(packed, 1, 0)
    projected = project(nz, nx, normed.reshape(seq_count, token_count, -1), packed)
    lanes = nx * seq_count
    blocks = projected[:, : 3 * HEAD].astype(jnp.bfloat16).reshape(lanes, token_count, 3 * HEAD)
    latents = projected[:, 3 * HEAD :].astype(jnp.bfloat16).reshape(nx, row_total, LANES)
    at_beta += 3 * HEAD
    beta_gate = jax.nn.sigmoid(projected[:, at_beta]).reshape(lanes, token_count)
    own_rate = lax.dynamic_index_in_dim(decay_rate, head_group * nx + x, 0, False)
    log_decay = -own_rate * jax.nn.softplus(projected[:, at_beta + 1]).reshape(lanes, token_count)
    gate_sum = jnp.cumsum(log_decay, axis=-1)
    lines = jnp.stack([beta_gate, gate_sum], axis=1)
    empty = jnp.zeros_like(lines)
    odd = lax.rem(z, 2) == 1
    lines = jnp.concatenate([jnp.where(odd, empty, lines), jnp.where(odd, lines, empty)], axis=-1)
    lines = jnp.pad(lines, ((0, 0), (0, 6), (0, 0)))
    blocks_in, lines_in, latents_in = spread(nz, nx, blocks, lines, latents)
    homed = delta(nz, nx, blocks_in, lines_in, delta_gain.reshape(1, HEAD))
    delta_heads = jnp.transpose(homed, (0, 2, 1, 3)).reshape(row_total, nx * HEAD)

    def joined(start, width):
        return jnp.moveaxis(latents_in[:, :, start : start + width], 0, 1).reshape(row_total, -1)

    q_latent = joined(0, q_width)
    kv_latent = joined(q_width, kv_width)
    rope_raw = joined(q_width + kv_width, rope_width)
    q_lat32 = q_latent.astype(f32)
    kv_lat32 = kv_latent.astype(f32)
    q_normed = (q_lat32 * rms_scale(q_lat32) * query_gain).astype(jnp.bfloat16)
    kv_normed = (kv_lat32 * rms_scale(kv_lat32) * latent_gain).astype(jnp.bfloat16)
    cosine_table, sine_table = rope_tables(positions, rope_raw.shape[1])
    rope_keys = rotate(
        rope_raw.astype(f32).reshape(seq_count, token_count, rope_raw.shape[1]),
        cosine_table,
        sine_table,
    ).astype(jnp.bfloat16)
    latent_count = query_up.shape[1] // (NOPE + ROPE)
    query_all = stored(jnp.dot(q_normed, query_up, preferred_element_type=f32)).reshape(
        seq_count, token_count, latent_count, NOPE + ROPE
    )
    query_plain = query_all[..., :NOPE]
    query_turned = rotate(
        query_all[..., NOPE:].astype(f32), cosine_table[:, None, :], sine_table[:, None, :]
    ).astype(jnp.bfloat16)
    score_scale = (NOPE + ROPE) ** (-0.5)
    query_block = positions // BLOCK
    kv_seq = kv_normed.reshape(seq_count, token_count, kv_normed.shape[1])

    def attend_block(totals, key_plain, value_rows, rope_rows, key_start):
        row_max, row_sum, weighted = totals
        key_block = (key_start + jnp.arange(key_plain.shape[1])) // BLOCK
        allowed = key_block[None, :] <= query_block[:, None]
        logits = (
            jnp.einsum("sqhd,skhd->shqk", query_plain, key_plain, preferred_element_type=f32)
            + jnp.einsum("sqhd,skd->shqk", query_turned, rope_rows, preferred_element_type=f32)
        ) * score_scale
        logits = jnp.where(allowed[None, None], logits, -jnp.inf)
        new_max = jnp.maximum(row_max, jnp.max(logits, axis=-1))
        shift = jnp.where(jnp.isfinite(new_max), new_max, 0.0)
        weights = jnp.where(allowed[None, None], jnp.exp(logits - shift[..., None]), 0.0)
        rescale = jnp.exp(row_max - shift)
        row_sum = row_sum * rescale + jnp.sum(weights, axis=-1)
        weighted = weighted * rescale[..., None] + jnp.einsum(
            "shqk,skhd->shqd", weights.astype(jnp.bfloat16), value_rows, preferred_element_type=f32
        )
        return (new_max, row_sum, weighted)

    start_stats = (
        jnp.full((seq_count, latent_count, token_count), -jnp.inf, f32),
        jnp.zeros((seq_count, latent_count, token_count), f32),
        jnp.zeros((seq_count, latent_count, token_count, VDIM), f32),
    )

    def expand_latent(portion, row_start, span_rows):
        latent_rows = lax.dynamic_slice_in_dim(portion[0], row_start, span_rows, 1)
        expanded = jnp.dot(
            latent_rows.reshape(seq_count * span_rows, latent_rows.shape[2]),
            latent_up,
            preferred_element_type=f32,
        ).astype(jnp.bfloat16)
        expanded = expanded.reshape(seq_count, span_rows, latent_count, NOPE + VDIM)
        return (
            expanded[..., :NOPE],
            expanded[..., NOPE:],
            lax.dynamic_slice_in_dim(portion[1], row_start, span_rows, 1),
        )

    portion = sent_together((kv_seq, rope_keys), "sp", 1, 2)
    row_count = portion[0].shape[1]
    span_rows = math.gcd(row_count, token_count * max(1, 512 // token_count))

    def visit_rows(current):

        def visit_block(block_index, stats):
            row_start = block_index * span_rows
            key_plain, value_rows, rope_rows = expand_latent(portion, row_start, span_rows)
            return attend_block(stats, key_plain, value_rows, rope_rows, row_start)

        return lax.fori_loop(0, row_count // span_rows, visit_block, current)

    row_max, row_sum, weighted = lax.cond(
        jnp.int32(0) < query_start + token_count, visit_rows, keep_same, start_stats
    )
    latent_heads = (
        jnp.transpose(weighted / row_sum[..., None], (0, 2, 1, 3))
        .reshape(row_total, latent_count * VDIM)
        .astype(jnp.bfloat16)
    )
    heads_joined = jnp.concatenate([delta_heads, latent_heads], axis=1)
    out_rows = jnp.concatenate([delta_out, latent_out], axis=0)
    partial_value = jnp.dot(
        heads_joined, gather_axes(out_rows, ("sp", "fs"), 1), preferred_element_type=f32
    )
    whole_rows = taken_together(partial_value.astype(jnp.bfloat16), "tp").astype(jnp.float32)
    row_scale = rms_scale(whole_rows)
    half_width = post_gain.shape[0]
    own_half = lax.dynamic_slice_in_dim(whole_rows, head_group * half_width, half_width, 1)
    result = own_half * row_scale * post_gain
    return result.astype(jnp.bfloat16).reshape(seq_count, token_count, result.shape[1])


def solution(mesh):
    return jax.shard_map(
        local,
        mesh=mesh,
        in_specs=(
            P(("grp", "fs"), "sp", None),
            P(),
            P(("sp", "fs"), "tp"),
            P(("sp", "fs"), "tp"),
            P(("sp", "fs"), "tp"),
            P(),
            P(),
            P(),
            P(),
            P(("sp", "fs"), None),
            P(("sp", "fs"), None),
            P(),
            P(),
            P(),
            P(None, "tp"),
            P(None, "tp"),
            P("tp", ("sp", "fs")),
            P("tp", ("sp", "fs")),
            P("tp"),
        ),
        out_specs=P(("grp", "fs"), "sp", "tp"),
        check_vma=False,
    )
```

```python
import functools
import math

import jax
import jax.numpy as jnp
from jax import lax
from jax.experimental import pallas as pl
from jax.experimental.pallas import tpu as pltpu
from jax.sharding import PartitionSpec as P

HEAD = 128
NOPE = 64
ROPE = 32
VDIM = 64
BLOCK = 64
LANES = 128

NORM_EPS = 1e-06
ROPE_THETA = 10000.0
F32 = jnp.float32
BF16 = jnp.bfloat16
MESH = pl.DeviceIdType.MESH
VM = pltpu.VMEM


def remote(src, dst, send_sem, recv_sem, where):
    return pltpu.make_async_remote_copy(
        src_ref=src,
        dst_ref=dst,
        send_sem=send_sem,
        recv_sem=recv_sem,
        device_id=where,
        device_id_type=MESH,
    )


def greet(places, count):
    barrier = pltpu.get_barrier_semaphore()
    for place in places:
        pl.semaphore_signal(barrier, inc=1, device_id=place, device_id_type=MESH)
    pl.semaphore_wait(barrier, count)


def mm(left, right):
    return lax.dot_general(
        left.astype(BF16), right.astype(BF16), (((1,), (0,)), ((), ())), preferred_element_type=F32
    )


def mm_nt(left, right):
    return lax.dot_general(
        left.astype(BF16), right.astype(BF16), (((1,), (1,)), ((), ())), preferred_element_type=F32
    )


def project_kernel(
    nz, nx, tok_ref, wp_ref, wt_ref, out_ref, wz_ref, toks, ws,
    loc_sem, tok_send, tok_recv, fwd_send, fwd_recv, wx_send, wx_recv, r_send, r_recv, l_send, l_recv,
):
    z, x, t = lax.axis_index("sp"), lax.axis_index("fs"), lax.axis_index("tp")
    rows = wp_ref.shape[1]
    right, left = {"sp": lax.rem(z + 1, nz)}, {"sp": lax.rem(z + nz - 1, nz)}
    partner = {"tp": 1 - t}
    others = [lax.rem(x + d, nx) for d in range(1, nx)]
    greet([{"fs": o} for o in others] + [right, left, partner], nx + 2)

    def chunk(slot, part):
        if part is None:
            return wz_ref.at[slot]
        return ws.at[slot, pl.ds(part * rows, rows)]

    def mark(part):
        return nx if part is None else part

    own_w = pltpu.make_async_copy(wp_ref.at[x], chunk(z, x), loc_sem.at[0])
    own_w.start()
    wx = [
        remote(wp_ref.at[o], chunk(z, x), wx_send.at[d], wx_recv.at[d], {"fs": o})
        for d, o in enumerate(others)
    ]
    for copy in wx:
        copy.start()
    own_o = pltpu.make_async_copy(wt_ref, wz_ref.at[z], loc_sem.at[2])
    own_o.start()
    own_t = pltpu.make_async_copy(tok_ref, toks.at[pl.ds(2 * x, 2)], loc_sem.at[1])
    own_t.start()
    tok = [
        remote(tok_ref.at[t], toks.at[2 * x + t], tok_send.at[d], tok_recv.at[d], {"fs": o})
        for d, o in enumerate(others)
    ]
    for copy in tok:
        copy.start()

    reach_r, reach_l = nz // 2, nz // 2 - 1

    def go_right(step, part, slot):
        return remote(
            chunk(slot, part), chunk(slot, part), r_send.at[step, mark(part)], r_recv.at[step, mark(part)], right
        )

    def go_left(step, part, slot):
        return remote(
            chunk(slot, part), chunk(slot, part), l_send.at[step, mark(part)], l_recv.at[step, mark(part)], left
        )

    for d in range(nx):
        part = lax.rem(x + nx - d, nx)
        if d == 0:
            own_w.wait()
        else:
            wx[d - 1].wait_recv()
        go_right(0, part, z).start()
        go_left(0, part, z).start()
    own_o.wait()
    go_right(0, None, z).start()
    go_left(0, None, z).start()

    def ring(step, carry):
        from_left = lax.rem(z + 2 * nz - 1 - step, nz)
        from_right = lax.rem(z + 1 + step, nz)
        for d in range(nx + 1):
            part = lax.rem(x + nx - d, nx) if d < nx else None
            go_right(step, part, from_left).wait_recv()

            @pl.when(step < reach_r - 1)
            def _():
                go_right(step + 1, part, from_left).start()

            @pl.when(step < reach_l)
            def _():
                go_left(step, part, from_right).wait_recv()

            @pl.when(step < reach_l - 1)
            def _():
                go_left(step + 1, part, from_right).start()

        return carry

    lax.fori_loop(0, reach_r, ring, 0)

    own_t.wait()
    fwd = []
    for d in range(nx - 1):
        source = lax.rem(x + nx - 1 - d, nx)
        tok[d].wait_recv()
        copy = remote(
            toks.at[2 * source + t], toks.at[2 * source + t], fwd_send.at[d], fwd_recv.at[d], partner
        )
        copy.start()
        fwd.append(copy)
    for copy in fwd:
        copy.wait_recv()

    depth = ws.shape[0] * ws.shape[1]
    weight = ws[...].reshape(depth, ws.shape[2])
    pair = 2 * toks.shape[1]

    def tile(i, carry):
        lhs = toks[pl.ds(2 * i, 2)].reshape(pair, depth)
        out_ref[pl.ds(pl.multiple_of(i * pair, pair), pair), :] = lax.dot_general(
            lhs, weight, (((1,), (0,)), ((), ())), preferred_element_type=F32
        )
        return carry

    lax.fori_loop(0, nx, tile, 0)

    for copy in wx + tok + fwd:
        copy.wait_send()

    def drain(step, carry):
        for part in [*range(nx), None]:
            go_right(step, part, z).wait_send()

            @pl.when(step < reach_l)
            def _():
                go_left(step, part, z).wait_send()

        return carry

    lax.fori_loop(0, reach_r, drain, 0)


def project(nz, nx, normed, packed, out_cols):
    seqs, length, width = normed.shape
    rows, cols = packed.shape[1:]
    dma = pltpu.SemaphoreType.DMA
    return pl.pallas_call(
        functools.partial(project_kernel, nz, nx),
        out_shape=(
            jax.ShapeDtypeStruct((seqs * nx * length, cols), F32),
            jax.ShapeDtypeStruct((nz, *out_cols.shape), BF16),
        ),
        in_specs=[pl.BlockSpec(memory_space=VM)] * 3,
        out_specs=(pl.BlockSpec(memory_space=VM),) * 2,
        scratch_shapes=[
            VM((seqs * nx, length, width), BF16),
            VM((nz, nx * rows, cols), BF16),
            dma((3,)),
            dma((nx - 1,)),
            dma((nx - 1,)),
            dma((nx - 1,)),
            dma((nx - 1,)),
            dma((nx - 1,)),
            dma((nx - 1,)),
            dma((nz // 2, nx + 1)),
            dma((nz // 2, nx + 1)),
            dma((nz // 2 - 1, nx + 1)),
            dma((nz // 2 - 1, nx + 1)),
        ],
        compiler_params=pltpu.CompilerParams(collective_id=1, has_side_effects=True),
        name="project",
    )(normed, packed, out_cols)


def unit(values):
    return values * lax.rsqrt(jnp.sum(values * values, axis=-1, keepdims=True) + NORM_EPS)


def swish(values):
    return values * (1.0 / (1.0 + jnp.exp(-values)))


def mix_kernel(
    nz, nx, d_ref, g_ref, l_ref, wz_ref, qup_ref, qgain_ref, kvgain_ref, wuk_ref, wuv_ref,
    cos_ref, sin_ref, dgain_ref, pgain_ref, out_ref,
    dr, gr, lr, kvg, wo, homed, ready, state_out, state_in, part_out, part_in,
    loc_sem, a_send, a_recv, d_send, d_recv, g_send, g_recv, kr_send, kr_recv, kl_send, kl_recv,
    kp_send, kp_recv, w_send, w_recv, st_send, st_recv, h_send, h_recv, p_send, p_recv,
):
    z, x, t = lax.axis_index("sp"), lax.axis_index("fs"), lax.axis_index("tp")
    half = nz // 2
    zh, zl = z // half, lax.rem(z, half)
    lane_t = 1 - zh
    partner = {"tp": 1 - t}
    near = [
        (dx, dt, lax.rem(x + dx, nx), lax.rem(t + dt, 2), lax.rem(x + nx - dx, nx))
        for dx in range(nx)
        for dt in range(2)
        if dx or dt
    ]
    right, left = {"sp": lax.rem(z + 1, nz)}, {"sp": lax.rem(z + nz - 1, nz)}
    east, west = {"fs": lax.rem(x + 1, nx)}, {"fs": lax.rem(x + nx - 1, nx)}
    sources = [{"fs": back, "tp": to} for dx, dt, fx, to, back in near]
    sources += [right, left]
    sources += [{"sp": half * t + j, "tp": 1 - zh} for j in range(half)]
    sources += [
        {"fs": xl, "sp": 2 * x + sl + half * (1 - t), "tp": zh} for sl in range(2) for xl in range(nx)
    ]
    greet(sources, len(sources))
    started = []

    def begin(copy):
        copy.start()
        started.append(copy)
        return copy

    own_l = pltpu.make_async_copy(l_ref.at[x], lr.at[2 * x + t], loc_sem.at[0])
    own_l.start()
    for k, (dx, dt, fx, to, back) in enumerate(near):
        begin(
            remote(l_ref.at[fx], lr.at[2 * x + t], a_send.at[k], a_recv.at[k], {"fs": fx, "tp": to})
        )

    def send_lane(s):
        where = {"sp": s + half * (1 - t), "tp": zh}
        begin(remote(g_ref.at[s], gr.at[zl], g_send.at[s], g_recv.at[zl], where))
        begin(remote(d_ref.at[s], dr.at[zl], d_send.at[s], d_recv.at[zl], where))

    send_lane(0)
    send_lane(1)

    def w_part(owner, upper):
        return wo.at[pl.ds(half * upper, half), owner]

    own_w = pltpu.make_async_copy(wz_ref, wo.at[:, x], loc_sem.at[1])
    own_w.start()
    for upper, where, k in ((0, east, 0), (1, west, 1), (1, east, 2), (0, west, 3)):
        begin(
            remote(
                wz_ref.at[pl.ds(half * upper, half)], w_part(x, upper), w_send.at[k], w_recv.at[k], where
            )
        )

    for k, (dx, dt, fx, to, back) in enumerate(near):
        slot = lr.at[2 * back + to]
        remote(slot, slot, a_send.at[k], a_recv.at[k], {"fs": back, "tp": to}).wait_recv()
    own_l.wait()

    cores = 2 * nx
    rows = lr.shape[1]
    count = rows // BLOCK
    lane = lax.broadcasted_iota(jnp.int32, (rows, LANES), 1)
    q_width, kv_width = qup_ref.shape[0] // cores // 2, wuv_ref.shape[1] // cores
    at_rope = q_width + kv_width
    rope_width = ROPE // cores
    parts = [lr[c].astype(F32) for c in range(cores)]
    q_square = sum(jnp.where(lane < q_width, part * part, 0.0) for part in parts)
    kv_square = sum(
        jnp.where((lane >= q_width) & (lane < at_rope), part * part, 0.0) for part in parts
    )
    q_scale = lax.rsqrt(jnp.sum(q_square, axis=-1, keepdims=True) / (q_width * cores) + NORM_EPS)
    kv_scale = lax.rsqrt(jnp.sum(kv_square, axis=-1, keepdims=True) / (kv_width * cores) + NORM_EPS)
    from_lane = lax.broadcasted_iota(jnp.int32, (LANES, 4 * LANES), 0)
    to_lane = lax.broadcasted_iota(jnp.int32, (LANES, 4 * LANES), 1)
    kv_total = kv_width * cores
    slab = jnp.zeros((rows, 4 * LANES), F32)
    for c in range(cores):
        kept = jnp.where(lane < at_rope, parts[c] * kv_scale * kvgain_ref[c], parts[c])
        is_kv = (from_lane >= q_width) & (from_lane < at_rope)
        is_rope = (from_lane >= at_rope) & (from_lane < at_rope + rope_width)
        entry = from_lane - at_rope + rope_width * c
        spot = to_lane - kv_total
        place = jnp.where(
            is_kv & (to_lane == from_lane - q_width + kv_width * c), 1.0, 0.0
        )
        spot_in = spot % ROPE
        straight = is_rope & (spot >= 0) & (spot < LANES) & (spot_in == entry)
        swapped = is_rope & (spot >= LANES) & ((spot_in + ROPE // 2) % ROPE == entry)
        sign = jnp.where(spot_in < ROPE // 2, -1.0, 1.0)
        place = place + jnp.where(straight, 1.0, 0.0) + jnp.where(swapped, sign, 0.0)
        slab = slab + mm(kept, place)
    turned = slab[:, kv_total : kv_total + LANES].astype(BF16).astype(F32) * cos_ref[...]
    turned = turned + slab[:, kv_total + LANES :].astype(BF16).astype(F32) * sin_ref[...]
    keys = jnp.concatenate([slab[:, :kv_total], turned], axis=1).astype(BF16)
    for s in range(count):
        kvg[s, z] = keys[s * BLOCK : (s + 1) * BLOCK]

    def go_right(step, slot):
        return remote(kvg.at[t, slot], kvg.at[t, slot], kr_send.at[step], kr_recv.at[step], right)

    def go_left(step, slot):
        return remote(kvg.at[t, slot], kvg.at[t, slot], kl_send.at[step], kl_recv.at[step], left)

    def across(slot, k):
        return remote(kvg.at[t, slot], kvg.at[t, slot], kp_send.at[k], kp_recv.at[k], partner)

    begin(go_right(0, z))
    begin(go_left(0, z))

    q_rows = jnp.concatenate(
        [(parts[c] * q_scale * qgain_ref[c]).astype(BF16) for c in range(cores)], axis=1
    )
    query = mm(q_rows, qup_ref[...]).astype(BF16)
    heads = wuv_ref.shape[0]
    plain_width = heads * NOPE
    turn_width = heads * ROPE
    stacked = [[] for _ in range(count)]
    for h in range(heads):
        base = (h // 2) * LANES
        mine = (lane // NOPE) == h % 2
        plain = jnp.where(mine, query[:, base : base + LANES].astype(F32), 0.0)
        absorbed = mm(plain, wuk_ref[h // 2]).astype(BF16)
        base = plain_width + (h * ROPE // LANES) * LANES
        raw = query[:, base : base + LANES].astype(F32)
        swap = query[:, base + turn_width : base + turn_width + LANES].astype(F32)
        turn = raw * cos_ref[...] + swap * sin_ref[...]
        turn = jnp.where((lane // ROPE) == h % (LANES // ROPE), turn, 0.0).astype(BF16)
        joined = jnp.concatenate([absorbed, turn], axis=1)
        for s in range(count):
            stacked[s].append(joined[s * BLOCK : (s + 1) * BLOCK])

    reach_r, reach_l = nz // 2, nz // 2 - 1
    for step in range(reach_r):
        if step + 2 < half:
            send_lane(step + 2)
        from_left = lax.rem(z + 2 * nz - 1 - step, nz)
        from_right = lax.rem(z + 1 + step, nz)
        go_right(step, from_left).wait_recv()
        if step < reach_r - 1:
            begin(go_right(step + 1, from_left))
        begin(across(from_left, step))
        if step < reach_l:
            go_left(step, from_right).wait_recv()
            if step < reach_l - 1:
                begin(go_left(step + 1, from_right))
            begin(across(from_right, reach_r + step))

    remote(w_part(x, 0), w_part(x, 0), w_send.at[0], w_recv.at[0], west).wait_recv()
    begin(
        remote(w_part(lax.rem(x + nx - 1, nx), 0), w_part(lax.rem(x + nx - 1, nx), 0),
               w_send.at[4], w_recv.at[4], east)
    )
    remote(w_part(x, 1), w_part(x, 1), w_send.at[1], w_recv.at[1], east).wait_recv()
    begin(
        remote(w_part(lax.rem(x + 1, nx), 1), w_part(lax.rem(x + 1, nx), 1),
               w_send.at[5], w_recv.at[5], west)
    )

    for j in range(half):
        where = {"sp": half * t + j, "tp": 1 - zh}
        remote(gr.at[j], gr.at[j], g_send.at[j], g_recv.at[j], where).wait_recv()
        remote(dr.at[j], dr.at[j], d_send.at[j], d_recv.at[j], where).wait_recv()

    size = 2 * BLOCK
    row = lax.broadcasted_iota(jnp.int32, (size, size), 0)
    col = lax.broadcasted_iota(jnp.int32, (size, size), 1)
    eye = row == col
    same = (row // BLOCK) == (col // BLOCK)
    strict = same & (row > col)
    causal = same & (row >= col)
    wide_row = lax.broadcasted_iota(jnp.int32, (size, 2 * size), 0)

    def upright(line, where):
        return jnp.sum(jnp.where(where, line, 0.0), axis=1, keepdims=True)

    terms = []
    for p in range(half // 2):
        block = dr[2 * p : 2 * p + 2].reshape(size, 3 * HEAD).astype(F32)
        q = unit(swish(block[:, :HEAD])) * HEAD**-0.5
        k = unit(swish(block[:, HEAD : 2 * HEAD]))
        v = swish(block[:, 2 * HEAD :])
        lines = gr[2 * p] + gr[2 * p + 1]
        beta_row, gate_row = lines[0:1], lines[1:2]
        beta, gate = upright(beta_row, eye), upright(gate_row, eye)
        last = upright(gate_row, col == (row // BLOCK) * BLOCK + BLOCK - 1)
        decay = jnp.exp(jnp.where(causal, gate - gate_row, 0.0))
        lower = jnp.where(strict, beta * mm_nt(k, k) * decay, 0.0)
        scores = jnp.where(causal, mm_nt(q, k) * decay, 0.0)
        inverse = jnp.where(eye, 1.0, 0.0) - jnp.where((row // 2 == col // 2), lower, 0.0)
        width = 2
        while width < BLOCK:
            pick = (row // (2 * width) == col // (2 * width)) & (row // width != col // width)
            inverse = inverse - mm(mm(inverse, jnp.where(pick, lower, 0.0)), inverse)
            width *= 2
        both = mm(inverse, jnp.concatenate([beta * v, beta * k * jnp.exp(gate)], axis=1))
        key_t = (k * jnp.exp(last - gate)).T
        moves = [
            mm(key_t, jnp.where(wide_row // BLOCK == h, both, 0.0)) for h in range(2)
        ]
        factors = [jnp.exp(last[h * BLOCK : h * BLOCK + 1]) for h in range(2)]
        terms.append((q * jnp.exp(gate), scores, both, moves, factors))

    total = jnp.concatenate([jnp.zeros((size, size), F32), jnp.where(eye, 1.0, 0.0)], axis=1)
    states = []
    for j in range(half):
        states.append(total)
        move, factor = terms[j // 2][3][j % 2], terms[j // 2][4][j % 2]
        grown = factor * total - mm(move[:, size:], total)
        total = jnp.concatenate([grown[:, :size] + move[:, :size], grown[:, size:]], axis=1)

    state_out[...] = total[:, :size]
    crossing = remote(state_out, state_in, st_send.at[0], st_recv.at[0], partner)

    @pl.when(t == 0)
    def _():
        state_in[...] = jnp.zeros_like(state_in)
        crossing.start()

    @pl.when(t == 1)
    def _():
        crossing.wait_recv()

    start = state_in[...]
    for p in range(half // 2):
        queries, scores, both, _, _ = terms[p]
        read, fixed = [], []
        for h in range(2):
            j = 2 * p + h
            state = states[j][:, :size] + mm(states[j][:, size:], start)
            span = slice(h * BLOCK, (h + 1) * BLOCK)
            got = mm(jnp.concatenate([both[span, size:], queries[span]], axis=0), state)
            fixed.append(both[span, :size] - got[:BLOCK])
            read.append(got[BLOCK:])
        raw = jnp.concatenate(read, axis=0) + mm(scores, jnp.concatenate(fixed, axis=0))
        raw = raw * lax.rsqrt(jnp.mean(raw * raw, axis=-1, keepdims=True) + NORM_EPS)
        done = (raw * dgain_ref[...]).astype(BF16)
        ready[2 * p] = done[:BLOCK]
        ready[2 * p + 1] = done[BLOCK:]

    for j in range(half):
        begin(
            remote(
                ready.at[j],
                homed.at[lax.rem(zl, 2), x],
                h_send.at[j],
                h_recv.at[lax.rem(zl, 2), x],
                {"fs": zl // 2, "sp": half * t + j, "tp": lane_t},
            )
        )

    for k in range(nz - 1):
        slot = kvg.at[1 - t, lax.rem(z + 1, nz)]
        remote(slot, slot, kp_send.at[k], kp_recv.at[k], partner).wait_recv()
    allowed = lax.broadcasted_iota(jnp.int32, (1, nz * BLOCK), 1) < (z + 1) * BLOCK
    outs = []
    for s in range(count):
        keys = kvg[s].reshape(nz * BLOCK, kvg.shape[3])
        scores = mm_nt(jnp.concatenate(stacked[s], axis=0), keys) * (NOPE + ROPE) ** (-0.5)
        scores = jnp.where(allowed, scores, -1e30)
        peak = jnp.max(scores, axis=-1, keepdims=True)
        weights = jnp.where(allowed, jnp.exp(scores - peak), 0.0)
        total = jnp.sum(weights, axis=-1, keepdims=True)
        mixed = (mm(weights, keys[:, :kv_total]) / total).astype(BF16)
        pairs = []
        for p in range(heads // 2):
            upper = mm(mixed[2 * p * BLOCK : (2 * p + 1) * BLOCK], wuv_ref[2 * p])
            lower_head = mm(mixed[(2 * p + 1) * BLOCK : (2 * p + 2) * BLOCK], wuv_ref[2 * p + 1])
            pairs.append((upper + lower_head).astype(BF16))
        outs.append(jnp.concatenate(pairs, axis=1))
    latent_heads = jnp.concatenate(outs, axis=0)

    own_w.wait()
    for k, owner, upper in (
        (2, lax.rem(x + nx - 1, nx), 1),
        (3, lax.rem(x + 1, nx), 0),
        (4, lax.rem(x + 2, nx), 0),
        (5, lax.rem(x + 2, nx), 1),
    ):
        remote(
            w_part(owner, upper), w_part(owner, upper), w_send.at[k], w_recv.at[k], east
        ).wait_recv()
    for sl in range(2):
        for xl in range(nx):
            slot = homed.at[sl, xl]
            where = {"fs": xl, "sp": 2 * x + sl + half * (1 - t), "tp": zh}
            remote(slot, slot, h_send.at[0], h_recv.at[sl, xl], where).wait_recv()
    delta_heads = [homed[:, xl].reshape(rows, HEAD) for xl in range(nx)]
    joined = jnp.concatenate(delta_heads + [latent_heads], axis=1)
    width = wo.shape[0] * wo.shape[1] * wo.shape[2]
    columns = wo[...].reshape(width, wo.shape[3])
    part_out[...] = mm_nt(joined, columns).astype(BF16)
    swap_parts = begin(remote(part_out, part_in, p_send.at[0], p_recv.at[0], partner))
    swap_parts.wait_recv()
    whole = part_out[...].astype(F32) + part_in[...].astype(F32)
    scale = lax.rsqrt(jnp.mean(whole * whole, axis=-1, keepdims=True) + NORM_EPS)
    own_half = jnp.where(t == 0, whole[:, : width // 2], whole[:, width // 2 :])
    out_ref[...] = (own_half * scale * pgain_ref[...]).astype(BF16)

    for copy in started:
        copy.wait_send()

    @pl.when(t == 0)
    def _():
        crossing.wait_send()


def mix(nz, nx, *operands):
    blocks, gates, latents, out_cols = operands[:4]
    half = nz // 2
    heads = operands[8].shape[0]
    rows = latents.shape[1]
    slab = operands[8].shape[1] + LANES
    width = nz * nx * out_cols.shape[1]
    dma = pltpu.SemaphoreType.DMA
    one = lambda count: [dma((count,)), dma((count,))]
    return pl.pallas_call(
        functools.partial(mix_kernel, nz, nx),
        out_shape=jax.ShapeDtypeStruct((rows, width // 2), BF16),
        in_specs=[pl.BlockSpec(memory_space=VM)] * len(operands),
        out_specs=pl.BlockSpec(memory_space=VM),
        scratch_shapes=[
            VM((half, *blocks.shape[1:]), BF16),
            VM((half, *gates.shape[1:]), F32),
            VM((2 * nx, *latents.shape[1:]), BF16),
            VM((rows // BLOCK, nz, BLOCK, slab), BF16),
            VM((nz, nx, *out_cols.shape[1:]), BF16),
            VM((2, nx, BLOCK, HEAD), BF16),
            VM((half, BLOCK, HEAD), BF16),
            VM((HEAD, HEAD), F32),
            VM((HEAD, HEAD), F32),
            VM((rows, width), BF16),
            VM((rows, width), BF16),
            dma((2,)),
            *one(2 * nx - 1),
            *one(half),
            *one(half),
            *one(nz // 2),
            *one(nz // 2 - 1),
            *one(nz - 1),
            *one(6),
            *one(1),
            dma((half,)),
            dma((2, nx)),
            *one(1),
        ],
        compiler_params=pltpu.CompilerParams(collective_id=2, has_side_effects=True),
        name="mix",
    )(*operands)


def rms_scale(values):
    return lax.rsqrt(jnp.mean(values * values, axis=-1, keepdims=True) + NORM_EPS)


def rope_tables(positions, rope_width):
    frequency = ROPE_THETA ** (-jnp.arange(0, rope_width, 2, dtype=jnp.float32) / rope_width)
    angles = positions.astype(jnp.float32)[:, None] * frequency[None, :]
    return (jnp.cos(angles), jnp.sin(angles))


def local(
    tokens,
    pre_gain,
    query_weight,
    key_weight,
    value_weight,
    beta_weight,
    decay_weight,
    decay_rate,
    delta_gain,
    query_down,
    latent_down,
    rope_weight,
    query_gain,
    latent_gain,
    query_up,
    latent_up,
    delta_out,
    latent_out,
    post_gain,
):
    f32 = jnp.float32
    seq_count, token_count = (tokens.shape[0], tokens.shape[1])
    row_total = seq_count * token_count
    sequence = tokens.reshape(row_total, tokens.shape[2]).astype(f32)
    query_start = lax.axis_index("sp") * token_count
    positions = query_start + jnp.arange(token_count)
    normed = (sequence * rms_scale(sequence) * pre_gain).astype(jnp.bfloat16)
    head_group = lax.axis_index("tp")
    nz, nx = lax.axis_size("sp"), lax.axis_size("fs")
    z, x = lax.axis_index("sp"), lax.axis_index("fs")
    row_span = query_weight.shape[0]
    row_start = (z * nx + x) * row_span

    def own_rows(array):
        return lax.dynamic_slice_in_dim(array, row_start, row_span, 0)

    def for_cores(array):
        parts = array.reshape(row_span, nx, 2, -1)
        return lax.dynamic_index_in_dim(parts, head_group, 2, False)

    def for_heads(array):
        parts = array.reshape(row_span, 2, nx, -1)
        return lax.dynamic_index_in_dim(parts, head_group, 1, False)

    q_width = query_down.shape[1] // (2 * nx)
    kv_width = latent_down.shape[1] // (2 * nx)
    rope_width = rope_weight.shape[1] // (2 * nx)
    side = jnp.concatenate(
        [
            for_cores(query_down),
            for_cores(latent_down),
            for_cores(own_rows(rope_weight)),
            for_heads(own_rows(beta_weight)),
            for_heads(own_rows(decay_weight)),
        ],
        axis=-1,
    )
    at_beta = q_width + kv_width + rope_width
    side = jnp.pad(side, ((0, 0), (0, 0), (0, LANES - side.shape[-1])))
    packed = jnp.concatenate(
        [w.reshape(row_span, nx, HEAD) for w in (query_weight, key_weight, value_weight)] + [side],
        axis=-1,
    )
    packed = jnp.moveaxis(packed, 1, 0)
    out_cols = jnp.concatenate([delta_out, latent_out], axis=0).T
    projected, out_slabs = project(
        nz, nx, normed.reshape(seq_count, token_count, -1), packed, out_cols
    )
    lanes = nx * seq_count
    blocks = projected[:, : 3 * HEAD].astype(jnp.bfloat16).reshape(lanes, token_count, 3 * HEAD)
    latents = projected[:, 3 * HEAD :].astype(jnp.bfloat16).reshape(nx, row_total, LANES)
    at_beta += 3 * HEAD
    beta_gate = jax.nn.sigmoid(projected[:, at_beta]).reshape(lanes, token_count)
    own_rate = lax.dynamic_index_in_dim(decay_rate, head_group * nx + x, 0, False)
    log_decay = -own_rate * jax.nn.softplus(projected[:, at_beta + 1]).reshape(lanes, token_count)
    gate_sum = jnp.cumsum(log_decay, axis=-1)
    lines = jnp.stack([beta_gate, gate_sum], axis=1)
    empty = jnp.zeros_like(lines)
    odd = lax.rem(z, 2) == 1
    lines = jnp.concatenate([jnp.where(odd, empty, lines), jnp.where(odd, lines, empty)], axis=-1)
    lines = jnp.pad(lines, ((0, 0), (0, 6), (0, 0)))
    cores = 2 * nx

    def at_lanes(array, start):
        stop = LANES - start - array.shape[1]
        return jnp.pad(array, ((0, 0), (start, stop)) + ((0, 0),) * (array.ndim - 2))

    q_gain = at_lanes(query_gain.reshape(cores, q_width), 0)[:, None, :]
    kv_gain = at_lanes(latent_gain.reshape(cores, kv_width), q_width)[:, None, :]
    up = query_up.reshape(query_up.shape[0], -1, NOPE + ROPE)
    heads = up.shape[1]
    turn = up[..., NOPE:]
    swap = jnp.concatenate([-turn[..., ROPE // 2 :], turn[..., : ROPE // 2]], axis=-1)
    up = jnp.concatenate(
        [u.reshape(u.shape[0], -1) for u in (up[..., :NOPE], turn, swap)], axis=1
    )
    up = at_lanes(up.reshape(cores, q_width, -1), 0).reshape(cores * LANES, -1)
    pairs = latent_up.reshape(latent_up.shape[0], heads, NOPE + VDIM)
    key_up = jnp.transpose(pairs[..., :NOPE], (1, 2, 0)).reshape(heads // 2, 2 * NOPE, -1)
    value_up = jnp.transpose(pairs[..., NOPE:], (1, 0, 2)).reshape(heads // 2, 2, -1, VDIM)
    value_up = jnp.stack(
        [
            jnp.pad(value_up[:, 0], ((0, 0), (0, 0), (0, VDIM))),
            jnp.pad(value_up[:, 1], ((0, 0), (0, 0), (VDIM, 0))),
        ],
        axis=1,
    ).reshape(heads, -1, 2 * VDIM)
    positions = z * token_count + jnp.arange(token_count)
    tables = rope_tables(positions, ROPE)
    cosine, sine = (jnp.tile(table, (seq_count, LANES // (ROPE // 2))) for table in tables)
    result = mix(
        nz, nx, blocks, lines, latents, out_slabs, up, q_gain, kv_gain, key_up, value_up,
        cosine, sine, delta_gain.reshape(1, HEAD), post_gain.reshape(1, -1),
    )
    return result.reshape(seq_count, token_count, result.shape[1])


def solution(mesh):
    return jax.shard_map(
        local,
        mesh=mesh,
        in_specs=(
            P(("grp", "fs"), "sp", None),
            P(),
            P(("sp", "fs"), "tp"),
            P(("sp", "fs"), "tp"),
            P(("sp", "fs"), "tp"),
            P(),
            P(),
            P(),
            P(),
            P(("sp", "fs"), None),
            P(("sp", "fs"), None),
            P(),
            P(),
            P(),
            P(None, "tp"),
            P(None, "tp"),
            P("tp", ("sp", "fs")),
            P("tp", ("sp", "fs")),
            P("tp"),
        ),
        out_specs=P(("grp", "fs"), "sp", "tp"),
        check_vma=False,
    )
```

```python
import functools

import jax
import jax.numpy as jnp
import numpy as np
from jax import lax
from jax.experimental import pallas as pl
from jax.experimental.pallas import tpu as pltpu
from jax.sharding import PartitionSpec as P

HEAD = 128
NOPE = 64
ROPE = 32
VDIM = 64
BLOCK = 64
LANES = 128

NORM_EPS = 1e-06
ROPE_THETA = 10000.0
F32 = jnp.float32
BF16 = jnp.bfloat16
MESH = pl.DeviceIdType.MESH
VM = pltpu.VMEM


def remote(src, dst, send_sem, recv_sem, where):
    return pltpu.make_async_remote_copy(
        src_ref=src,
        dst_ref=dst,
        send_sem=send_sem,
        recv_sem=recv_sem,
        device_id=where,
        device_id_type=MESH,
    )


def greet(places, count):
    barrier = pltpu.get_barrier_semaphore()
    for place in places:
        pl.semaphore_signal(barrier, inc=1, device_id=place, device_id_type=MESH)
    pl.semaphore_wait(barrier, count)


def mm(left, right):
    return lax.dot_general(
        left.astype(BF16), right.astype(BF16), (((1,), (0,)), ((), ())), preferred_element_type=F32
    )


def mm_nt(left, right):
    return lax.dot_general(
        left.astype(BF16), right.astype(BF16), (((1,), (1,)), ((), ())), preferred_element_type=F32
    )


def unit(values):
    return values * lax.rsqrt(jnp.sum(values * values, axis=-1, keepdims=True) + NORM_EPS)


def swish(values):
    return values * (1.0 / (1.0 + jnp.exp(-values)))


def layer_kernel(
    nz, nx, tok_ref, pre_ref, wq_ref, wk_ref, wv_ref, qd_ref, kvd_ref, small_ref, rate_ref, wt_ref,
    qgain_ref, kvgain_ref, qup_ref, lup_ref, far_ref, near_ref, dgain_ref, post_ref, out_ref,
    toks, normed, ws, wz, side, proj, place, blocks, lines_out, latents,
    dr, gr, lr, kvg, wo, homed, ready, state_out, state_in, part_out, part_in,
    loc_sem, wx_send, wx_recv, tok_send, tok_recv, fwd_send, fwd_recv, r_send, r_recv, l_send, l_recv,
    a_send, a_recv, d_send, d_recv, g_send, g_recv, kr_send, kr_recv, kl_send, kl_recv,
    kp_send, kp_recv, w_send, w_recv, st_send, st_recv, h_send, h_recv, p_send, p_recv,
):
    z, x, t = lax.axis_index("sp"), lax.axis_index("fs"), lax.axis_index("tp")
    half = nz // 2
    zh, zl = z // half, lax.rem(z, half)
    lane_t = 1 - zh
    cores = 2 * nx
    span = wq_ref.shape[0]
    rows = tok_ref.shape[0] * tok_ref.shape[1]
    count = rows // BLOCK
    partner = {"tp": 1 - t}
    near = [
        (dx, dt, lax.rem(x + dx, nx), lax.rem(t + dt, 2), lax.rem(x + nx - dx, nx))
        for dx in range(nx)
        for dt in range(2)
        if dx or dt
    ]
    others = [lax.rem(x + d, nx) for d in range(1, nx)]
    right, left = {"sp": lax.rem(z + 1, nz)}, {"sp": lax.rem(z + nz - 1, nz)}
    east, west = {"fs": lax.rem(x + 1, nx)}, {"fs": lax.rem(x + nx - 1, nx)}
    sources = [{"fs": back, "tp": to} for dx, dt, fx, to, back in near]
    sources += [right, left]
    sources += [{"sp": half * t + j, "tp": 1 - zh} for j in range(half)]
    sources += [
        {"fs": xl, "sp": 2 * x + sl + half * (1 - t), "tp": zh} for sl in range(2) for xl in range(nx)
    ]
    greet(sources, len(sources))
    started = []

    def begin(copy):
        copy.start()
        started.append(copy)
        return copy

    def local(src, dst, k):
        copy = pltpu.make_async_copy(src, dst, loc_sem.at[k])
        copy.start()
        return copy

    def chunk(slot, part):
        if part is None:
            return wz.at[slot]
        return ws.at[slot, pl.ds(pl.multiple_of(part * span, span), span)]

    def piece(k):
        return ws.at[z, pl.ds(pl.multiple_of(x * span, span), span), pl.ds(k * LANES, LANES)]

    def columns_of(ref, owner):
        return ref.at[:, pl.ds(pl.multiple_of(owner * LANES, LANES), LANES)]

    mains = (wq_ref, wk_ref, wv_ref)
    for d, o in enumerate(others):
        for k, ref in enumerate(mains):
            begin(
                remote(columns_of(ref, o), piece(k), wx_send.at[d, k], wx_recv.at[d, k], {"fs": o})
            )
    own_w = [local(columns_of(ref, x), piece(k), k) for k, ref in enumerate(mains)]
    own_o = local(wt_ref, wz.at[z], 3)
    own_t = local(tok_ref, toks.at[pl.ds(2 * x, 2)], 4)

    q_width, kv_width = qd_ref.shape[1] // cores, kvd_ref.shape[1] // cores
    rope_width = ROPE // cores
    at_rope = q_width + kv_width
    at_beta = at_rope + rope_width

    def picked(source, lane, first, stop, start):
        return (lane >= first) & (lane < stop) & (source == start + lane - first)

    def ones(mask):
        return jnp.where(mask, 1.0, 0.0)

    def iotas(depth):
        shape = (depth, LANES)
        return lax.broadcasted_iota(jnp.int32, shape, 0), lax.broadcasted_iota(jnp.int32, shape, 1)

    for o in range(nx):
        core, head = 2 * o + t, nx * t + o
        source, lane = iotas(qd_ref.shape[1])
        made = mm(qd_ref[...], ones(picked(source, lane, 0, q_width, q_width * core)))
        source, lane = iotas(kvd_ref.shape[1])
        made += mm(kvd_ref[...], ones(picked(source, lane, q_width, at_rope, kv_width * core)))
        source, lane = iotas(LANES)
        select = picked(source, lane, at_rope, at_beta, rope_width * core)
        select = select | picked(source, lane, at_beta, at_beta + 1, ROPE + head)
        select = select | picked(source, lane, at_beta + 1, at_beta + 2, ROPE + cores + head)
        made += mm(small_ref[...], ones(select))
        side[o] = made.astype(BF16)
    for d, o in enumerate(others):
        k = len(mains)
        begin(remote(side.at[o], piece(k), wx_send.at[d, k], wx_recv.at[d, k], {"fs": o}))
    own_w.append(local(side.at[x], piece(len(mains)), 5))
    for d, o in enumerate(others):
        begin(remote(tok_ref.at[t], toks.at[2 * x + t], tok_send.at[d], tok_recv.at[d], {"fs": o}))

    reach_r, reach_l = nz // 2, nz // 2 - 1

    def go_right(step, part, slot):
        mark = nx if part is None else part
        return remote(
            chunk(slot, part), chunk(slot, part), r_send.at[step, mark], r_recv.at[step, mark], right
        )

    def go_left(step, part, slot):
        mark = nx if part is None else part
        return remote(
            chunk(slot, part), chunk(slot, part), l_send.at[step, mark], l_recv.at[step, mark], left
        )

    for d in range(nx):
        part = lax.rem(x + nx - d, nx)
        if d == 0:
            for copy in own_w:
                copy.wait()
        else:
            for k in range(len(mains) + 1):
                remote(
                    piece(k), piece(k), wx_send.at[d - 1, k], wx_recv.at[d - 1, k], {"fs": part}
                ).wait_recv()
        go_right(0, part, z).start()
        go_left(0, part, z).start()
    own_o.wait()
    go_right(0, None, z).start()
    go_left(0, None, z).start()

    from_lane = lax.broadcasted_iota(jnp.int32, (LANES, 4 * LANES), 0)
    to_lane = lax.broadcasted_iota(jnp.int32, (LANES, 4 * LANES), 1)
    kv_total = kv_width * cores
    spot = to_lane - kv_total
    spot_in = lax.rem(to_lane, ROPE)
    sign = jnp.where(spot_in < ROPE // 2, -1.0, 1.0)
    is_kv = (from_lane >= q_width) & (from_lane < at_rope)
    is_rope = (from_lane >= at_rope) & (from_lane < at_beta)
    for c in range(cores):
        entry = from_lane - at_rope + rope_width * c
        kept = is_kv & (to_lane == from_lane - q_width + kv_width * c)
        straight = is_rope & (spot >= 0) & (spot < LANES) & (spot_in == entry)
        swapped = is_rope & (spot >= LANES) & (lax.rem(spot_in + ROPE // 2, ROPE) == entry)
        place[c] = (ones(kept | straight) + jnp.where(swapped, sign, 0.0)).astype(BF16)

    def ring(step, carry):
        from_left = lax.rem(z + 2 * nz - 1 - step, nz)
        from_right = lax.rem(z + 1 + step, nz)
        for d in range(nx + 1):
            part = lax.rem(x + nx - d, nx) if d < nx else None
            go_right(step, part, from_left).wait_recv()

            @pl.when(step < reach_r - 1)
            def _():
                go_right(step + 1, part, from_left).start()

            @pl.when(step < reach_l)
            def _():
                go_left(step, part, from_right).wait_recv()

            @pl.when(step < reach_l - 1)
            def _():
                go_left(step + 1, part, from_right).start()

        return carry

    early = (reach_r * 5) // 8
    lax.fori_loop(0, early, ring, 0)
    own_t.wait()
    for d in range(nx - 1):
        held = toks.at[2 * lax.rem(x + nx - 1 - d, nx) + t]
        remote(held, held, tok_send.at[d], tok_recv.at[d], partner).wait_recv()
        begin(remote(held, held, fwd_send.at[d], fwd_recv.at[d], partner))
    lax.fori_loop(early, early + 1, ring, 0)
    for d in range(nx - 1):
        held = toks.at[2 * lax.rem(x + nx - 1 - d, nx) + 1 - t]
        remote(held, held, fwd_send.at[d], fwd_recv.at[d], partner).wait_recv()

    def normalize(i, carry):
        values = toks[i].astype(F32)
        scale = lax.rsqrt(jnp.mean(values * values, axis=-1, keepdims=True) + NORM_EPS)
        normed[pl.ds(pl.multiple_of(i * BLOCK, BLOCK), BLOCK), :] = (
            values * scale * pre_ref[...]
        ).astype(BF16)
        return carry

    lax.fori_loop(0, toks.shape[0], normalize, 0)
    lax.fori_loop(early + 1, reach_r - 1, ring, 0)
    depth = ws.shape[1]

    def product(slot):
        lhs = normed[:, pl.ds(pl.multiple_of(slot * depth, depth), depth)]
        return lax.dot_general(lhs, ws[slot], (((1,), (0,)), ((), ())), preferred_element_type=F32)

    def gather_product(i, carry):
        proj[...] += product(lax.rem(z + nz - reach_l + i, nz))
        return carry

    proj[...] = product(z + 0)
    lax.fori_loop(0, reach_l, gather_product, 0)
    lax.fori_loop(reach_l + 1, 2 * reach_l + 1, gather_product, 0)
    lax.fori_loop(reach_r - 1, reach_r, ring, 0)
    proj[...] += product(lax.rem(z + reach_r, nz))

    for o in range(nx):
        latents[o] = proj[o * rows : (o + 1) * rows, 3 * HEAD :].astype(BF16)
    own_l = local(latents.at[x], lr.at[2 * x + t], 0)
    for k, (dx, dt, fx, to, back) in enumerate(near):
        begin(
            remote(latents.at[fx], lr.at[2 * x + t], a_send.at[k], a_recv.at[k], {"fs": fx, "tp": to})
        )

    def w_part(owner, upper):
        return wo.at[pl.ds(half * upper, half), owner]

    own_c = local(wz, wo.at[:, x], 1)
    for upper, where, k in ((0, east, 0), (1, west, 1), (1, east, 2), (0, west, 3)):
        begin(
            remote(wz.at[pl.ds(half * upper, half)], w_part(x, upper), w_send.at[k], w_recv.at[k], where)
        )

    size = 2 * BLOCK
    row = lax.broadcasted_iota(jnp.int32, (size, size), 0)
    col = lax.broadcasted_iota(jnp.int32, (size, size), 1)
    eye = row == col
    same = (row // BLOCK) == (col // BLOCK)
    rate = rate_ref[nx * t + x]
    even = lax.rem(z, 2) == 0
    line = lax.broadcasted_iota(jnp.int32, (8, LANES), 0)
    first_half = lax.broadcasted_iota(jnp.int32, (8, LANES), 1) < LANES // 2
    for p in range(half // 2):
        blocks[2 * p : 2 * p + 2] = (
            proj[p * size : (p + 1) * size, : 3 * HEAD].astype(BF16).reshape(2, BLOCK, 3 * HEAD)
        )
        tail = proj[p * size : (p + 1) * size, 3 * HEAD :]
        write = 1.0 / (1.0 + jnp.exp(-tail[:, at_beta : at_beta + 1]))
        pushed = tail[:, at_beta + 1 : at_beta + 2]
        fade = -rate * (jnp.maximum(pushed, 0.0) + jnp.log1p(jnp.exp(-jnp.abs(pushed))))
        write_row = jnp.sum(jnp.where(eye, write, 0.0), axis=0, keepdims=True)
        fade_row = jnp.sum(jnp.where(same & (row <= col), fade, 0.0), axis=0, keepdims=True)
        both_rows = jnp.where(line == 0, write_row, jnp.where(line == 1, fade_row, 0.0))
        rolled = pltpu.roll(both_rows, LANES // 2, 1)
        lines_out[2 * p] = jnp.where(
            even, jnp.where(first_half, both_rows, 0.0), jnp.where(first_half, 0.0, rolled)
        )
        lines_out[2 * p + 1] = jnp.where(
            even, jnp.where(first_half, rolled, 0.0), jnp.where(first_half, 0.0, both_rows)
        )

    def send_lane(i):
        s = lax.rem(zl + i, half)
        where = {"sp": s + half * (1 - t), "tp": zh}
        begin(remote(lines_out.at[s], gr.at[zl], g_send.at[i], g_recv.at[zl], where))
        begin(remote(blocks.at[s], dr.at[zl], d_send.at[i], d_recv.at[zl], where))

    send_lane(0)
    send_lane(1)

    for k, (dx, dt, fx, to, back) in enumerate(near):
        slot = lr.at[2 * back + to]
        remote(slot, slot, a_send.at[k], a_recv.at[k], {"fs": back, "tp": to}).wait_recv()
    own_l.wait()

    lane = lax.broadcasted_iota(jnp.int32, (rows, LANES), 1)
    far_cos, far_sin = far_ref[0, pl.ds(z, 1), :], far_ref[1, pl.ds(z, 1), :]
    near_cos = jnp.concatenate([near_ref[0]] * count, axis=0)
    near_sin = jnp.concatenate([near_ref[1]] * count, axis=0)
    cosine = far_cos * near_cos - far_sin * near_sin
    sine = far_sin * near_cos + far_cos * near_sin
    slab = mm(lr[0], place[0])
    for c in range(1, cores):
        slab = slab + mm(lr[c], place[c])
    kv_lat = slab[:, :kv_total]
    kv_lat = kv_lat * lax.rsqrt(jnp.mean(kv_lat * kv_lat, axis=-1, keepdims=True) + NORM_EPS)
    turned = slab[:, kv_total : kv_total + LANES] * cosine + slab[:, kv_total + LANES :] * sine
    keys = jnp.concatenate([kv_lat * kvgain_ref[...], turned], axis=1).astype(BF16)
    for s in range(count):
        kvg[s, z] = keys[s * BLOCK : (s + 1) * BLOCK]

    def key_right(step, slot):
        return remote(kvg.at[t, slot], kvg.at[t, slot], kr_send.at[step], kr_recv.at[step], right)

    def key_left(step, slot):
        return remote(kvg.at[t, slot], kvg.at[t, slot], kl_send.at[step], kl_recv.at[step], left)

    def across(slot, k):
        return remote(kvg.at[t, slot], kvg.at[t, slot], kp_send.at[k], kp_recv.at[k], partner)

    begin(key_right(0, z))
    begin(key_left(0, z))

    q_lat = jnp.concatenate(
        [
            jnp.where(
                lane < LANES // 2,
                lr[c].astype(F32),
                pltpu.roll(lr[c + 1].astype(F32), LANES // 2, 1),
            )
            for c in range(0, cores, 2)
        ],
        axis=1,
    )
    q_lat = q_lat * lax.rsqrt(jnp.mean(q_lat * q_lat, axis=-1, keepdims=True) + NORM_EPS)
    query = mm(q_lat * qgain_ref[...], qup_ref[...]).astype(BF16).astype(F32)
    head_width = NOPE + ROPE
    heads = query.shape[1] // head_width
    is_turn = (lane >= NOPE) & (lane < head_width)
    from_turn = (row >= NOPE) & (row < head_width)
    low_turn = (col >= NOPE) & (col < NOPE + ROPE // 2)
    high_turn = (col >= NOPE + ROPE // 2) & (col < head_width)
    exchange = jnp.where(from_turn & high_turn & (row == col - ROPE // 2), 1.0, 0.0)
    exchange = exchange - jnp.where(from_turn & low_turn & (row == col + ROPE // 2), 1.0, 0.0)
    stacked = [[] for _ in range(count)]
    for h in range(heads):
        own = query[:, h * head_width : (h + 1) * head_width]
        own = jnp.concatenate([own, jnp.zeros((rows, LANES - head_width), F32)], axis=1)
        absorbed = mm_nt(
            jnp.where(lane < NOPE, own, 0.0), lup_ref[:, h * LANES : (h + 1) * LANES]
        )
        turn = jnp.where(is_turn, own * cosine + mm(own, exchange) * sine, 0.0)
        joined = jnp.concatenate([absorbed, turn], axis=1).astype(BF16)
        for s in range(count):
            stacked[s].append(joined[s * BLOCK : (s + 1) * BLOCK])

    for step in range(reach_r):
        if step + 2 < half:
            send_lane(step + 2)
        from_left = lax.rem(z + 2 * nz - 1 - step, nz)
        from_right = lax.rem(z + 1 + step, nz)
        key_right(step, from_left).wait_recv()
        if step < reach_r - 1:
            begin(key_right(step + 1, from_left))
        begin(across(from_left, step))
        if step < reach_l:
            key_left(step, from_right).wait_recv()
            if step < reach_l - 1:
                begin(key_left(step + 1, from_right))
            begin(across(from_right, reach_r + step))

    behind, ahead = lax.rem(x + nx - 1, nx), lax.rem(x + 1, nx)
    remote(w_part(behind, 0), w_part(behind, 0), w_send.at[0], w_recv.at[0], west).wait_recv()
    begin(remote(w_part(behind, 0), w_part(behind, 0), w_send.at[4], w_recv.at[4], east))
    remote(w_part(ahead, 1), w_part(ahead, 1), w_send.at[1], w_recv.at[1], east).wait_recv()
    begin(remote(w_part(ahead, 1), w_part(ahead, 1), w_send.at[5], w_recv.at[5], west))

    for j in range(half):
        where = {"sp": half * t + j, "tp": 1 - zh}
        remote(gr.at[j], gr.at[j], g_send.at[j], g_recv.at[j], where).wait_recv()
        remote(dr.at[j], dr.at[j], d_send.at[j], d_recv.at[j], where).wait_recv()

    strict = same & (row > col)
    causal = same & (row >= col)
    wide_row = lax.broadcasted_iota(jnp.int32, (size, 2 * size), 0)

    def upright(line, where):
        return jnp.sum(jnp.where(where, line, 0.0), axis=1, keepdims=True)

    terms = []
    for p in range(half // 2):
        block = dr[2 * p : 2 * p + 2].reshape(size, 3 * HEAD).astype(F32)
        q = unit(swish(block[:, :HEAD])) * HEAD**-0.5
        k = unit(swish(block[:, HEAD : 2 * HEAD]))
        v = swish(block[:, 2 * HEAD :])
        lines = gr[2 * p] + gr[2 * p + 1]
        beta_row, gate_row = lines[0:1], lines[1:2]
        beta, gate = upright(beta_row, eye), upright(gate_row, eye)
        last = upright(gate_row, col == (row // BLOCK) * BLOCK + BLOCK - 1)
        decay = jnp.exp(jnp.where(causal, gate - gate_row, 0.0))
        lower = jnp.where(strict, beta * mm_nt(k, k) * decay, 0.0)
        scores = jnp.where(causal, mm_nt(q, k) * decay, 0.0)
        inverse = jnp.where(eye, 1.0, 0.0) - jnp.where((row // 2 == col // 2), lower, 0.0)
        width = 2
        while width < BLOCK:
            pick = (row // (2 * width) == col // (2 * width)) & (row // width != col // width)
            inverse = inverse - mm(mm(inverse, jnp.where(pick, lower, 0.0)), inverse)
            width *= 2
        both = mm(inverse, jnp.concatenate([beta * v, beta * k * jnp.exp(gate)], axis=1))
        key_t = (k * jnp.exp(last - gate)).T
        moves = [
            mm(key_t, jnp.where(wide_row // BLOCK == h, both, 0.0)) for h in range(2)
        ]
        factors = [jnp.exp(last[h * BLOCK : h * BLOCK + 1]) for h in range(2)]
        terms.append((q * jnp.exp(gate), scores, both, moves, factors))

    total = jnp.concatenate([jnp.zeros((size, size), F32), jnp.where(eye, 1.0, 0.0)], axis=1)
    states = []
    for j in range(half):
        states.append(total)
        move, factor = terms[j // 2][3][j % 2], terms[j // 2][4][j % 2]
        grown = factor * total - mm(move[:, size:], total)
        total = jnp.concatenate([grown[:, :size] + move[:, :size], grown[:, size:]], axis=1)

    state_out[...] = total[:, :size]
    crossing = remote(state_out, state_in, st_send.at[0], st_recv.at[0], partner)

    @pl.when(t == 0)
    def _():
        state_in[...] = jnp.zeros_like(state_in)
        crossing.start()

    @pl.when(t == 1)
    def _():
        crossing.wait_recv()

    start = state_in[...]
    for p in range(half // 2):
        queries, scores, both, _, _ = terms[p]
        read, fixed = [], []
        for h in range(2):
            j = 2 * p + h
            state = states[j][:, :size] + mm(states[j][:, size:], start)
            cut = slice(h * BLOCK, (h + 1) * BLOCK)
            got = mm(jnp.concatenate([both[cut, size:], queries[cut]], axis=0), state)
            fixed.append(both[cut, :size] - got[:BLOCK])
            read.append(got[BLOCK:])
        raw = jnp.concatenate(read, axis=0) + mm(scores, jnp.concatenate(fixed, axis=0))
        raw = raw * lax.rsqrt(jnp.mean(raw * raw, axis=-1, keepdims=True) + NORM_EPS)
        done = (raw * dgain_ref[...]).astype(BF16)
        ready[2 * p] = done[:BLOCK]
        ready[2 * p + 1] = done[BLOCK:]

    for i in range(half):
        j = lax.rem(zl + i, half)
        begin(
            remote(
                ready.at[j],
                homed.at[lax.rem(zl, 2), x],
                h_send.at[i],
                h_recv.at[lax.rem(zl, 2), x],
                {"fs": zl // 2, "sp": half * t + j, "tp": lane_t},
            )
        )

    for k in range(nz - 1):
        slot = kvg.at[1 - t, lax.rem(z + 1, nz)]
        remote(slot, slot, kp_send.at[k], kp_recv.at[k], partner).wait_recv()
    allowed = lax.broadcasted_iota(jnp.int32, (1, nz * BLOCK), 1) < (z + 1) * BLOCK
    outs = []
    low = lax.broadcasted_iota(jnp.int32, (BLOCK, LANES), 1) < LANES // 2
    for s in range(count):
        keys = kvg[s].reshape(nz * BLOCK, kvg.shape[3])
        scores = mm_nt(jnp.concatenate(stacked[s], axis=0), keys) * (NOPE + ROPE) ** (-0.5)
        scores = jnp.where(allowed, scores, -1e30)
        peak = jnp.max(scores, axis=-1, keepdims=True)
        weights = jnp.where(allowed, jnp.exp(scores - peak), 0.0)
        total = jnp.sum(weights, axis=-1, keepdims=True)
        mixed = (mm(weights, keys[:, :kv_total]) / total).astype(BF16)
        made = [
            mm(mixed[h * BLOCK : (h + 1) * BLOCK], lup_ref[:, h * LANES : (h + 1) * LANES])
            for h in range(heads)
        ]
        pairs = [
            jnp.where(low, pltpu.roll(made[h], LANES // 2, 1), made[h + 1]).astype(BF16)
            for h in range(0, heads, 2)
        ]
        outs.append(jnp.concatenate(pairs, axis=1))
    latent_heads = jnp.concatenate(outs, axis=0)

    own_c.wait()
    for k, owner, upper in (
        (2, lax.rem(x + nx - 1, nx), 1),
        (3, lax.rem(x + 1, nx), 0),
        (4, lax.rem(x + 2, nx), 0),
        (5, lax.rem(x + 2, nx), 1),
    ):
        remote(
            w_part(owner, upper), w_part(owner, upper), w_send.at[k], w_recv.at[k], east
        ).wait_recv()
    for sl in range(2):
        for xl in range(nx):
            slot = homed.at[sl, xl]
            where = {"fs": xl, "sp": 2 * x + sl + half * (1 - t), "tp": zh}
            remote(slot, slot, h_send.at[0], h_recv.at[sl, xl], where).wait_recv()
    delta_heads = [homed[:, xl].reshape(rows, HEAD) for xl in range(nx)]
    joined = jnp.concatenate(delta_heads + [latent_heads], axis=1)
    width = wo.shape[0] * wo.shape[1] * wo.shape[2]
    columns = wo[...].reshape(width, wo.shape[3])
    part_out[...] = mm_nt(joined, columns).astype(BF16)
    swap_parts = begin(remote(part_out, part_in, p_send.at[0], p_recv.at[0], partner))
    swap_parts.wait_recv()
    whole = part_out[...].astype(F32) + part_in[...].astype(F32)
    scale = lax.rsqrt(jnp.mean(whole * whole, axis=-1, keepdims=True) + NORM_EPS)
    own_half = jnp.where(t == 0, whole[:, : width // 2], whole[:, width // 2 :])
    out_ref[...] = (own_half * scale * post_ref[...]).astype(BF16)

    for copy in started:
        copy.wait_send()

    def drain(step, carry):
        for part in [*range(nx), None]:
            go_right(step, part, z).wait_send()

            @pl.when(step < reach_l)
            def _():
                go_left(step, part, z).wait_send()

        return carry

    lax.fori_loop(0, reach_r, drain, 0)

    @pl.when(t == 0)
    def _():
        crossing.wait_send()


def layer(nz, nx, *operands):
    tokens, query_weight, out_cols, latent_up = (operands[k] for k in (0, 2, 9, 13))
    half = nz // 2
    seqs, length, width = tokens.shape
    rows = seqs * length
    span = query_weight.shape[0]
    slab = latent_up.shape[0] + LANES
    dma = pltpu.SemaphoreType.DMA

    def pair(*shape):
        return [dma(shape), dma(shape)]

    specs = [pl.BlockSpec(memory_space=VM)] * len(operands)
    specs[8] = pl.BlockSpec(memory_space=pltpu.SMEM)
    return pl.pallas_call(
        functools.partial(layer_kernel, nz, nx),
        out_shape=jax.ShapeDtypeStruct((rows, width // 2), BF16),
        in_specs=specs,
        out_specs=pl.BlockSpec(memory_space=VM),
        scratch_shapes=[
            VM((seqs * nx, length, width), BF16),
            VM((nx * rows, width), BF16),
            VM((nz, nx * span, 4 * LANES), BF16),
            VM((nz, *out_cols.shape), BF16),
            VM((nx, span, LANES), BF16),
            VM((nx * rows, 4 * LANES), F32),
            VM((2 * nx, LANES, 4 * LANES), BF16),
            VM((half, BLOCK, 3 * HEAD), BF16),
            VM((half, 8, LANES), F32),
            VM((nx, rows, LANES), BF16),
            VM((half, BLOCK, 3 * HEAD), BF16),
            VM((half, 8, LANES), F32),
            VM((2 * nx, rows, LANES), BF16),
            VM((seqs, nz, length, slab), BF16),
            VM((nz, nx, *out_cols.shape), BF16),
            VM((2, nx, BLOCK, HEAD), BF16),
            VM((half, BLOCK, HEAD), BF16),
            VM((HEAD, HEAD), F32),
            VM((HEAD, HEAD), F32),
            VM((rows, width), BF16),
            VM((rows, width), BF16),
            dma((6,)),
            *pair(nx - 1, 4),
            *pair(nx - 1),
            *pair(nx - 1),
            *pair(half, nx + 1),
            *pair(half - 1, nx + 1),
            *pair(2 * nx - 1),
            *pair(half),
            *pair(half),
            *pair(half),
            *pair(half - 1),
            *pair(nz - 1),
            *pair(6),
            *pair(1),
            dma((half,)),
            dma((2, nx)),
            *pair(1),
        ],
        compiler_params=pltpu.CompilerParams(collective_id=1, has_side_effects=True),
        name="layer",
    )(*operands)


def rope_tables(count, length):
    frequency = ROPE_THETA ** (-np.arange(0, ROPE, 2, dtype=np.float64) / ROPE)
    frequency = np.tile(frequency, LANES // (ROPE // 2))[None, :]

    def both(positions):
        angles = positions[:, None] * frequency
        return np.stack([np.cos(angles), np.sin(angles)]).astype(np.float32)

    return both(np.arange(count) * float(length)), both(np.arange(length) * 1.0)


def local(
    tokens,
    pre_gain,
    query_weight,
    key_weight,
    value_weight,
    beta_weight,
    decay_weight,
    decay_rate,
    delta_gain,
    query_down,
    latent_down,
    rope_weight,
    query_gain,
    latent_gain,
    query_up,
    latent_up,
    delta_out,
    latent_out,
    post_gain,
):
    nz, nx = lax.axis_size("sp"), lax.axis_size("fs")
    z, x = lax.axis_index("sp"), lax.axis_index("fs")
    seq_count, token_count = tokens.shape[:2]
    span = query_weight.shape[0]
    small = jnp.concatenate(
        [
            lax.dynamic_slice_in_dim(array, (z * nx + x) * span, span, 0)
            for array in (rope_weight, beta_weight, decay_weight)
        ],
        axis=1,
    )
    small = jnp.pad(small, ((0, 0), (0, LANES - small.shape[1])))
    out_cols = jnp.concatenate([delta_out, latent_out], axis=0).T
    far, near = rope_tables(nz, token_count)
    result = layer(
        nz,
        nx,
        tokens,
        pre_gain[None],
        query_weight,
        key_weight,
        value_weight,
        query_down,
        latent_down,
        small,
        decay_rate,
        out_cols,
        query_gain[None],
        latent_gain[None],
        query_up,
        latent_up,
        jnp.asarray(far),
        jnp.asarray(near),
        delta_gain[None],
        post_gain[None],
    )
    return result.reshape(seq_count, token_count, result.shape[1])


def solution(mesh):
    return jax.shard_map(
        local,
        mesh=mesh,
        in_specs=(
            P(("grp", "fs"), "sp", None),
            P(),
            P(("sp", "fs"), "tp"),
            P(("sp", "fs"), "tp"),
            P(("sp", "fs"), "tp"),
            P(),
            P(),
            P(),
            P(),
            P(("sp", "fs"), None),
            P(("sp", "fs"), None),
            P(),
            P(),
            P(),
            P(None, "tp"),
            P(None, "tp"),
            P("tp", ("sp", "fs")),
            P("tp", ("sp", "fs")),
            P("tp"),
        ),
        out_specs=P(("grp", "fs"), "sp", "tp"),
        check_vma=False,
    )
```

```python
import functools

import jax
import jax.numpy as jnp
import numpy as np
from jax import lax
from jax.experimental import pallas as pl
from jax.experimental.pallas import tpu as pltpu
from jax.sharding import PartitionSpec as P

HEAD = 128
NOPE = 64
ROPE = 32
VDIM = 64
BLOCK = 64
LANES = 128

NORM_EPS = 1e-06
ROPE_THETA = 10000.0
F32 = jnp.float32
BF16 = jnp.bfloat16
MESH = pl.DeviceIdType.MESH
VM = pltpu.VMEM


def remote(src, dst, send_sem, recv_sem, where):
    return pltpu.make_async_remote_copy(
        src_ref=src,
        dst_ref=dst,
        send_sem=send_sem,
        recv_sem=recv_sem,
        device_id=where,
        device_id_type=MESH,
    )


def greet(places, count):
    barrier = pltpu.get_barrier_semaphore()
    for place in places:
        pl.semaphore_signal(barrier, inc=1, device_id=place, device_id_type=MESH)
    pl.semaphore_wait(barrier, count)


def mm(left, right):
    return lax.dot_general(
        left.astype(BF16), right.astype(BF16), (((1,), (0,)), ((), ())), preferred_element_type=F32
    )


def mm_nt(left, right):
    return lax.dot_general(
        left.astype(BF16), right.astype(BF16), (((1,), (1,)), ((), ())), preferred_element_type=F32
    )


def unit(values):
    return values * lax.rsqrt(jnp.sum(values * values, axis=-1, keepdims=True) + NORM_EPS)


def swish(values):
    return values * (1.0 / (1.0 + jnp.exp(-values)))


def layer_kernel(
    nz, nx, tok_ref, pre_ref, wq_ref, wk_ref, wv_ref, qd_ref, kvd_ref, small_ref, rate_ref, wt_ref,
    qgain_ref, kvgain_ref, qup_ref, lup_ref, far_ref, near_ref, dgain_ref, post_ref, out_ref,
    toks, normed, ws, wz, side, proj, place, blocks, lines_out, latents,
    dr, gr, lr, kvg, wo, homed, ready, state_out, state_in, part_out, part_in,
    loc_sem, wx_send, wx_recv, tok_send, tok_recv, fwd_send, fwd_recv, r_send, r_recv, l_send, l_recv,
    a_send, a_recv, d_send, d_recv, g_send, g_recv, kr_send, kr_recv, kl_send, kl_recv,
    kp_send, kp_recv, w_send, w_recv, st_send, st_recv, h_send, h_recv, p_send, p_recv,
):
    z, x, t = lax.axis_index("sp"), lax.axis_index("fs"), lax.axis_index("tp")
    half = nz // 2
    zh, zl = z // half, lax.rem(z, half)
    lane_t = 1 - zh
    cores = 2 * nx
    span = wq_ref.shape[0]
    rows = tok_ref.shape[0] * tok_ref.shape[1]
    count = rows // BLOCK
    partner = {"tp": 1 - t}
    near = [
        (dx, dt, lax.rem(x + dx, nx), lax.rem(t + dt, 2), lax.rem(x + nx - dx, nx))
        for dx in range(nx)
        for dt in range(2)
        if dx or dt
    ]
    others = [lax.rem(x + d, nx) for d in range(1, nx)]
    right, left = {"sp": lax.rem(z + 1, nz)}, {"sp": lax.rem(z + nz - 1, nz)}
    east, west = {"fs": lax.rem(x + 1, nx)}, {"fs": lax.rem(x + nx - 1, nx)}
    sources = [{"fs": back, "tp": to} for dx, dt, fx, to, back in near]
    sources += [{"sp": lax.rem(z + hop, nz)} for hop in (1, 2, nz - 2, nz - 1)]
    sources += [{"sp": half * t + j, "tp": 1 - zh} for j in range(half)]
    sources += [
        {"fs": xl, "sp": 2 * x + sl + half * (1 - t), "tp": zh} for sl in range(2) for xl in range(nx)
    ]
    greet(sources, len(sources))
    started = []

    def begin(copy):
        copy.start()
        started.append(copy)
        return copy

    def local(src, dst, k):
        copy = pltpu.make_async_copy(src, dst, loc_sem.at[k])
        copy.start()
        return copy

    def chunk(slot, part):
        if part is None:
            return wz.at[slot]
        return ws.at[slot, pl.ds(pl.multiple_of(part * span, span), span)]

    def piece(k):
        return ws.at[z, pl.ds(pl.multiple_of(x * span, span), span), pl.ds(k * LANES, LANES)]

    def columns_of(ref, owner):
        return ref.at[:, pl.ds(pl.multiple_of(owner * LANES, LANES), LANES)]

    mains = (wq_ref, wk_ref, wv_ref)
    for d, o in enumerate(others):
        for k, ref in enumerate(mains):
            begin(
                remote(columns_of(ref, o), piece(k), wx_send.at[d, k], wx_recv.at[d, k], {"fs": o})
            )
    own_w = [local(columns_of(ref, x), piece(k), k) for k, ref in enumerate(mains)]
    own_o = local(wt_ref, wz.at[z], 3)
    own_t = local(tok_ref, toks.at[pl.ds(2 * x, 2)], 4)

    reach_r, reach_l = nz // 2, nz // 2 - 1

    def go_right(step, part, slot):
        mark = nx if part is None else part
        return remote(
            chunk(slot, part), chunk(slot, part), r_send.at[step, mark], r_recv.at[step, mark], right
        )

    def go_left(step, part, slot):
        mark = nx if part is None else part
        return remote(
            chunk(slot, part), chunk(slot, part), l_send.at[step, mark], l_recv.at[step, mark], left
        )

    own_o.wait()
    go_right(0, None, z).start()
    go_left(0, None, z).start()

    q_width, kv_width = qd_ref.shape[1] // cores, kvd_ref.shape[1] // cores
    rope_width = ROPE // cores
    at_rope = q_width + kv_width
    at_beta = at_rope + rope_width

    def picked(source, lane, first, stop, start):
        return (lane >= first) & (lane < stop) & (source == start + lane - first)

    def ones(mask):
        return jnp.where(mask, 1.0, 0.0)

    def iotas(depth):
        shape = (depth, LANES)
        return lax.broadcasted_iota(jnp.int32, shape, 0), lax.broadcasted_iota(jnp.int32, shape, 1)

    for o in range(nx):
        core, head = 2 * o + t, nx * t + o
        source, lane = iotas(qd_ref.shape[1])
        made = mm(qd_ref[...], ones(picked(source, lane, 0, q_width, q_width * core)))
        source, lane = iotas(kvd_ref.shape[1])
        made += mm(kvd_ref[...], ones(picked(source, lane, q_width, at_rope, kv_width * core)))
        source, lane = iotas(LANES)
        select = picked(source, lane, at_rope, at_beta, rope_width * core)
        select = select | picked(source, lane, at_beta, at_beta + 1, ROPE + head)
        select = select | picked(source, lane, at_beta + 1, at_beta + 2, ROPE + cores + head)
        made += mm(small_ref[...], ones(select))
        side[o] = made.astype(BF16)
    for d, o in enumerate(others):
        k = len(mains)
        begin(remote(side.at[o], piece(k), wx_send.at[d, k], wx_recv.at[d, k], {"fs": o}))
    own_w.append(local(side.at[x], piece(len(mains)), 5))
    for d, o in enumerate(others):
        begin(remote(tok_ref.at[t], toks.at[2 * x + t], tok_send.at[d], tok_recv.at[d], {"fs": o}))

    for d in range(nx):
        part = lax.rem(x + nx - d, nx)
        if d == 0:
            for copy in own_w:
                copy.wait()
        else:
            for k in range(len(mains) + 1):
                remote(
                    piece(k), piece(k), wx_send.at[d - 1, k], wx_recv.at[d - 1, k], {"fs": part}
                ).wait_recv()
        go_right(0, part, z).start()
        go_left(0, part, z).start()

    from_lane = lax.broadcasted_iota(jnp.int32, (LANES, 4 * LANES), 0)
    to_lane = lax.broadcasted_iota(jnp.int32, (LANES, 4 * LANES), 1)
    kv_total = kv_width * cores
    spot = to_lane - kv_total
    spot_in = lax.rem(to_lane, ROPE)
    sign = jnp.where(spot_in < ROPE // 2, -1.0, 1.0)
    is_kv = (from_lane >= q_width) & (from_lane < at_rope)
    is_rope = (from_lane >= at_rope) & (from_lane < at_beta)
    for c in range(cores):
        entry = from_lane - at_rope + rope_width * c
        kept = is_kv & (to_lane == from_lane - q_width + kv_width * c)
        straight = is_rope & (spot >= 0) & (spot < LANES) & (spot_in == entry)
        swapped = is_rope & (spot >= LANES) & (lax.rem(spot_in + ROPE // 2, ROPE) == entry)
        place[c] = (ones(kept | straight) + jnp.where(swapped, sign, 0.0)).astype(BF16)

    def ring(step, carry):
        from_left = lax.rem(z + 2 * nz - 1 - step, nz)
        from_right = lax.rem(z + 1 + step, nz)
        for d in range(-1, nx):
            part = lax.rem(x + nx - d, nx) if d >= 0 else None
            go_right(step, part, from_left).wait_recv()

            @pl.when(step < reach_r - 1)
            def _():
                go_right(step + 1, part, from_left).start()

            @pl.when(step < reach_l)
            def _():
                go_left(step, part, from_right).wait_recv()

            @pl.when(step < reach_l - 1)
            def _():
                go_left(step + 1, part, from_right).start()

        return carry

    early = (reach_r * 5) // 8
    lax.fori_loop(0, early, ring, 0)
    own_t.wait()
    for d in range(nx - 1):
        held = toks.at[2 * lax.rem(x + nx - 1 - d, nx) + t]
        remote(held, held, tok_send.at[d], tok_recv.at[d], partner).wait_recv()
        begin(remote(held, held, fwd_send.at[d], fwd_recv.at[d], partner))
    lax.fori_loop(early, early + 1, ring, 0)
    for d in range(nx - 1):
        held = toks.at[2 * lax.rem(x + nx - 1 - d, nx) + 1 - t]
        remote(held, held, fwd_send.at[d], fwd_recv.at[d], partner).wait_recv()

    def normalize(i, carry):
        values = toks[i].astype(F32)
        scale = lax.rsqrt(jnp.mean(values * values, axis=-1, keepdims=True) + NORM_EPS)
        normed[pl.ds(pl.multiple_of(i * BLOCK, BLOCK), BLOCK), :] = (
            values * scale * pre_ref[...]
        ).astype(BF16)
        return carry

    lax.fori_loop(0, toks.shape[0], normalize, 0)
    lax.fori_loop(early + 1, reach_r - 1, ring, 0)
    depth = ws.shape[1]

    def product(slot):
        lhs = normed[:, pl.ds(pl.multiple_of(slot * depth, depth), depth)]
        return lax.dot_general(lhs, ws[slot], (((1,), (0,)), ((), ())), preferred_element_type=F32)

    def gather_product(i, carry):
        proj[...] += product(lax.rem(z + nz - reach_l + i, nz))
        return carry

    proj[...] = product(z + 0)
    lax.fori_loop(0, reach_l, gather_product, 0)
    lax.fori_loop(reach_l + 1, 2 * reach_l + 1, gather_product, 0)
    lax.fori_loop(reach_r - 1, reach_r, ring, 0)
    proj[...] += product(lax.rem(z + reach_r, nz))

    for o in range(nx):
        latents[o] = proj[o * rows : (o + 1) * rows, 3 * HEAD :].astype(BF16)
    own_l = local(latents.at[x], lr.at[2 * x + t], 0)
    for k, (dx, dt, fx, to, back) in enumerate(near):
        begin(
            remote(latents.at[fx], lr.at[2 * x + t], a_send.at[k], a_recv.at[k], {"fs": fx, "tp": to})
        )

    def w_part(owner, upper):
        return wo.at[pl.ds(half * upper, half), owner]

    own_c = local(wz, wo.at[:, x], 1)
    for upper, where, k in ((0, east, 0), (1, west, 1), (1, east, 2), (0, west, 3)):
        begin(
            remote(wz.at[pl.ds(half * upper, half)], w_part(x, upper), w_send.at[k], w_recv.at[k], where)
        )

    size = 2 * BLOCK
    row = lax.broadcasted_iota(jnp.int32, (size, size), 0)
    col = lax.broadcasted_iota(jnp.int32, (size, size), 1)
    eye = row == col
    same = (row // BLOCK) == (col // BLOCK)
    rate = rate_ref[nx * t + x]
    even = lax.rem(z, 2) == 0
    line = lax.broadcasted_iota(jnp.int32, (2, LANES), 0)
    first_half = lax.broadcasted_iota(jnp.int32, (2, LANES), 1) < LANES // 2
    for p in range(half // 2):
        blocks[2 * p : 2 * p + 2] = (
            proj[p * size : (p + 1) * size, : 3 * HEAD].astype(BF16).reshape(2, BLOCK, 3 * HEAD)
        )
        tail = proj[p * size : (p + 1) * size, 3 * HEAD :]
        write = 1.0 / (1.0 + jnp.exp(-tail[:, at_beta : at_beta + 1]))
        pushed = tail[:, at_beta + 1 : at_beta + 2]
        fade = -rate * (jnp.maximum(pushed, 0.0) + jnp.log1p(jnp.exp(-jnp.abs(pushed))))
        write_row = jnp.sum(jnp.where(eye, write, 0.0), axis=0, keepdims=True)
        fade_row = jnp.sum(jnp.where(same & (row <= col), fade, 0.0), axis=0, keepdims=True)
        both_rows = jnp.where(line == 0, write_row, fade_row)
        rolled = pltpu.roll(both_rows, LANES // 2, 1)
        lines_out[2 * p] = jnp.where(
            even, jnp.where(first_half, both_rows, 0.0), jnp.where(first_half, 0.0, rolled)
        )
        lines_out[2 * p + 1] = jnp.where(
            even, jnp.where(first_half, rolled, 0.0), jnp.where(first_half, 0.0, both_rows)
        )

    def send_lane(i):
        s = lax.rem(zl + i, half)
        where = {"sp": s + half * (1 - t), "tp": zh}
        begin(remote(lines_out.at[s], gr.at[zl], g_send.at[i], g_recv.at[zl], where))
        begin(remote(blocks.at[s], dr.at[zl], d_send.at[i], d_recv.at[zl], where))

    send_lane(0)
    send_lane(1)

    for k, (dx, dt, fx, to, back) in enumerate(near):
        slot = lr.at[2 * back + to]
        remote(slot, slot, a_send.at[k], a_recv.at[k], {"fs": back, "tp": to}).wait_recv()
    own_l.wait()

    lane = lax.broadcasted_iota(jnp.int32, (rows, LANES), 1)
    far_cos, far_sin = far_ref[0, pl.ds(z, 1), :], far_ref[1, pl.ds(z, 1), :]
    near_cos = jnp.concatenate([near_ref[0]] * count, axis=0)
    near_sin = jnp.concatenate([near_ref[1]] * count, axis=0)
    cosine = far_cos * near_cos - far_sin * near_sin
    sine = far_sin * near_cos + far_cos * near_sin
    slab = mm(lr[0], place[0])
    for c in range(1, cores):
        slab = slab + mm(lr[c], place[c])
    kv_lat = slab[:, :kv_total]
    kv_lat = kv_lat * lax.rsqrt(jnp.mean(kv_lat * kv_lat, axis=-1, keepdims=True) + NORM_EPS)
    turned = slab[:, kv_total : kv_total + LANES] * cosine + slab[:, kv_total + LANES :] * sine
    latent_keys = (kv_lat * kvgain_ref[...]).astype(BF16)
    groups = LANES // ROPE
    short = BLOCK // groups
    in_group = lax.broadcasted_iota(jnp.int32, (short, LANES), 1) // ROPE
    for s in range(count):
        kvg[s, z, 0:BLOCK] = latent_keys[s * BLOCK : (s + 1) * BLOCK]
        tight = jnp.zeros((short, LANES), F32)
        for g in range(groups):
            at = s * BLOCK + g * short
            tight = jnp.where(in_group == g, turned[at : at + short], tight)
        kvg[s, z, BLOCK : BLOCK + short] = jnp.concatenate(
            [tight, jnp.zeros((short, kv_total - LANES), F32)], axis=1
        ).astype(BF16)

    def key_right(distance, slot):
        hop = 2 - distance % 2
        sems = kr_send.at[distance - 1], kr_recv.at[distance - 1]
        return remote(kvg.at[t, slot], kvg.at[t, slot], *sems, {"sp": lax.rem(z + hop, nz)})

    def key_left(distance, slot):
        hop = 2 - distance % 2
        sems = kl_send.at[distance - 1], kl_recv.at[distance - 1]
        return remote(kvg.at[t, slot], kvg.at[t, slot], *sems, {"sp": lax.rem(z + nz - hop, nz)})

    def across(slot, k):
        return remote(kvg.at[t, slot], kvg.at[t, slot], kp_send.at[k], kp_recv.at[k], partner)

    for distance in (2, 1):
        begin(key_right(distance, z))
        begin(key_left(distance, z))

    q_lat = jnp.concatenate(
        [
            jnp.where(
                lane < LANES // 2,
                lr[c].astype(F32),
                pltpu.roll(lr[c + 1].astype(F32), LANES // 2, 1),
            )
            for c in range(0, cores, 2)
        ],
        axis=1,
    )
    q_lat = q_lat * lax.rsqrt(jnp.mean(q_lat * q_lat, axis=-1, keepdims=True) + NORM_EPS)
    query = mm(q_lat * qgain_ref[...], qup_ref[...]).astype(BF16).astype(F32)
    head_width = NOPE + ROPE
    heads = query.shape[1] // head_width
    entry = lax.rem(col, ROPE)
    repeat = ones(row == NOPE + entry)
    exchange = jnp.where((entry >= ROPE // 2) & (row == NOPE + entry - ROPE // 2), 1.0, 0.0)
    exchange = exchange - ones((entry < ROPE // 2) & (row == NOPE + entry + ROPE // 2))
    stacked = [[] for _ in range(count)]
    for h in range(heads):
        own = query[:, h * head_width : (h + 1) * head_width]
        own = jnp.concatenate([own, jnp.zeros((rows, LANES - head_width), F32)], axis=1)
        absorbed = mm_nt(
            jnp.where(lane < NOPE, own, 0.0), lup_ref[:, h * LANES : (h + 1) * LANES]
        )
        turn = mm(own, repeat) * cosine + mm(own, exchange) * sine
        joined = jnp.concatenate([absorbed, turn], axis=1).astype(BF16)
        for s in range(count):
            stacked[s].append(joined[s * BLOCK : (s + 1) * BLOCK])

    for turn_at in range(reach_r // 2):
        for i in (2 * turn_at + 2, 2 * turn_at + 3):
            if i < half:
                send_lane(i)
        for distance in (2 * turn_at + 2, 2 * turn_at + 1):
            from_left = lax.rem(z + nz - distance, nz)
            from_right = lax.rem(z + distance, nz)
            key_right(distance, from_left).wait_recv()
            if distance % 2 == 0:
                for further in (distance + 2, distance + 1):
                    if further <= reach_r:
                        begin(key_right(further, from_left))
            begin(across(from_left, distance - 1))
            if distance <= reach_l:
                key_left(distance, from_right).wait_recv()
                if distance % 2 == 0:
                    for further in (distance + 2, distance + 1):
                        if further <= reach_l:
                            begin(key_left(further, from_right))
                begin(across(from_right, reach_r + distance - 1))
        if turn_at == reach_r // 2 - 2:
            behind, ahead = lax.rem(x + nx - 1, nx), lax.rem(x + 1, nx)
            remote(w_part(behind, 0), w_part(behind, 0), w_send.at[0], w_recv.at[0], west).wait_recv()
            begin(remote(w_part(behind, 0), w_part(behind, 0), w_send.at[4], w_recv.at[4], east))
            remote(w_part(ahead, 1), w_part(ahead, 1), w_send.at[1], w_recv.at[1], east).wait_recv()
            begin(remote(w_part(ahead, 1), w_part(ahead, 1), w_send.at[5], w_recv.at[5], west))

    for j in range(half):
        where = {"sp": half * t + j, "tp": 1 - zh}
        remote(gr.at[j], gr.at[j], g_send.at[j], g_recv.at[j], where).wait_recv()
        remote(dr.at[j], dr.at[j], d_send.at[j], d_recv.at[j], where).wait_recv()

    strict = same & (row > col)
    causal = same & (row >= col)
    wide_row = lax.broadcasted_iota(jnp.int32, (size, 2 * size), 0)

    def upright(line, where):
        return jnp.sum(jnp.where(where, line, 0.0), axis=1, keepdims=True)

    pairs_at = range(half // 2)
    raws = [dr[2 * p : 2 * p + 2].reshape(size, 3 * HEAD).astype(F32) for p in pairs_at]
    qs = [unit(swish(raw[:, :HEAD])) * HEAD**-0.5 for raw in raws]
    ks = [unit(swish(raw[:, HEAD : 2 * HEAD])) for raw in raws]
    vs = [swish(raw[:, 2 * HEAD :]) for raw in raws]
    marks = [gr[2 * p] + gr[2 * p + 1] for p in pairs_at]
    betas = [upright(mark[0:1], eye) for mark in marks]
    sums = [upright(mark[1:2], eye) for mark in marks]
    ends = [
        upright(mark[1:2], col == (row // BLOCK) * BLOCK + BLOCK - 1) for mark in marks
    ]
    decays = [
        jnp.exp(jnp.where(causal, upon - mark[1:2], 0.0)) for upon, mark in zip(sums, marks)
    ]
    lowers = [
        jnp.where(strict, beta * mm_nt(k, k) * decay, 0.0)
        for beta, k, decay in zip(betas, ks, decays)
    ]
    inverses = [
        jnp.where(eye, 1.0, 0.0) - jnp.where((row // 2 == col // 2), low, 0.0) for low in lowers
    ]
    level = 2
    while level < BLOCK:
        pick = (row // (2 * level) == col // (2 * level)) & (row // level != col // level)
        firsts = [mm(inv, jnp.where(pick, low, 0.0)) for inv, low in zip(inverses, lowers)]
        inverses = [inv - mm(first, inv) for first, inv in zip(firsts, inverses)]
        level *= 2
    scores_of = [
        jnp.where(causal, mm_nt(q, k) * decay, 0.0) for q, k, decay in zip(qs, ks, decays)
    ]
    boths = [
        mm(inv, jnp.concatenate([beta * v, beta * k * jnp.exp(upon)], axis=1))
        for inv, beta, v, k, upon in zip(inverses, betas, vs, ks, sums)
    ]
    keys_t = [(k * jnp.exp(end - upon)).T for k, end, upon in zip(ks, ends, sums)]
    moves_of = [
        [mm(key_t, jnp.where(wide_row // BLOCK == h, both, 0.0)) for h in range(2)]
        for key_t, both in zip(keys_t, boths)
    ]
    terms = [
        (
            qs[p] * jnp.exp(sums[p]),
            scores_of[p],
            boths[p],
            moves_of[p],
            [jnp.exp(ends[p][h * BLOCK : h * BLOCK + 1]) for h in range(2)],
        )
        for p in pairs_at
    ]

    total = jnp.concatenate([jnp.zeros((size, size), F32), jnp.where(eye, 1.0, 0.0)], axis=1)
    states = []
    for j in range(half):
        states.append(total)
        move, factor = terms[j // 2][3][j % 2], terms[j // 2][4][j % 2]
        grown = factor * total - mm(move[:, size:], total)
        total = jnp.concatenate([grown[:, :size] + move[:, :size], grown[:, size:]], axis=1)

    state_out[...] = total[:, :size]
    crossing = remote(state_out, state_in, st_send.at[0], st_recv.at[0], partner)

    @pl.when(t == 0)
    def _():
        state_in[...] = jnp.zeros_like(state_in)
        crossing.start()

    @pl.when(t == 1)
    def _():
        crossing.wait_recv()

    start = state_in[...]
    for p in range(half // 2):
        queries, scores, both, _, _ = terms[p]
        read, fixed = [], []
        for h in range(2):
            j = 2 * p + h
            state = states[j][:, :size] + mm(states[j][:, size:], start)
            cut = slice(h * BLOCK, (h + 1) * BLOCK)
            got = mm(jnp.concatenate([both[cut, size:], queries[cut]], axis=0), state)
            fixed.append(both[cut, :size] - got[:BLOCK])
            read.append(got[BLOCK:])
        raw = jnp.concatenate(read, axis=0) + mm(scores, jnp.concatenate(fixed, axis=0))
        raw = raw * lax.rsqrt(jnp.mean(raw * raw, axis=-1, keepdims=True) + NORM_EPS)
        done = (raw * dgain_ref[...]).astype(BF16)
        ready[2 * p] = done[:BLOCK]
        ready[2 * p + 1] = done[BLOCK:]

    for i in range(half):
        j = lax.rem(zl + i, half)
        begin(
            remote(
                ready.at[j],
                homed.at[lax.rem(zl, 2), x],
                h_send.at[i],
                h_recv.at[lax.rem(zl, 2), x],
                {"fs": zl // 2, "sp": half * t + j, "tp": lane_t},
            )
        )

    for k in range(nz - 1):
        slot = kvg.at[1 - t, lax.rem(z + 1, nz)]
        remote(slot, slot, kp_send.at[k], kp_recv.at[k], partner).wait_recv()
    allowed = lax.broadcasted_iota(jnp.int32, (1, nz * BLOCK), 1) < (z + 1) * BLOCK
    rope_group = lax.broadcasted_iota(jnp.int32, (nz, short, LANES), 2) // ROPE
    outs = []
    low = lax.broadcasted_iota(jnp.int32, (BLOCK, LANES), 1) < LANES // 2
    for s in range(count):
        tight = kvg[s, :, BLOCK : BLOCK + short, :LANES].astype(F32)
        spread = [jnp.where(rope_group == g, tight, 0.0) for g in range(groups)]
        keys = jnp.concatenate(
            [
                kvg[s, :, 0:BLOCK, :].reshape(nz * BLOCK, kv_total),
                jnp.concatenate(spread, axis=1).reshape(nz * BLOCK, LANES).astype(BF16),
            ],
            axis=1,
        )
        scores = mm_nt(jnp.concatenate(stacked[s], axis=0), keys) * (NOPE + ROPE) ** (-0.5)
        scores = jnp.where(allowed, scores, -1e30)
        peak = jnp.max(scores, axis=-1, keepdims=True)
        weights = jnp.where(allowed, jnp.exp(scores - peak), 0.0)
        total = jnp.sum(weights, axis=-1, keepdims=True)
        mixed = (mm(weights, keys[:, :kv_total]) / total).astype(BF16)
        made = [
            mm(mixed[h * BLOCK : (h + 1) * BLOCK], lup_ref[:, h * LANES : (h + 1) * LANES])
            for h in range(heads)
        ]
        pairs = [
            jnp.where(low, pltpu.roll(made[h], LANES // 2, 1), made[h + 1]).astype(BF16)
            for h in range(0, heads, 2)
        ]
        outs.append(jnp.concatenate(pairs, axis=1))
    latent_heads = jnp.concatenate(outs, axis=0)

    own_c.wait()
    for k, owner, upper in (
        (2, lax.rem(x + nx - 1, nx), 1),
        (3, lax.rem(x + 1, nx), 0),
        (4, lax.rem(x + 2, nx), 0),
        (5, lax.rem(x + 2, nx), 1),
    ):
        remote(
            w_part(owner, upper), w_part(owner, upper), w_send.at[k], w_recv.at[k], east
        ).wait_recv()
    for sl in range(2):
        for xl in range(nx):
            slot = homed.at[sl, xl]
            where = {"fs": xl, "sp": 2 * x + sl + half * (1 - t), "tp": zh}
            remote(slot, slot, h_send.at[0], h_recv.at[sl, xl], where).wait_recv()
    delta_heads = [homed[:, xl].reshape(rows, HEAD) for xl in range(nx)]
    joined = jnp.concatenate(delta_heads + [latent_heads], axis=1)
    width = wo.shape[0] * wo.shape[1] * wo.shape[2]
    columns = wo[...].reshape(width, wo.shape[3])
    part_out[...] = mm_nt(joined, columns).astype(BF16)
    swap_parts = begin(remote(part_out, part_in, p_send.at[0], p_recv.at[0], partner))
    swap_parts.wait_recv()
    whole = part_out[...].astype(F32) + part_in[...].astype(F32)
    scale = lax.rsqrt(jnp.mean(whole * whole, axis=-1, keepdims=True) + NORM_EPS)
    own_half = jnp.where(t == 0, whole[:, : width // 2], whole[:, width // 2 :])
    out_ref[...] = (own_half * scale * post_ref[...]).astype(BF16)

    for copy in started:
        copy.wait_send()

    def drain(step, carry):
        for part in [*range(nx), None]:
            go_right(step, part, z).wait_send()

            @pl.when(step < reach_l)
            def _():
                go_left(step, part, z).wait_send()

        return carry

    lax.fori_loop(0, reach_r, drain, 0)

    @pl.when(t == 0)
    def _():
        crossing.wait_send()


def layer(nz, nx, *operands):
    tokens, query_weight, out_cols, latent_up = (operands[k] for k in (0, 2, 9, 13))
    half = nz // 2
    seqs, length, width = tokens.shape
    rows = seqs * length
    span = query_weight.shape[0]
    dma = pltpu.SemaphoreType.DMA

    def pair(*shape):
        return [dma(shape), dma(shape)]

    specs = [pl.BlockSpec(memory_space=VM)] * len(operands)
    specs[8] = pl.BlockSpec(memory_space=pltpu.SMEM)
    return pl.pallas_call(
        functools.partial(layer_kernel, nz, nx),
        out_shape=jax.ShapeDtypeStruct((rows, width // 2), BF16),
        in_specs=specs,
        out_specs=pl.BlockSpec(memory_space=VM),
        scratch_shapes=[
            VM((seqs * nx, length, width), BF16),
            VM((nx * rows, width), BF16),
            VM((nz, nx * span, 4 * LANES), BF16),
            VM((nz, *out_cols.shape), BF16),
            VM((nx, span, LANES), BF16),
            VM((nx * rows, 4 * LANES), F32),
            VM((2 * nx, LANES, 4 * LANES), BF16),
            VM((half, BLOCK, 3 * HEAD), BF16),
            VM((half, 2, LANES), F32),
            VM((nx, rows, LANES), BF16),
            VM((half, BLOCK, 3 * HEAD), BF16),
            VM((half, 2, LANES), F32),
            VM((2 * nx, rows, LANES), BF16),
            VM((seqs, nz, length + length * ROPE // LANES, latent_up.shape[0]), BF16),
            VM((nz, nx, *out_cols.shape), BF16),
            VM((2, nx, BLOCK, HEAD), BF16),
            VM((half, BLOCK, HEAD), BF16),
            VM((HEAD, HEAD), F32),
            VM((HEAD, HEAD), F32),
            VM((rows, width), BF16),
            VM((rows, width), BF16),
            dma((6,)),
            *pair(nx - 1, 4),
            *pair(nx - 1),
            *pair(nx - 1),
            *pair(half, nx + 1),
            *pair(half - 1, nx + 1),
            *pair(2 * nx - 1),
            *pair(half),
            *pair(half),
            *pair(half),
            *pair(half - 1),
            *pair(nz - 1),
            *pair(6),
            *pair(1),
            dma((half,)),
            dma((2, nx)),
            *pair(1),
        ],
        compiler_params=pltpu.CompilerParams(collective_id=1, has_side_effects=True),
        name="layer",
    )(*operands)


def rope_tables(count, length):
    frequency = ROPE_THETA ** (-np.arange(0, ROPE, 2, dtype=np.float64) / ROPE)
    frequency = np.tile(frequency, LANES // (ROPE // 2))[None, :]

    def both(positions):
        angles = positions[:, None] * frequency
        return np.stack([np.cos(angles), np.sin(angles)]).astype(np.float32)

    return both(np.arange(count) * float(length)), both(np.arange(length) * 1.0)


def local(
    tokens,
    pre_gain,
    query_weight,
    key_weight,
    value_weight,
    beta_weight,
    decay_weight,
    decay_rate,
    delta_gain,
    query_down,
    latent_down,
    rope_weight,
    query_gain,
    latent_gain,
    query_up,
    latent_up,
    delta_out,
    latent_out,
    post_gain,
):
    nz, nx = lax.axis_size("sp"), lax.axis_size("fs")
    z, x = lax.axis_index("sp"), lax.axis_index("fs")
    seq_count, token_count = tokens.shape[:2]
    span = query_weight.shape[0]
    small = jnp.concatenate(
        [
            lax.dynamic_slice_in_dim(array, (z * nx + x) * span, span, 0)
            for array in (rope_weight, beta_weight, decay_weight)
        ],
        axis=1,
    )
    small = jnp.pad(small, ((0, 0), (0, LANES - small.shape[1])))
    out_cols = jnp.concatenate([delta_out, latent_out], axis=0).T
    far, near = rope_tables(nz, token_count)
    result = layer(
        nz,
        nx,
        tokens,
        pre_gain[None],
        query_weight,
        key_weight,
        value_weight,
        query_down,
        latent_down,
        small,
        decay_rate,
        out_cols,
        query_gain[None],
        latent_gain[None],
        query_up,
        latent_up,
        jnp.asarray(far),
        jnp.asarray(near),
        delta_gain[None],
        post_gain[None],
    )
    return result.reshape(seq_count, token_count, result.shape[1])


def solution(mesh):
    return jax.shard_map(
        local,
        mesh=mesh,
        in_specs=(
            P(("grp", "fs"), "sp", None),
            P(),
            P(("sp", "fs"), "tp"),
            P(("sp", "fs"), "tp"),
            P(("sp", "fs"), "tp"),
            P(),
            P(),
            P(),
            P(),
            P(("sp", "fs"), None),
            P(("sp", "fs"), None),
            P(),
            P(),
            P(),
            P(None, "tp"),
            P(None, "tp"),
            P("tp", ("sp", "fs")),
            P("tp", ("sp", "fs")),
            P("tp"),
        ),
        out_specs=P(("grp", "fs"), "sp", "tp"),
        check_vma=False,
    )
```

```python
import functools

import jax
import jax.numpy as jnp
import numpy as np
from jax import lax
from jax.experimental import pallas as pl
from jax.experimental.pallas import tpu as pltpu
from jax.sharding import PartitionSpec as P

HEAD = 128
NOPE = 64
ROPE = 32
VDIM = 64
BLOCK = 64
LANES = 128

NORM_EPS = 1e-06
ROPE_THETA = 10000.0
F32 = jnp.float32
BF16 = jnp.bfloat16
MESH = pl.DeviceIdType.MESH
VM = pltpu.VMEM


def remote(src, dst, send_sem, recv_sem, where):
    return pltpu.make_async_remote_copy(
        src_ref=src,
        dst_ref=dst,
        send_sem=send_sem,
        recv_sem=recv_sem,
        device_id=where,
        device_id_type=MESH,
    )


def greet(places, count):
    barrier = pltpu.get_barrier_semaphore()
    for place in places:
        pl.semaphore_signal(barrier, inc=1, device_id=place, device_id_type=MESH)
    pl.semaphore_wait(barrier, count)


def mm(left, right):
    return lax.dot_general(
        left.astype(BF16), right.astype(BF16), (((1,), (0,)), ((), ())), preferred_element_type=F32
    )


def mm_nt(left, right):
    return lax.dot_general(
        left.astype(BF16), right.astype(BF16), (((1,), (1,)), ((), ())), preferred_element_type=F32
    )


def unit(values):
    return values * lax.rsqrt(jnp.sum(values * values, axis=-1, keepdims=True) + NORM_EPS)


def swish(values):
    return values * (1.0 / (1.0 + jnp.exp(-values)))


def layer_kernel(
    nz, nx, tok_ref, pre_ref, wq_ref, wk_ref, wv_ref, qd_ref, kvd_ref, small_ref, rate_ref, wt_ref,
    qgain_ref, kvgain_ref, qup_ref, lup_ref, far_ref, near_ref, dgain_ref, post_ref, out_ref,
    toks, normed, ws, wz, side, proj, place, blocks, lines_out, latents,
    dr, gr, lr, kvg, wo, homed, ready, state_out, state_in, part_out, part_in,
    loc_sem, wx_send, wx_recv, tok_send, tok_recv, fwd_send, fwd_recv, r_send, r_recv, l_send, l_recv,
    a_send, a_recv, d_send, d_recv, g_send, g_recv, kr_send, kr_recv, kl_send, kl_recv,
    kp_send, kp_recv, w_send, w_recv, v_send, v_recv, st_send, st_recv, h_send, h_recv, p_send, p_recv,
):
    z, x, t = lax.axis_index("sp"), lax.axis_index("fs"), lax.axis_index("tp")
    half = nz // 2
    zh, zl = z // half, lax.rem(z, half)
    lane_t = 1 - zh
    cores = 2 * nx
    span = wq_ref.shape[0]
    rows = tok_ref.shape[0] * tok_ref.shape[1]
    count = rows // BLOCK
    partner = {"tp": 1 - t}
    near = [
        (dx, dt, lax.rem(x + dx, nx), lax.rem(t + dt, 2), lax.rem(x + nx - dx, nx))
        for dx in range(nx)
        for dt in range(2)
        if dx or dt
    ]
    others = [lax.rem(x + d, nx) for d in range(1, nx)]
    right, left = {"sp": lax.rem(z + 1, nz)}, {"sp": lax.rem(z + nz - 1, nz)}
    east, west = {"fs": lax.rem(x + 1, nx)}, {"fs": lax.rem(x + nx - 1, nx)}
    sources = [{"fs": back, "tp": to} for dx, dt, fx, to, back in near]
    sources += [{"sp": lax.rem(z + hop, nz)} for hop in (1, 2, nz - 2, nz - 1)]
    sources += [{"sp": half * t + j, "tp": 1 - zh} for j in range(half)]
    sources += [
        {"fs": xl, "sp": 2 * x + sl + half * (1 - t), "tp": zh} for sl in range(2) for xl in range(nx)
    ]
    greet(sources, len(sources))
    started = []

    def begin(copy):
        copy.start()
        started.append(copy)
        return copy

    def local(src, dst, k):
        copy = pltpu.make_async_copy(src, dst, loc_sem.at[k])
        copy.start()
        return copy

    def chunk(slot, part):
        if part is None:
            return wz.at[slot]
        return ws.at[slot, pl.ds(pl.multiple_of(part * span, span), span)]

    def piece(k):
        return ws.at[z, pl.ds(pl.multiple_of(x * span, span), span), pl.ds(k * LANES, LANES)]

    def columns_of(ref, owner):
        return ref.at[:, pl.ds(pl.multiple_of(owner * LANES, LANES), LANES)]

    mains = (wq_ref, wk_ref, wv_ref)
    for d, o in enumerate(others):
        for k, ref in enumerate(mains):
            begin(
                remote(columns_of(ref, o), piece(k), wx_send.at[d, k], wx_recv.at[d, k], {"fs": o})
            )
    own_w = [local(columns_of(ref, x), piece(k), k) for k, ref in enumerate(mains)]
    own_o = local(wt_ref, wz.at[z], 3)
    own_t = local(tok_ref, toks.at[pl.ds(2 * x, 2)], 4)

    reach_r, reach_l = nz // 2, nz // 2 - 1

    def go_right(step, part, slot):
        mark = nx if part is None else part
        return remote(
            chunk(slot, part), chunk(slot, part), r_send.at[step, mark], r_recv.at[step, mark], right
        )

    def go_left(step, part, slot):
        mark = nx if part is None else part
        return remote(
            chunk(slot, part), chunk(slot, part), l_send.at[step, mark], l_recv.at[step, mark], left
        )

    own_o.wait()
    go_right(0, None, z).start()
    go_left(0, None, z).start()

    q_width, kv_width = qd_ref.shape[1] // cores, kvd_ref.shape[1] // cores
    rope_width = ROPE // cores
    at_rope = q_width + kv_width
    at_beta = at_rope + rope_width

    def picked(source, lane, first, stop, start):
        return (lane >= first) & (lane < stop) & (source == start + lane - first)

    def ones(mask):
        return jnp.where(mask, 1.0, 0.0)

    def iotas(depth):
        shape = (depth, LANES)
        return lax.broadcasted_iota(jnp.int32, shape, 0), lax.broadcasted_iota(jnp.int32, shape, 1)

    for o in range(nx):
        core, head = 2 * o + t, nx * t + o
        source, lane = iotas(qd_ref.shape[1])
        made = mm(qd_ref[...], ones(picked(source, lane, 0, q_width, q_width * core)))
        source, lane = iotas(kvd_ref.shape[1])
        made += mm(kvd_ref[...], ones(picked(source, lane, q_width, at_rope, kv_width * core)))
        source, lane = iotas(LANES)
        select = picked(source, lane, at_rope, at_beta, rope_width * core)
        select = select | picked(source, lane, at_beta, at_beta + 1, ROPE + head)
        select = select | picked(source, lane, at_beta + 1, at_beta + 2, ROPE + cores + head)
        made += mm(small_ref[...], ones(select))
        side[o] = made.astype(BF16)
    for d, o in enumerate(others):
        k = len(mains)
        begin(remote(side.at[o], piece(k), wx_send.at[d, k], wx_recv.at[d, k], {"fs": o}))
    own_w.append(local(side.at[x], piece(len(mains)), 5))
    for d, o in enumerate(others):
        begin(remote(tok_ref.at[t], toks.at[2 * x + t], tok_send.at[d], tok_recv.at[d], {"fs": o}))

    for d in range(nx):
        part = lax.rem(x + nx - d, nx)
        if d == 0:
            for copy in own_w:
                copy.wait()
        else:
            for k in range(len(mains) + 1):
                remote(
                    piece(k), piece(k), wx_send.at[d - 1, k], wx_recv.at[d - 1, k], {"fs": part}
                ).wait_recv()
        go_right(0, part, z).start()
        go_left(0, part, z).start()

    from_lane = lax.broadcasted_iota(jnp.int32, (LANES, 4 * LANES), 0)
    to_lane = lax.broadcasted_iota(jnp.int32, (LANES, 4 * LANES), 1)
    kv_total = kv_width * cores
    spot = to_lane - kv_total
    spot_in = lax.rem(to_lane, ROPE)
    sign = jnp.where(spot_in < ROPE // 2, -1.0, 1.0)
    is_kv = (from_lane >= q_width) & (from_lane < at_rope)
    is_rope = (from_lane >= at_rope) & (from_lane < at_beta)
    for c in range(cores):
        entry = from_lane - at_rope + rope_width * c
        kept = is_kv & (to_lane == from_lane - q_width + kv_width * c)
        straight = is_rope & (spot >= 0) & (spot < LANES) & (spot_in == entry)
        swapped = is_rope & (spot >= LANES) & (lax.rem(spot_in + ROPE // 2, ROPE) == entry)
        place[c] = (ones(kept | straight) + jnp.where(swapped, sign, 0.0)).astype(BF16)

    early = (reach_r * 5) // 8

    def columns_on(slot):
        for k, where in enumerate((east, west)):
            remote(wz.at[slot], wo.at[slot, x], w_send.at[k, slot], w_recv.at[k, slot], where).start()

    def columns_step(step):
        from_left = lax.rem(z + 2 * nz - 1 - step, nz)
        from_right = lax.rem(z + 1 + step, nz)
        go_right(step, None, from_left).wait_recv()
        columns_on(from_left)

        @pl.when(step < reach_r - 1)
        def _():
            go_right(step + 1, None, from_left).start()

        @pl.when(step < reach_l)
        def _():
            go_left(step, None, from_right).wait_recv()
            columns_on(from_right)

        @pl.when(step < reach_l - 1)
        def _():
            go_left(step + 1, None, from_right).start()

    def weights_step(step):
        from_left = lax.rem(z + 2 * nz - 1 - step, nz)
        from_right = lax.rem(z + 1 + step, nz)
        for d in range(nx):
            part = lax.rem(x + nx - d, nx)
            go_right(step, part, from_left).wait_recv()

            @pl.when(step < reach_r - 1)
            def _():
                go_right(step + 1, part, from_left).start()

            @pl.when(step < reach_l)
            def _():
                go_left(step, part, from_right).wait_recv()

            @pl.when(step < reach_l - 1)
            def _():
                go_left(step + 1, part, from_right).start()

    def ring(step, carry):
        columns_step(step)
        weights_step(step)
        return carry

    columns_on(z)
    lax.fori_loop(0, early, ring, 0)
    own_t.wait()
    for d in range(nx - 1):
        held = toks.at[2 * lax.rem(x + nx - 1 - d, nx) + t]
        remote(held, held, tok_send.at[d], tok_recv.at[d], partner).wait_recv()
        begin(remote(held, held, fwd_send.at[d], fwd_recv.at[d], partner))
    lax.fori_loop(early, early + 1, ring, 0)
    for d in range(nx - 1):
        held = toks.at[2 * lax.rem(x + nx - 1 - d, nx) + 1 - t]
        remote(held, held, fwd_send.at[d], fwd_recv.at[d], partner).wait_recv()

    def normalize(i, carry):
        values = toks[i].astype(F32)
        scale = lax.rsqrt(jnp.mean(values * values, axis=-1, keepdims=True) + NORM_EPS)
        normed[pl.ds(pl.multiple_of(i * BLOCK, BLOCK), BLOCK), :] = (
            values * scale * pre_ref[...]
        ).astype(BF16)
        return carry

    lax.fori_loop(0, toks.shape[0], normalize, 0)
    lax.fori_loop(early + 1, reach_r - 1, ring, 0)
    depth = ws.shape[1]

    def product(slot):
        lhs = normed[:, pl.ds(pl.multiple_of(slot * depth, depth), depth)]
        return lax.dot_general(lhs, ws[slot], (((1,), (0,)), ((), ())), preferred_element_type=F32)

    def gather_product(i, carry):
        proj[...] += product(lax.rem(z + nz - reach_l + i, nz))
        return carry

    proj[...] = product(z + 0)
    lax.fori_loop(0, reach_l, gather_product, 0)
    lax.fori_loop(reach_l + 1, 2 * reach_l + 1, gather_product, 0)
    lax.fori_loop(reach_r - 1, reach_r, ring, 0)
    proj[...] += product(lax.rem(z + reach_r, nz))

    for o in range(nx):
        latents[o] = proj[o * rows : (o + 1) * rows, 3 * HEAD :].astype(BF16)
    own_l = local(latents.at[x], lr.at[2 * x + t], 0)
    for k, (dx, dt, fx, to, back) in enumerate(near):
        begin(
            remote(latents.at[fx], lr.at[2 * x + t], a_send.at[k], a_recv.at[k], {"fs": fx, "tp": to})
        )

    def w_part(owner, upper):
        return wo.at[pl.ds(half * upper, half), owner]

    size = 2 * BLOCK
    row = lax.broadcasted_iota(jnp.int32, (size, size), 0)
    col = lax.broadcasted_iota(jnp.int32, (size, size), 1)
    eye = row == col
    same = (row // BLOCK) == (col // BLOCK)
    rate = rate_ref[nx * t + x]
    even = lax.rem(z, 2) == 0
    line = lax.broadcasted_iota(jnp.int32, (2, LANES), 0)
    first_half = lax.broadcasted_iota(jnp.int32, (2, LANES), 1) < LANES // 2
    for p in range(half // 2):
        blocks[2 * p : 2 * p + 2] = (
            proj[p * size : (p + 1) * size, : 3 * HEAD].astype(BF16).reshape(2, BLOCK, 3 * HEAD)
        )
        tail = proj[p * size : (p + 1) * size, 3 * HEAD :]
        write = 1.0 / (1.0 + jnp.exp(-tail[:, at_beta : at_beta + 1]))
        pushed = tail[:, at_beta + 1 : at_beta + 2]
        fade = -rate * (jnp.maximum(pushed, 0.0) + jnp.log1p(jnp.exp(-jnp.abs(pushed))))
        write_row = jnp.sum(jnp.where(eye, write, 0.0), axis=0, keepdims=True)
        fade_row = jnp.sum(jnp.where(same & (row <= col), fade, 0.0), axis=0, keepdims=True)
        both_rows = jnp.where(line == 0, write_row, fade_row)
        rolled = pltpu.roll(both_rows, LANES // 2, 1)
        lines_out[2 * p] = jnp.where(
            even, jnp.where(first_half, both_rows, 0.0), jnp.where(first_half, 0.0, rolled)
        )
        lines_out[2 * p + 1] = jnp.where(
            even, jnp.where(first_half, rolled, 0.0), jnp.where(first_half, 0.0, both_rows)
        )

    def send_lane(i):
        s = lax.rem(zl + i, half)
        where = {"sp": s + half * (1 - t), "tp": zh}
        begin(remote(lines_out.at[s], gr.at[zl], g_send.at[i], g_recv.at[zl], where))
        begin(remote(blocks.at[s], dr.at[zl], d_send.at[i], d_recv.at[zl], where))

    for i in range(half):
        send_lane(i)

    for k, (dx, dt, fx, to, back) in enumerate(near):
        slot = lr.at[2 * back + to]
        remote(slot, slot, a_send.at[k], a_recv.at[k], {"fs": back, "tp": to}).wait_recv()
    own_l.wait()

    lane = lax.broadcasted_iota(jnp.int32, (rows, LANES), 1)
    far_cos, far_sin = far_ref[0, pl.ds(z, 1), :], far_ref[1, pl.ds(z, 1), :]
    near_cos = jnp.concatenate([near_ref[0]] * count, axis=0)
    near_sin = jnp.concatenate([near_ref[1]] * count, axis=0)
    cosine = far_cos * near_cos - far_sin * near_sin
    sine = far_sin * near_cos + far_cos * near_sin
    slab = mm(lr[0], place[0])
    for c in range(1, cores):
        slab = slab + mm(lr[c], place[c])
    kv_lat = slab[:, :kv_total]
    kv_lat = kv_lat * lax.rsqrt(jnp.mean(kv_lat * kv_lat, axis=-1, keepdims=True) + NORM_EPS)
    turned = slab[:, kv_total : kv_total + LANES] * cosine + slab[:, kv_total + LANES :] * sine
    latent_keys = (kv_lat * kvgain_ref[...]).astype(BF16)
    groups = LANES // ROPE
    short = BLOCK // groups
    in_group = lax.broadcasted_iota(jnp.int32, (short, LANES), 1) // ROPE
    for s in range(count):
        kvg[s, z, 0:BLOCK] = latent_keys[s * BLOCK : (s + 1) * BLOCK]
        tight = jnp.zeros((short, LANES), F32)
        for g in range(groups):
            at = s * BLOCK + g * short
            tight = jnp.where(in_group == g, turned[at : at + short], tight)
        kvg[s, z, BLOCK : BLOCK + short] = jnp.concatenate(
            [tight, jnp.zeros((short, kv_total - LANES), F32)], axis=1
        ).astype(BF16)

    def key_right(distance, slot):
        hop = 2 - distance % 2
        sems = kr_send.at[distance - 1], kr_recv.at[distance - 1]
        return remote(kvg.at[t, slot], kvg.at[t, slot], *sems, {"sp": lax.rem(z + hop, nz)})

    def key_left(distance, slot):
        hop = 2 - distance % 2
        sems = kl_send.at[distance - 1], kl_recv.at[distance - 1]
        return remote(kvg.at[t, slot], kvg.at[t, slot], *sems, {"sp": lax.rem(z + nz - hop, nz)})

    def across(slot, k):
        return remote(kvg.at[t, slot], kvg.at[t, slot], kp_send.at[k], kp_recv.at[k], partner)

    for distance in (2, 1):
        begin(key_right(distance, z))
        begin(key_left(distance, z))

    q_lat = jnp.concatenate(
        [
            jnp.where(
                lane < LANES // 2,
                lr[c].astype(F32),
                pltpu.roll(lr[c + 1].astype(F32), LANES // 2, 1),
            )
            for c in range(0, cores, 2)
        ],
        axis=1,
    )
    q_lat = q_lat * lax.rsqrt(jnp.mean(q_lat * q_lat, axis=-1, keepdims=True) + NORM_EPS)
    query = mm(q_lat * qgain_ref[...], qup_ref[...]).astype(BF16).astype(F32)
    head_width = NOPE + ROPE
    heads = query.shape[1] // head_width
    entry = lax.rem(col, ROPE)
    repeat = ones(row == NOPE + entry)
    exchange = jnp.where((entry >= ROPE // 2) & (row == NOPE + entry - ROPE // 2), 1.0, 0.0)
    exchange = exchange - ones((entry < ROPE // 2) & (row == NOPE + entry + ROPE // 2))
    stacked = [[] for _ in range(count)]
    for h in range(heads):
        own = query[:, h * head_width : (h + 1) * head_width]
        own = jnp.concatenate([own, jnp.zeros((rows, LANES - head_width), F32)], axis=1)
        absorbed = mm_nt(
            jnp.where(lane < NOPE, own, 0.0), lup_ref[:, h * LANES : (h + 1) * LANES]
        )
        turn = mm(own, repeat) * cosine + mm(own, exchange) * sine
        joined = jnp.concatenate([absorbed, turn], axis=1).astype(BF16)
        for s in range(count):
            stacked[s].append(joined[s * BLOCK : (s + 1) * BLOCK])

    own_c = local(wz, wo.at[:, x], 1)
    behind, ahead = lax.rem(x + nx - 1, nx), lax.rem(x + 1, nx)

    def arrived(k, first, owner):
        def one(slot, carry):
            held = wo.at[slot, owner]
            remote(held, held, w_send.at[k, slot], w_recv.at[k, slot], east).wait_recv()
            return carry

        lax.fori_loop(first, first + half, one, 0)

    def key_turn(turn_at):
        for distance in (2 * turn_at + 2, 2 * turn_at + 1):
            from_left = lax.rem(z + nz - distance, nz)
            from_right = lax.rem(z + distance, nz)
            key_right(distance, from_left).wait_recv()
            if distance % 2 == 0:
                for further in (distance + 2, distance + 1):
                    if further <= reach_r:
                        begin(key_right(further, from_left))
            begin(across(from_left, distance - 1))
            if distance <= reach_l:
                key_left(distance, from_right).wait_recv()
                if distance % 2 == 0:
                    for further in (distance + 2, distance + 1):
                        if further <= reach_l:
                            begin(key_left(further, from_right))
                begin(across(from_right, reach_r + distance - 1))

    key_turn(0)
    arrived(0, 0, behind)
    begin(remote(w_part(behind, 0), w_part(behind, 0), v_send.at[0], v_recv.at[0], east))
    arrived(1, half, ahead)
    begin(remote(w_part(ahead, 1), w_part(ahead, 1), v_send.at[1], v_recv.at[1], west))

    for j in range(half):
        where = {"sp": half * t + j, "tp": 1 - zh}
        remote(gr.at[j], gr.at[j], g_send.at[j], g_recv.at[j], where).wait_recv()
        remote(dr.at[j], dr.at[j], d_send.at[j], d_recv.at[j], where).wait_recv()

    strict = same & (row > col)
    causal = same & (row >= col)
    wide_row = lax.broadcasted_iota(jnp.int32, (size, 2 * size), 0)

    def upright(line, where):
        return jnp.sum(jnp.where(where, line, 0.0), axis=1, keepdims=True)

    pairs_at = range(half // 2)
    raws = [dr[2 * p : 2 * p + 2].reshape(size, 3 * HEAD).astype(F32) for p in pairs_at]
    qs = [unit(swish(raw[:, :HEAD])) * HEAD**-0.5 for raw in raws]
    ks = [unit(swish(raw[:, HEAD : 2 * HEAD])) for raw in raws]
    vs = [swish(raw[:, 2 * HEAD :]) for raw in raws]
    marks = [gr[2 * p] + gr[2 * p + 1] for p in pairs_at]
    betas = [upright(mark[0:1], eye) for mark in marks]
    sums = [upright(mark[1:2], eye) for mark in marks]
    ends = [
        upright(mark[1:2], col == (row // BLOCK) * BLOCK + BLOCK - 1) for mark in marks
    ]
    decays = [
        jnp.exp(jnp.where(causal, upon - mark[1:2], 0.0)) for upon, mark in zip(sums, marks)
    ]
    lowers = [
        jnp.where(strict, beta * mm_nt(k, k) * decay, 0.0)
        for beta, k, decay in zip(betas, ks, decays)
    ]
    inverses = [
        jnp.where(eye, 1.0, 0.0) - jnp.where((row // 2 == col // 2), low, 0.0) for low in lowers
    ]
    level = 2
    while level < BLOCK:
        pick = (row // (2 * level) == col // (2 * level)) & (row // level != col // level)
        firsts = [mm(inv, jnp.where(pick, low, 0.0)) for inv, low in zip(inverses, lowers)]
        inverses = [inv - mm(first, inv) for first, inv in zip(firsts, inverses)]
        level *= 2
    scores_of = [
        jnp.where(causal, mm_nt(q, k) * decay, 0.0) for q, k, decay in zip(qs, ks, decays)
    ]
    boths = [
        mm(inv, jnp.concatenate([beta * v, beta * k * jnp.exp(upon)], axis=1))
        for inv, beta, v, k, upon in zip(inverses, betas, vs, ks, sums)
    ]
    keys_t = [(k * jnp.exp(end - upon)).T for k, end, upon in zip(ks, ends, sums)]
    moves_of = [
        [mm(key_t, jnp.where(wide_row // BLOCK == h, both, 0.0)) for h in range(2)]
        for key_t, both in zip(keys_t, boths)
    ]
    terms = [
        (
            qs[p] * jnp.exp(sums[p]),
            scores_of[p],
            boths[p],
            moves_of[p],
            [jnp.exp(ends[p][h * BLOCK : h * BLOCK + 1]) for h in range(2)],
        )
        for p in pairs_at
    ]

    key_turn(1)
    total = jnp.concatenate([jnp.zeros((size, size), F32), jnp.where(eye, 1.0, 0.0)], axis=1)
    states = []
    for j in range(half):
        states.append(total)
        move, factor = terms[j // 2][3][j % 2], terms[j // 2][4][j % 2]
        grown = factor * total - mm(move[:, size:], total)
        total = jnp.concatenate([grown[:, :size] + move[:, :size], grown[:, size:]], axis=1)

    state_out[...] = total[:, :size]
    crossing = remote(state_out, state_in, st_send.at[0], st_recv.at[0], partner)

    @pl.when(t == 0)
    def _():
        state_in[...] = jnp.zeros_like(state_in)
        crossing.start()

    key_turn(2)

    @pl.when(t == 1)
    def _():
        crossing.wait_recv()

    start = state_in[...]
    for p in range(half // 2):
        queries, scores, both, _, _ = terms[p]
        read, fixed = [], []
        for h in range(2):
            j = 2 * p + h
            state = states[j][:, :size] + mm(states[j][:, size:], start)
            cut = slice(h * BLOCK, (h + 1) * BLOCK)
            got = mm(jnp.concatenate([both[cut, size:], queries[cut]], axis=0), state)
            fixed.append(both[cut, :size] - got[:BLOCK])
            read.append(got[BLOCK:])
        raw = jnp.concatenate(read, axis=0) + mm(scores, jnp.concatenate(fixed, axis=0))
        raw = raw * lax.rsqrt(jnp.mean(raw * raw, axis=-1, keepdims=True) + NORM_EPS)
        done = (raw * dgain_ref[...]).astype(BF16)
        ready[2 * p] = done[:BLOCK]
        ready[2 * p + 1] = done[BLOCK:]

    for i in range(half):
        j = lax.rem(zl + i, half)
        begin(
            remote(
                ready.at[j],
                homed.at[lax.rem(zl, 2), x],
                h_send.at[i],
                h_recv.at[lax.rem(zl, 2), x],
                {"fs": zl // 2, "sp": half * t + j, "tp": lane_t},
            )
        )

    for turn_at in range(3, reach_r // 2):
        key_turn(turn_at)
    for k in range(nz - 1):
        slot = kvg.at[1 - t, lax.rem(z + 1, nz)]
        remote(slot, slot, kp_send.at[k], kp_recv.at[k], partner).wait_recv()
    allowed = lax.broadcasted_iota(jnp.int32, (1, nz * BLOCK), 1) < (z + 1) * BLOCK
    rope_group = lax.broadcasted_iota(jnp.int32, (nz, short, LANES), 2) // ROPE
    outs = []
    low = lax.broadcasted_iota(jnp.int32, (BLOCK, LANES), 1) < LANES // 2
    for s in range(count):
        tight = kvg[s, :, BLOCK : BLOCK + short, :LANES].astype(F32)
        spread = [jnp.where(rope_group == g, tight, 0.0) for g in range(groups)]
        keys = jnp.concatenate(
            [
                kvg[s, :, 0:BLOCK, :].reshape(nz * BLOCK, kv_total),
                jnp.concatenate(spread, axis=1).reshape(nz * BLOCK, LANES).astype(BF16),
            ],
            axis=1,
        )
        scores = mm_nt(jnp.concatenate(stacked[s], axis=0), keys) * (NOPE + ROPE) ** (-0.5)
        scores = jnp.where(allowed, scores, -1e30)
        peak = jnp.max(scores, axis=-1, keepdims=True)
        weights = jnp.where(allowed, jnp.exp(scores - peak), 0.0)
        total = jnp.sum(weights, axis=-1, keepdims=True)
        mixed = (mm(weights, keys[:, :kv_total]) / total).astype(BF16)
        made = [
            mm(mixed[h * BLOCK : (h + 1) * BLOCK], lup_ref[:, h * LANES : (h + 1) * LANES])
            for h in range(heads)
        ]
        pairs = [
            jnp.where(low, pltpu.roll(made[h], LANES // 2, 1), made[h + 1]).astype(BF16)
            for h in range(0, heads, 2)
        ]
        outs.append(jnp.concatenate(pairs, axis=1))
    latent_heads = jnp.concatenate(outs, axis=0)

    own_c.wait()
    arrived(0, half, behind)
    arrived(1, 0, ahead)
    for k, where in enumerate((west, east)):
        held = w_part(lax.rem(x + 2, nx), k)
        remote(held, held, v_send.at[k], v_recv.at[k], where).wait_recv()
    for sl in range(2):
        for xl in range(nx):
            slot = homed.at[sl, xl]
            where = {"fs": xl, "sp": 2 * x + sl + half * (1 - t), "tp": zh}
            remote(slot, slot, h_send.at[0], h_recv.at[sl, xl], where).wait_recv()
    delta_heads = [homed[:, xl].reshape(rows, HEAD) for xl in range(nx)]
    joined = jnp.concatenate(delta_heads + [latent_heads], axis=1)
    width = wo.shape[0] * wo.shape[1] * wo.shape[2]
    columns = wo[...].reshape(width, wo.shape[3])
    part_out[...] = mm_nt(joined, columns).astype(BF16)
    swap_parts = begin(remote(part_out, part_in, p_send.at[0], p_recv.at[0], partner))
    swap_parts.wait_recv()
    whole = part_out[...].astype(F32) + part_in[...].astype(F32)
    scale = lax.rsqrt(jnp.mean(whole * whole, axis=-1, keepdims=True) + NORM_EPS)
    own_half = jnp.where(t == 0, whole[:, : width // 2], whole[:, width // 2 :])
    out_ref[...] = (own_half * scale * post_ref[...]).astype(BF16)

    for copy in started:
        copy.wait_send()

    def drain(step, carry):
        for part in [*range(nx), None]:
            go_right(step, part, z).wait_send()

            @pl.when(step < reach_l)
            def _():
                go_left(step, part, z).wait_send()

        return carry

    lax.fori_loop(0, reach_r, drain, 0)

    def drain_columns(slot, carry):
        for k, where in enumerate((east, west)):
            remote(
                wz.at[slot], wo.at[slot, x], w_send.at[k, slot], w_recv.at[k, slot], where
            ).wait_send()
        return carry

    lax.fori_loop(0, nz, drain_columns, 0)

    @pl.when(t == 0)
    def _():
        crossing.wait_send()


def layer(nz, nx, *operands):
    tokens, query_weight, out_cols, latent_up = (operands[k] for k in (0, 2, 9, 13))
    half = nz // 2
    seqs, length, width = tokens.shape
    rows = seqs * length
    span = query_weight.shape[0]
    dma = pltpu.SemaphoreType.DMA

    def pair(*shape):
        return [dma(shape), dma(shape)]

    specs = [pl.BlockSpec(memory_space=VM)] * len(operands)
    specs[8] = pl.BlockSpec(memory_space=pltpu.SMEM)
    return pl.pallas_call(
        functools.partial(layer_kernel, nz, nx),
        out_shape=jax.ShapeDtypeStruct((rows, width // 2), BF16),
        in_specs=specs,
        out_specs=pl.BlockSpec(memory_space=VM),
        scratch_shapes=[
            VM((seqs * nx, length, width), BF16),
            VM((nx * rows, width), BF16),
            VM((nz, nx * span, 4 * LANES), BF16),
            VM((nz, *out_cols.shape), BF16),
            VM((nx, span, LANES), BF16),
            VM((nx * rows, 4 * LANES), F32),
            VM((2 * nx, LANES, 4 * LANES), BF16),
            VM((half, BLOCK, 3 * HEAD), BF16),
            VM((half, 2, LANES), F32),
            VM((nx, rows, LANES), BF16),
            VM((half, BLOCK, 3 * HEAD), BF16),
            VM((half, 2, LANES), F32),
            VM((2 * nx, rows, LANES), BF16),
            VM((seqs, nz, length + length * ROPE // LANES, latent_up.shape[0]), BF16),
            VM((nz, nx, *out_cols.shape), BF16),
            VM((2, nx, BLOCK, HEAD), BF16),
            VM((half, BLOCK, HEAD), BF16),
            VM((HEAD, HEAD), F32),
            VM((HEAD, HEAD), F32),
            VM((rows, width), BF16),
            VM((rows, width), BF16),
            dma((6,)),
            *pair(nx - 1, 4),
            *pair(nx - 1),
            *pair(nx - 1),
            *pair(half, nx + 1),
            *pair(half - 1, nx + 1),
            *pair(2 * nx - 1),
            *pair(half),
            *pair(half),
            *pair(half),
            *pair(half - 1),
            *pair(nz - 1),
            *pair(2, nz),
            *pair(2),
            *pair(1),
            dma((half,)),
            dma((2, nx)),
            *pair(1),
        ],
        compiler_params=pltpu.CompilerParams(collective_id=1, has_side_effects=True),
        name="layer",
    )(*operands)


def rope_tables(count, length):
    frequency = ROPE_THETA ** (-np.arange(0, ROPE, 2, dtype=np.float64) / ROPE)
    frequency = np.tile(frequency, LANES // (ROPE // 2))[None, :]

    def both(positions):
        angles = positions[:, None] * frequency
        return np.stack([np.cos(angles), np.sin(angles)]).astype(np.float32)

    return both(np.arange(count) * float(length)), both(np.arange(length) * 1.0)


def local(
    tokens,
    pre_gain,
    query_weight,
    key_weight,
    value_weight,
    beta_weight,
    decay_weight,
    decay_rate,
    delta_gain,
    query_down,
    latent_down,
    rope_weight,
    query_gain,
    latent_gain,
    query_up,
    latent_up,
    delta_out,
    latent_out,
    post_gain,
):
    nz, nx = lax.axis_size("sp"), lax.axis_size("fs")
    z, x = lax.axis_index("sp"), lax.axis_index("fs")
    seq_count, token_count = tokens.shape[:2]
    span = query_weight.shape[0]
    small = jnp.concatenate(
        [
            lax.dynamic_slice_in_dim(array, (z * nx + x) * span, span, 0)
            for array in (rope_weight, beta_weight, decay_weight)
        ],
        axis=1,
    )
    small = jnp.pad(small, ((0, 0), (0, LANES - small.shape[1])))
    out_cols = jnp.concatenate([delta_out, latent_out], axis=0).T
    far, near = rope_tables(nz, token_count)
    result = layer(
        nz,
        nx,
        tokens,
        pre_gain[None],
        query_weight,
        key_weight,
        value_weight,
        query_down,
        latent_down,
        small,
        decay_rate,
        out_cols,
        query_gain[None],
        latent_gain[None],
        query_up,
        latent_up,
        jnp.asarray(far),
        jnp.asarray(near),
        delta_gain[None],
        post_gain[None],
    )
    return result.reshape(seq_count, token_count, result.shape[1])


def solution(mesh):
    return jax.shard_map(
        local,
        mesh=mesh,
        in_specs=(
            P(("grp", "fs"), "sp", None),
            P(),
            P(("sp", "fs"), "tp"),
            P(("sp", "fs"), "tp"),
            P(("sp", "fs"), "tp"),
            P(),
            P(),
            P(),
            P(),
            P(("sp", "fs"), None),
            P(("sp", "fs"), None),
            P(),
            P(),
            P(),
            P(None, "tp"),
            P(None, "tp"),
            P("tp", ("sp", "fs")),
            P("tp", ("sp", "fs")),
            P("tp"),
        ),
        out_specs=P(("grp", "fs"), "sp", "tp"),
        check_vma=False,
    )
```

```python
import functools

import jax
import jax.numpy as jnp
import numpy as np
from jax import lax
from jax.experimental import pallas as pl
from jax.experimental.pallas import tpu as pltpu
from jax.sharding import PartitionSpec as P

HEAD = 128
NOPE = 64
ROPE = 32
VDIM = 64
BLOCK = 64
LANES = 128

NORM_EPS = 1e-06
ROPE_THETA = 10000.0
F32 = jnp.float32
BF16 = jnp.bfloat16
MESH = pl.DeviceIdType.MESH
VM = pltpu.VMEM


def remote(src, dst, send_sem, recv_sem, where):
    return pltpu.make_async_remote_copy(
        src_ref=src,
        dst_ref=dst,
        send_sem=send_sem,
        recv_sem=recv_sem,
        device_id=where,
        device_id_type=MESH,
    )


def greet(places, count):
    barrier = pltpu.get_barrier_semaphore()
    for place in places:
        pl.semaphore_signal(barrier, inc=1, device_id=place, device_id_type=MESH)
    pl.semaphore_wait(barrier, count)


def mm(left, right):
    return lax.dot_general(
        left.astype(BF16), right.astype(BF16), (((1,), (0,)), ((), ())), preferred_element_type=F32
    )


def mm_nt(left, right):
    return lax.dot_general(
        left.astype(BF16), right.astype(BF16), (((1,), (1,)), ((), ())), preferred_element_type=F32
    )


def unit(values):
    return values * lax.rsqrt(jnp.sum(values * values, axis=-1, keepdims=True) + NORM_EPS)


def swish(values):
    return values * (1.0 / (1.0 + jnp.exp(-values)))


def layer_kernel(
    nz, nx, tok_ref, pre_ref, wq_ref, wk_ref, wv_ref, qd_ref, kvd_ref, small_ref, rate_ref, wt_ref,
    qgain_ref, kvgain_ref, qup_ref, lup_ref, far_ref, near_ref, dgain_ref, out_ref,
    toks, normed, ws, wz, side, proj, place, blocks, lines_out, latents,
    dr, gr, lr, kvg, wo, homed, ready, state_out, state_in, part_out, part_in,
    loc_sem, wx_send, wx_recv, tok_send, tok_recv, fwd_send, fwd_recv, r_send, r_recv, l_send, l_recv,
    a_send, a_recv, d_send, d_recv, g_send, g_recv, kr_send, kr_recv, kl_send, kl_recv,
    kp_send, kp_recv, w_send, w_recv, v_send, v_recv, st_send, st_recv, h_send, h_recv, p_send, p_recv,
):
    z, x, t = lax.axis_index("sp"), lax.axis_index("fs"), lax.axis_index("tp")
    half = nz // 2
    zh, zl = z // half, lax.rem(z, half)
    lane_t = 1 - zh
    cores = 2 * nx
    span = wq_ref.shape[0]
    rows = tok_ref.shape[0] * tok_ref.shape[1]
    count = rows // BLOCK
    partner = {"tp": 1 - t}
    near = [
        (dx, dt, lax.rem(x + dx, nx), lax.rem(t + dt, 2), lax.rem(x + nx - dx, nx))
        for dx in range(nx)
        for dt in range(2)
        if dx or dt
    ]
    others = [lax.rem(x + d, nx) for d in range(1, nx)]
    right, left = {"sp": lax.rem(z + 1, nz)}, {"sp": lax.rem(z + nz - 1, nz)}
    east, west = {"fs": lax.rem(x + 1, nx)}, {"fs": lax.rem(x + nx - 1, nx)}
    sources = [{"fs": back, "tp": to} for dx, dt, fx, to, back in near]
    sources += [{"sp": lax.rem(z + hop, nz)} for hop in (1, 2, nz - 2, nz - 1)]
    sources += [{"sp": half * t + j, "tp": 1 - zh} for j in range(half)]
    sources += [
        {"fs": xl, "sp": 2 * x + sl + half * (1 - t), "tp": zh} for sl in range(2) for xl in range(nx)
    ]
    greet(sources, len(sources))
    started = []

    def begin(copy):
        copy.start()
        started.append(copy)
        return copy

    def local(src, dst, k):
        copy = pltpu.make_async_copy(src, dst, loc_sem.at[k])
        copy.start()
        return copy

    def chunk(slot, part):
        if part is None:
            return wz.at[slot]
        return ws.at[slot, pl.ds(pl.multiple_of(part * span, span), span)]

    def piece(k):
        return ws.at[z, pl.ds(pl.multiple_of(x * span, span), span), pl.ds(k * LANES, LANES)]

    def columns_of(ref, owner):
        return ref.at[:, pl.ds(pl.multiple_of(owner * LANES, LANES), LANES)]

    mains = (wq_ref, wk_ref, wv_ref)
    for d, o in enumerate(others):
        for k, ref in enumerate(mains):
            begin(
                remote(columns_of(ref, o), piece(k), wx_send.at[d, k], wx_recv.at[d, k], {"fs": o})
            )
    own_w = [local(columns_of(ref, x), piece(k), k) for k, ref in enumerate(mains)]
    own_o = local(wt_ref, wz.at[z], 3)
    own_t = local(tok_ref, toks.at[pl.ds(2 * x, 2)], 4)

    reach_r, reach_l = nz // 2, nz // 2 - 1

    def go_right(step, part, slot):
        mark = nx if part is None else part
        return remote(
            chunk(slot, part), chunk(slot, part), r_send.at[step, mark], r_recv.at[step, mark], right
        )

    def go_left(step, part, slot):
        mark = nx if part is None else part
        return remote(
            chunk(slot, part), chunk(slot, part), l_send.at[step, mark], l_recv.at[step, mark], left
        )

    own_o.wait()
    go_right(0, None, z).start()
    go_left(0, None, z).start()

    q_width, kv_width = qd_ref.shape[1] // cores, kvd_ref.shape[1] // cores
    rope_width = ROPE // cores
    at_rope = q_width + kv_width
    at_beta = at_rope + rope_width

    def picked(source, lane, first, stop, start):
        return (lane >= first) & (lane < stop) & (source == start + lane - first)

    def ones(mask):
        return jnp.where(mask, 1.0, 0.0)

    def iotas(depth):
        shape = (depth, LANES)
        return lax.broadcasted_iota(jnp.int32, shape, 0), lax.broadcasted_iota(jnp.int32, shape, 1)

    for o in range(nx):
        core, head = 2 * o + t, nx * t + o
        source, lane = iotas(qd_ref.shape[1])
        made = mm(qd_ref[...], ones(picked(source, lane, 0, q_width, q_width * core)))
        source, lane = iotas(kvd_ref.shape[1])
        made += mm(kvd_ref[...], ones(picked(source, lane, q_width, at_rope, kv_width * core)))
        source, lane = iotas(LANES)
        select = picked(source, lane, at_rope, at_beta, rope_width * core)
        select = select | picked(source, lane, at_beta, at_beta + 1, ROPE + head)
        select = select | picked(source, lane, at_beta + 1, at_beta + 2, ROPE + cores + head)
        made += mm(small_ref[...], ones(select))
        side[o] = made.astype(BF16)
    for d, o in enumerate(others):
        k = len(mains)
        begin(remote(side.at[o], piece(k), wx_send.at[d, k], wx_recv.at[d, k], {"fs": o}))
    own_w.append(local(side.at[x], piece(len(mains)), 5))
    for d, o in enumerate(others):
        begin(remote(tok_ref.at[t], toks.at[2 * x + t], tok_send.at[d], tok_recv.at[d], {"fs": o}))

    for d in range(nx):
        part = lax.rem(x + nx - d, nx)
        if d == 0:
            for copy in own_w:
                copy.wait()
        else:
            for k in range(len(mains) + 1):
                remote(
                    piece(k), piece(k), wx_send.at[d - 1, k], wx_recv.at[d - 1, k], {"fs": part}
                ).wait_recv()
        go_right(0, part, z).start()
        go_left(0, part, z).start()

    from_lane = lax.broadcasted_iota(jnp.int32, (LANES, 4 * LANES), 0)
    to_lane = lax.broadcasted_iota(jnp.int32, (LANES, 4 * LANES), 1)
    kv_total = kv_width * cores
    spot = to_lane - kv_total
    spot_in = lax.rem(to_lane, ROPE)
    sign = jnp.where(spot_in < ROPE // 2, -1.0, 1.0)
    is_kv = (from_lane >= q_width) & (from_lane < at_rope)
    is_rope = (from_lane >= at_rope) & (from_lane < at_beta)
    for c in range(cores):
        entry = from_lane - at_rope + rope_width * c
        kept = is_kv & (to_lane == from_lane - q_width + kv_width * c)
        straight = is_rope & (spot >= 0) & (spot < LANES) & (spot_in == entry)
        swapped = is_rope & (spot >= LANES) & (lax.rem(spot_in + ROPE // 2, ROPE) == entry)
        place[c] = (ones(kept | straight) + jnp.where(swapped, sign, 0.0)).astype(BF16)

    early = (reach_r * 5) // 8

    def columns_on(slot):
        for k, where in enumerate((east, west)):
            remote(wz.at[slot], wo.at[slot, x], w_send.at[k, slot], w_recv.at[k, slot], where).start()

    def columns_step(step):
        from_left = lax.rem(z + 2 * nz - 1 - step, nz)
        from_right = lax.rem(z + 1 + step, nz)
        go_right(step, None, from_left).wait_recv()
        columns_on(from_left)

        @pl.when(step < reach_r - 1)
        def _():
            go_right(step + 1, None, from_left).start()

        @pl.when(step < reach_l)
        def _():
            go_left(step, None, from_right).wait_recv()
            columns_on(from_right)

        @pl.when(step < reach_l - 1)
        def _():
            go_left(step + 1, None, from_right).start()

    def weights_step(step):
        from_left = lax.rem(z + 2 * nz - 1 - step, nz)
        from_right = lax.rem(z + 1 + step, nz)
        for d in range(nx):
            part = lax.rem(x + nx - d, nx)
            go_right(step, part, from_left).wait_recv()

            @pl.when(step < reach_r - 1)
            def _():
                go_right(step + 1, part, from_left).start()

            @pl.when(step < reach_l)
            def _():
                go_left(step, part, from_right).wait_recv()

            @pl.when(step < reach_l - 1)
            def _():
                go_left(step + 1, part, from_right).start()

    def ring(step, carry):
        weights_step(step)
        columns_step(step)
        return carry

    def last_weights(step, carry):
        weights_step(step)
        return carry

    def last_columns(step, carry):
        columns_step(step)
        return carry

    columns_on(z)
    lax.fori_loop(0, early, ring, 0)
    own_t.wait()
    for d in range(nx - 1):
        held = toks.at[2 * lax.rem(x + nx - 1 - d, nx) + t]
        remote(held, held, tok_send.at[d], tok_recv.at[d], partner).wait_recv()
        begin(remote(held, held, fwd_send.at[d], fwd_recv.at[d], partner))
    lax.fori_loop(early, early + 1, ring, 0)
    for d in range(nx - 1):
        held = toks.at[2 * lax.rem(x + nx - 1 - d, nx) + 1 - t]
        remote(held, held, fwd_send.at[d], fwd_recv.at[d], partner).wait_recv()

    def normalize(i, carry):
        values = toks[i].astype(F32)
        scale = lax.rsqrt(jnp.mean(values * values, axis=-1, keepdims=True) + NORM_EPS)
        normed[pl.ds(pl.multiple_of(i * BLOCK, BLOCK), BLOCK), :] = (
            values * scale * pre_ref[...]
        ).astype(BF16)
        return carry

    lax.fori_loop(0, toks.shape[0], normalize, 0)
    lax.fori_loop(early + 1, reach_r - 1, ring, 0)
    depth = ws.shape[1]

    def product(slot):
        lhs = normed[:, pl.ds(pl.multiple_of(slot * depth, depth), depth)]
        return lax.dot_general(lhs, ws[slot], (((1,), (0,)), ((), ())), preferred_element_type=F32)

    def gather_product(i, carry):
        proj[...] += product(lax.rem(z + nz - reach_l + i, nz))
        return carry

    proj[...] = product(z + 0)
    lax.fori_loop(0, reach_l, gather_product, 0)
    lax.fori_loop(reach_l + 1, 2 * reach_l + 1, gather_product, 0)
    lax.fori_loop(reach_r - 1, reach_r, last_weights, 0)
    proj[...] += product(lax.rem(z + reach_r, nz))

    for o in range(nx):
        latents[o] = proj[o * rows : (o + 1) * rows, 3 * HEAD :].astype(BF16)
    own_l = local(latents.at[x], lr.at[2 * x + t], 0)
    for k, (dx, dt, fx, to, back) in enumerate(near):
        begin(
            remote(latents.at[fx], lr.at[2 * x + t], a_send.at[k], a_recv.at[k], {"fs": fx, "tp": to})
        )

    def w_part(owner, upper):
        return wo.at[pl.ds(half * upper, half), owner]

    size = 2 * BLOCK
    row = lax.broadcasted_iota(jnp.int32, (size, size), 0)
    col = lax.broadcasted_iota(jnp.int32, (size, size), 1)
    eye = row == col
    same = (row // BLOCK) == (col // BLOCK)
    rate = rate_ref[nx * t + x]
    even = lax.rem(z, 2) == 0
    line = lax.broadcasted_iota(jnp.int32, (2, LANES), 0)
    first_half = lax.broadcasted_iota(jnp.int32, (2, LANES), 1) < LANES // 2
    for p in range(half // 2):
        blocks[2 * p : 2 * p + 2] = (
            proj[p * size : (p + 1) * size, : 3 * HEAD].astype(BF16).reshape(2, BLOCK, 3 * HEAD)
        )
        tail = proj[p * size : (p + 1) * size, 3 * HEAD :]
        write = 1.0 / (1.0 + jnp.exp(-tail[:, at_beta : at_beta + 1]))
        pushed = tail[:, at_beta + 1 : at_beta + 2]
        fade = -rate * (jnp.maximum(pushed, 0.0) + jnp.log1p(jnp.exp(-jnp.abs(pushed))))
        write_row = jnp.sum(jnp.where(eye, write, 0.0), axis=0, keepdims=True)
        fade_row = jnp.sum(jnp.where(same & (row <= col), fade, 0.0), axis=0, keepdims=True)
        both_rows = jnp.where(line == 0, write_row, fade_row)
        rolled = pltpu.roll(both_rows, LANES // 2, 1)
        lines_out[2 * p] = jnp.where(
            even, jnp.where(first_half, both_rows, 0.0), jnp.where(first_half, 0.0, rolled)
        )
        lines_out[2 * p + 1] = jnp.where(
            even, jnp.where(first_half, rolled, 0.0), jnp.where(first_half, 0.0, both_rows)
        )

    def send_lane(i):
        s = lax.rem(zl + i, half)
        where = {"sp": s + half * (1 - t), "tp": zh}
        begin(remote(lines_out.at[s], gr.at[zl], g_send.at[i], g_recv.at[zl], where))
        begin(remote(blocks.at[s], dr.at[zl], d_send.at[i], d_recv.at[zl], where))

    for i in range(half):
        send_lane(i)
    lax.fori_loop(reach_r - 1, reach_r, last_columns, 0)

    for k, (dx, dt, fx, to, back) in enumerate(near):
        slot = lr.at[2 * back + to]
        remote(slot, slot, a_send.at[k], a_recv.at[k], {"fs": back, "tp": to}).wait_recv()
    own_l.wait()

    lane = lax.broadcasted_iota(jnp.int32, (rows, LANES), 1)
    far_cos, far_sin = far_ref[0, pl.ds(z, 1), :], far_ref[1, pl.ds(z, 1), :]
    near_cos = jnp.concatenate([near_ref[0]] * count, axis=0)
    near_sin = jnp.concatenate([near_ref[1]] * count, axis=0)
    cosine = far_cos * near_cos - far_sin * near_sin
    sine = far_sin * near_cos + far_cos * near_sin
    slab = mm(lr[0], place[0])
    for c in range(1, cores):
        slab = slab + mm(lr[c], place[c])
    kv_lat = slab[:, :kv_total]
    kv_lat = kv_lat * lax.rsqrt(jnp.mean(kv_lat * kv_lat, axis=-1, keepdims=True) + NORM_EPS)
    turned = slab[:, kv_total : kv_total + LANES] * cosine + slab[:, kv_total + LANES :] * sine
    latent_keys = (kv_lat * kvgain_ref[...]).astype(BF16)
    groups = LANES // ROPE
    short = BLOCK // groups
    in_group = lax.broadcasted_iota(jnp.int32, (short, LANES), 1) // ROPE
    for s in range(count):
        kvg[s, z, 0:BLOCK] = latent_keys[s * BLOCK : (s + 1) * BLOCK]
        tight = jnp.zeros((short, LANES), F32)
        for g in range(groups):
            at = s * BLOCK + g * short
            tight = jnp.where(in_group == g, turned[at : at + short], tight)
        kvg[s, z, BLOCK : BLOCK + short] = jnp.concatenate(
            [tight, jnp.zeros((short, kv_total - LANES), F32)], axis=1
        ).astype(BF16)

    def key_right(distance, slot):
        hop = 2 - distance % 2
        sems = kr_send.at[distance - 1], kr_recv.at[distance - 1]
        return remote(kvg.at[t, slot], kvg.at[t, slot], *sems, {"sp": lax.rem(z + hop, nz)})

    def key_left(distance, slot):
        hop = 2 - distance % 2
        sems = kl_send.at[distance - 1], kl_recv.at[distance - 1]
        return remote(kvg.at[t, slot], kvg.at[t, slot], *sems, {"sp": lax.rem(z + nz - hop, nz)})

    def across(slot, k):
        return remote(kvg.at[t, slot], kvg.at[t, slot], kp_send.at[k], kp_recv.at[k], partner)

    for distance in (2, 1):
        begin(key_right(distance, z))
        begin(key_left(distance, z))

    q_lat = jnp.concatenate(
        [
            jnp.where(
                lane < LANES // 2,
                lr[c].astype(F32),
                pltpu.roll(lr[c + 1].astype(F32), LANES // 2, 1),
            )
            for c in range(0, cores, 2)
        ],
        axis=1,
    )
    q_lat = q_lat * lax.rsqrt(jnp.mean(q_lat * q_lat, axis=-1, keepdims=True) + NORM_EPS)
    query = mm(q_lat * qgain_ref[...], qup_ref[...]).astype(BF16).astype(F32)
    head_width = NOPE + ROPE
    heads = query.shape[1] // head_width
    entry = lax.rem(col, ROPE)
    repeat = ones(row == NOPE + entry)
    exchange = jnp.where((entry >= ROPE // 2) & (row == NOPE + entry - ROPE // 2), 1.0, 0.0)
    exchange = exchange - ones((entry < ROPE // 2) & (row == NOPE + entry + ROPE // 2))
    stacked = [[] for _ in range(count)]
    for h in range(heads):
        own = query[:, h * head_width : (h + 1) * head_width]
        own = jnp.concatenate([own, jnp.zeros((rows, LANES - head_width), F32)], axis=1)
        absorbed = mm_nt(
            jnp.where(lane < NOPE, own, 0.0), lup_ref[:, h * LANES : (h + 1) * LANES]
        )
        turn = mm(own, repeat) * cosine + mm(own, exchange) * sine
        joined = jnp.concatenate([absorbed, turn], axis=1).astype(BF16)
        for s in range(count):
            stacked[s].append(joined[s * BLOCK : (s + 1) * BLOCK])

    own_c = local(wz, wo.at[:, x], 1)
    behind, ahead = lax.rem(x + nx - 1, nx), lax.rem(x + 1, nx)

    def arrived(k, first, owner):
        def one(slot, carry):
            held = wo.at[slot, owner]
            remote(held, held, w_send.at[k, slot], w_recv.at[k, slot], east).wait_recv()
            return carry

        lax.fori_loop(first, first + half, one, 0)

    def key_turn(turn_at):
        for distance in (2 * turn_at + 2, 2 * turn_at + 1):
            from_left = lax.rem(z + nz - distance, nz)
            from_right = lax.rem(z + distance, nz)
            key_right(distance, from_left).wait_recv()
            if distance % 2 == 0:
                for further in (distance + 2, distance + 1):
                    if further <= reach_r:
                        begin(key_right(further, from_left))
            begin(across(from_left, distance - 1))
            if distance <= reach_l:
                key_left(distance, from_right).wait_recv()
                if distance % 2 == 0:
                    for further in (distance + 2, distance + 1):
                        if further <= reach_l:
                            begin(key_left(further, from_right))
                begin(across(from_right, reach_r + distance - 1))

    key_turn(0)
    arrived(0, 0, behind)
    begin(remote(w_part(behind, 0), w_part(behind, 0), v_send.at[0], v_recv.at[0], east))
    arrived(1, half, ahead)
    begin(remote(w_part(ahead, 1), w_part(ahead, 1), v_send.at[1], v_recv.at[1], west))

    for j in range(half):
        where = {"sp": half * t + j, "tp": 1 - zh}
        remote(gr.at[j], gr.at[j], g_send.at[j], g_recv.at[j], where).wait_recv()
        remote(dr.at[j], dr.at[j], d_send.at[j], d_recv.at[j], where).wait_recv()

    strict = same & (row > col)
    causal = same & (row >= col)
    wide_row = lax.broadcasted_iota(jnp.int32, (size, 2 * size), 0)

    def upright(line, where):
        return jnp.sum(jnp.where(where, line, 0.0), axis=1, keepdims=True)

    pairs_at = range(half // 2)
    raws = [dr[2 * p : 2 * p + 2].reshape(size, 3 * HEAD).astype(F32) for p in pairs_at]
    qs = [unit(swish(raw[:, :HEAD])) * HEAD**-0.5 for raw in raws]
    ks = [unit(swish(raw[:, HEAD : 2 * HEAD])) for raw in raws]
    vs = [swish(raw[:, 2 * HEAD :]) for raw in raws]
    marks = [gr[2 * p] + gr[2 * p + 1] for p in pairs_at]
    betas = [upright(mark[0:1], eye) for mark in marks]
    sums = [upright(mark[1:2], eye) for mark in marks]
    ends = [
        upright(mark[1:2], col == (row // BLOCK) * BLOCK + BLOCK - 1) for mark in marks
    ]
    decays = [
        jnp.exp(jnp.where(causal, upon - mark[1:2], 0.0)) for upon, mark in zip(sums, marks)
    ]
    lowers = [
        jnp.where(strict, beta * mm_nt(k, k) * decay, 0.0)
        for beta, k, decay in zip(betas, ks, decays)
    ]
    inverses = [
        jnp.where(eye, 1.0, 0.0) - jnp.where((row // 2 == col // 2), low, 0.0) for low in lowers
    ]
    level = 2
    while level < BLOCK:
        pick = (row // (2 * level) == col // (2 * level)) & (row // level != col // level)
        firsts = [mm(inv, jnp.where(pick, low, 0.0)) for inv, low in zip(inverses, lowers)]
        inverses = [inv - mm(first, inv) for first, inv in zip(firsts, inverses)]
        level *= 2
    scores_of = [
        jnp.where(causal, mm_nt(q, k) * decay, 0.0) for q, k, decay in zip(qs, ks, decays)
    ]
    boths = [
        mm(inv, jnp.concatenate([beta * v, beta * k * jnp.exp(upon)], axis=1))
        for inv, beta, v, k, upon in zip(inverses, betas, vs, ks, sums)
    ]
    keys_t = [(k * jnp.exp(end - upon)).T for k, end, upon in zip(ks, ends, sums)]
    moves_of = [
        [mm(key_t, jnp.where(wide_row // BLOCK == h, both, 0.0)) for h in range(2)]
        for key_t, both in zip(keys_t, boths)
    ]
    terms = [
        (
            qs[p] * jnp.exp(sums[p]),
            scores_of[p],
            boths[p],
            moves_of[p],
            [jnp.exp(ends[p][h * BLOCK : h * BLOCK + 1]) for h in range(2)],
        )
        for p in pairs_at
    ]

    key_turn(1)
    total = jnp.concatenate([jnp.zeros((size, size), F32), jnp.where(eye, 1.0, 0.0)], axis=1)
    states = []
    for j in range(half):
        states.append(total)
        move, factor = terms[j // 2][3][j % 2], terms[j // 2][4][j % 2]
        grown = factor * total - mm(move[:, size:], total)
        total = jnp.concatenate([grown[:, :size] + move[:, :size], grown[:, size:]], axis=1)

    state_out[...] = total[:, :size]
    crossing = remote(state_out, state_in, st_send.at[0], st_recv.at[0], partner)

    @pl.when(t == 0)
    def _():
        state_in[...] = jnp.zeros_like(state_in)
        crossing.start()

    key_turn(2)

    @pl.when(t == 1)
    def _():
        crossing.wait_recv()

    start = state_in[...]
    for p in range(half // 2):
        queries, scores, both, _, _ = terms[p]
        read, fixed = [], []
        for h in range(2):
            j = 2 * p + h
            state = states[j][:, :size] + mm(states[j][:, size:], start)
            cut = slice(h * BLOCK, (h + 1) * BLOCK)
            got = mm(jnp.concatenate([both[cut, size:], queries[cut]], axis=0), state)
            fixed.append(both[cut, :size] - got[:BLOCK])
            read.append(got[BLOCK:])
        raw = jnp.concatenate(read, axis=0) + mm(scores, jnp.concatenate(fixed, axis=0))
        raw = raw * lax.rsqrt(jnp.mean(raw * raw, axis=-1, keepdims=True) + NORM_EPS)
        done = (raw * dgain_ref[...]).astype(BF16)
        ready[2 * p] = done[:BLOCK]
        ready[2 * p + 1] = done[BLOCK:]

    for i in range(half):
        j = lax.rem(zl + i, half)
        begin(
            remote(
                ready.at[j],
                homed.at[lax.rem(zl, 2), x],
                h_send.at[i],
                h_recv.at[lax.rem(zl, 2), x],
                {"fs": zl // 2, "sp": half * t + j, "tp": lane_t},
            )
        )

    for turn_at in range(3, reach_r // 2):
        key_turn(turn_at)
    for k in range(nz - 1):
        slot = kvg.at[1 - t, lax.rem(z + 1, nz)]
        remote(slot, slot, kp_send.at[k], kp_recv.at[k], partner).wait_recv()
    allowed = lax.broadcasted_iota(jnp.int32, (1, nz * BLOCK), 1) < (z + 1) * BLOCK
    rope_group = lax.broadcasted_iota(jnp.int32, (nz, short, LANES), 2) // ROPE
    outs = []
    low = lax.broadcasted_iota(jnp.int32, (BLOCK, LANES), 1) < LANES // 2
    for s in range(count):
        tight = kvg[s, :, BLOCK : BLOCK + short, :LANES].astype(F32)
        spread = [jnp.where(rope_group == g, tight, 0.0) for g in range(groups)]
        keys = jnp.concatenate(
            [
                kvg[s, :, 0:BLOCK, :].reshape(nz * BLOCK, kv_total),
                jnp.concatenate(spread, axis=1).reshape(nz * BLOCK, LANES).astype(BF16),
            ],
            axis=1,
        )
        scores = mm_nt(jnp.concatenate(stacked[s], axis=0), keys) * (NOPE + ROPE) ** (-0.5)
        scores = jnp.where(allowed, scores, -1e30)
        peak = jnp.max(scores, axis=-1, keepdims=True)
        weights = jnp.where(allowed, jnp.exp(scores - peak), 0.0)
        total = jnp.sum(weights, axis=-1, keepdims=True)
        mixed = (mm(weights, keys[:, :kv_total]) / total).astype(BF16)
        made = [
            mm(mixed[h * BLOCK : (h + 1) * BLOCK], lup_ref[:, h * LANES : (h + 1) * LANES])
            for h in range(heads)
        ]
        pairs = [
            jnp.where(low, pltpu.roll(made[h], LANES // 2, 1), made[h + 1]).astype(BF16)
            for h in range(0, heads, 2)
        ]
        outs.append(jnp.concatenate(pairs, axis=1))
    latent_heads = jnp.concatenate(outs, axis=0)

    own_c.wait()
    arrived(0, half, behind)
    arrived(1, 0, ahead)
    for k, where in enumerate((west, east)):
        held = w_part(lax.rem(x + 2, nx), k)
        remote(held, held, v_send.at[k], v_recv.at[k], where).wait_recv()
    for sl in range(2):
        for xl in range(nx):
            slot = homed.at[sl, xl]
            where = {"fs": xl, "sp": 2 * x + sl + half * (1 - t), "tp": zh}
            remote(slot, slot, h_send.at[0], h_recv.at[sl, xl], where).wait_recv()
    delta_heads = [homed[:, xl].reshape(rows, HEAD) for xl in range(nx)]
    joined = jnp.concatenate(delta_heads + [latent_heads], axis=1)
    width = wo.shape[0] * wo.shape[1] * wo.shape[2]
    columns = wo[...].reshape(width, wo.shape[3])
    part_out[...] = mm_nt(joined, columns).astype(BF16)
    swap_parts = begin(remote(part_out, part_in, p_send.at[0], p_recv.at[0], partner))
    swap_parts.wait_recv()
    whole = part_out[...].astype(F32) + part_in[...].astype(F32)
    scale = lax.rsqrt(jnp.mean(whole * whole, axis=-1, keepdims=True) + NORM_EPS)
    own_half = jnp.where(t == 0, whole[:, : width // 2], whole[:, width // 2 :])
    out_ref[...] = own_half * scale

    for copy in started:
        copy.wait_send()

    def drain(step, carry):
        for part in [*range(nx), None]:
            go_right(step, part, z).wait_send()

            @pl.when(step < reach_l)
            def _():
                go_left(step, part, z).wait_send()

        return carry

    lax.fori_loop(0, reach_r, drain, 0)

    def drain_columns(slot, carry):
        for k, where in enumerate((east, west)):
            remote(
                wz.at[slot], wo.at[slot, x], w_send.at[k, slot], w_recv.at[k, slot], where
            ).wait_send()
        return carry

    lax.fori_loop(0, nz, drain_columns, 0)

    @pl.when(t == 0)
    def _():
        crossing.wait_send()


def layer(nz, nx, *operands):
    tokens, query_weight, out_cols, latent_up = (operands[k] for k in (0, 2, 9, 13))
    half = nz // 2
    seqs, length, width = tokens.shape
    rows = seqs * length
    span = query_weight.shape[0]
    dma = pltpu.SemaphoreType.DMA

    def pair(*shape):
        return [dma(shape), dma(shape)]

    specs = [pl.BlockSpec(memory_space=VM)] * len(operands)
    specs[8] = pl.BlockSpec(memory_space=pltpu.SMEM)
    return pl.pallas_call(
        functools.partial(layer_kernel, nz, nx),
        out_shape=jax.ShapeDtypeStruct((rows, width // 2), F32),
        in_specs=specs,
        out_specs=pl.BlockSpec(memory_space=VM),
        scratch_shapes=[
            VM((seqs * nx, length, width), BF16),
            VM((nx * rows, width), BF16),
            VM((nz, nx * span, 4 * LANES), BF16),
            VM((nz, *out_cols.shape), BF16),
            VM((nx, span, LANES), BF16),
            VM((nx * rows, 4 * LANES), F32),
            VM((2 * nx, LANES, 4 * LANES), BF16),
            VM((half, BLOCK, 3 * HEAD), BF16),
            VM((half, 2, LANES), F32),
            VM((nx, rows, LANES), BF16),
            VM((half, BLOCK, 3 * HEAD), BF16),
            VM((half, 2, LANES), F32),
            VM((2 * nx, rows, LANES), BF16),
            VM((seqs, nz, length + length * ROPE // LANES, latent_up.shape[0]), BF16),
            VM((nz, nx, *out_cols.shape), BF16),
            VM((2, nx, BLOCK, HEAD), BF16),
            VM((half, BLOCK, HEAD), BF16),
            VM((HEAD, HEAD), F32),
            VM((HEAD, HEAD), F32),
            VM((rows, width), BF16),
            VM((rows, width), BF16),
            dma((6,)),
            *pair(nx - 1, 4),
            *pair(nx - 1),
            *pair(nx - 1),
            *pair(half, nx + 1),
            *pair(half - 1, nx + 1),
            *pair(2 * nx - 1),
            *pair(half),
            *pair(half),
            *pair(half),
            *pair(half - 1),
            *pair(nz - 1),
            *pair(2, nz),
            *pair(2),
            *pair(1),
            dma((half,)),
            dma((2, nx)),
            *pair(1),
        ],
        compiler_params=pltpu.CompilerParams(collective_id=1, has_side_effects=True),
        name="layer",
    )(*operands)


def rope_tables(count, length):
    frequency = ROPE_THETA ** (-np.arange(0, ROPE, 2, dtype=np.float64) / ROPE)
    frequency = np.tile(frequency, LANES // (ROPE // 2))[None, :]

    def both(positions):
        angles = positions[:, None] * frequency
        return np.stack([np.cos(angles), np.sin(angles)]).astype(np.float32)

    return both(np.arange(count) * float(length)), both(np.arange(length) * 1.0)


def local(
    tokens,
    pre_gain,
    query_weight,
    key_weight,
    value_weight,
    beta_weight,
    decay_weight,
    decay_rate,
    delta_gain,
    query_down,
    latent_down,
    rope_weight,
    query_gain,
    latent_gain,
    query_up,
    latent_up,
    delta_out,
    latent_out,
    post_gain,
):
    nz, nx = lax.axis_size("sp"), lax.axis_size("fs")
    z, x = lax.axis_index("sp"), lax.axis_index("fs")
    seq_count, token_count = tokens.shape[:2]
    span = query_weight.shape[0]
    small = jnp.concatenate(
        [
            lax.dynamic_slice_in_dim(array, (z * nx + x) * span, span, 0)
            for array in (rope_weight, beta_weight, decay_weight)
        ],
        axis=1,
    )
    small = jnp.pad(small, ((0, 0), (0, LANES - small.shape[1])))
    out_cols = jnp.concatenate([delta_out, latent_out], axis=0).T
    far, near = rope_tables(nz, token_count)
    result = layer(
        nz,
        nx,
        tokens,
        pre_gain[None],
        query_weight,
        key_weight,
        value_weight,
        query_down,
        latent_down,
        small,
        decay_rate,
        out_cols,
        query_gain[None],
        latent_gain[None],
        query_up,
        latent_up,
        jnp.asarray(far),
        jnp.asarray(near),
        delta_gain[None],
    )
    result = (result * post_gain[None]).astype(BF16)
    return result.reshape(seq_count, token_count, result.shape[1])


def solution(mesh):
    return jax.shard_map(
        local,
        mesh=mesh,
        in_specs=(
            P(("grp", "fs"), "sp", None),
            P(),
            P(("sp", "fs"), "tp"),
            P(("sp", "fs"), "tp"),
            P(("sp", "fs"), "tp"),
            P(),
            P(),
            P(),
            P(),
            P(("sp", "fs"), None),
            P(("sp", "fs"), None),
            P(),
            P(),
            P(),
            P(None, "tp"),
            P(None, "tp"),
            P("tp", ("sp", "fs")),
            P("tp", ("sp", "fs")),
            P("tp"),
        ),
        out_specs=P(("grp", "fs"), "sp", "tp"),
        check_vma=False,
    )
```
